256 devices in a mesh: dp: 4 (over y), kv: 32 (over z, x), tp: 2 (over core).
Axes of the slice: x: 4, y: 4, z: 8, core: 2. Of those that a mesh axis runs over, the one named last changes fastest.
Arguments:
- tokens: bfloat16 [256, 4096], P('dp', ('kv', 'tp')), may hold values from -27 to 27
- lengths: int32 [256], P(('dp', 'kv')), may hold values from 1 to 64, 4096 in all
- state: float32 [256, 4, 384, 768], P(('dp', 'kv'), 'tp'), may hold values from -6 to 6
- cache_keys: bfloat16 [256, 4, 64, 384], P(('dp', 'kv'), 'tp'), may hold values from -6 to 6
- cache_values: bfloat16 [256, 4, 64, 768], P(('dp', 'kv'), 'tp'), may hold values from -6 to 6
- cache_rates: float32 [256, 4, 64, 384], P(('dp', 'kv'), 'tp'), may hold values from 0.002 to 0.3
- attn_gain: bfloat16 [4096], P('kv'), may hold values from 0.099609375 to 1.8984375
- w_query: bfloat16 [4096, 1536], P('kv', 'tp'), may hold values from -0.09375 to 0.09375
- w_key: bfloat16 [4096, 1536], P('kv', 'tp'), may hold values from -0.09375 to 0.09375
- w_value: bfloat16 [4096, 3072], P('kv', 'tp'), may hold values from -0.09375 to 0.09375
- w_gate: bfloat16 [4096, 3072], P('kv', 'tp'), may hold values from -0.09375 to 0.09375
- w_decay: bfloat16 [4096, 1536], P('kv', 'tp'), may hold values from -0.375 to 0.375
- head_gain: bfloat16 [4, 768], P('tp'), may hold values from 0.099609375 to 1.8984375
- w_out: bfloat16 [3072, 4096], P(None, ('kv', 'tp')), may hold values from -0.109375 to 0.109375
- mlp_gain: bfloat16 [4096], replicated, may hold values from 0.099609375 to 1.8984375
- w_mlp_gate: bfloat16 [4096, 11008], P(None, ('kv', 'tp')), may hold values from -0.09375 to 0.09375
- w_mlp_up: bfloat16 [4096, 11008], P(None, ('kv', 'tp')), may hold values from -0.09375 to 0.09375
- w_mlp_down: bfloat16 [11008, 4096], P(('kv', 'tp')), may hold values from -0.15625 to 0.15625
Outputs:
- result: bfloat16 [256, 4096], P('dp', ('kv', 'tp'))
The draws below stay inside these ranges and needn't reach their ends.
Inputs may be any that keep to these rules, and one draw needn't show every extreme that they name: `lengths`: each sequence's count of live slots in its block cache; slots from that count on take no part.
All inputs are finite; a program needn't handle non-finite values.
Results may differ from the reference program's by a relative error of at most 0.0085.
Values may be sent and summed in bfloat16 or wider, within the bound.
A program may use at most 64 MiB of HBM per device.

```python
import math
import jax
import jax.numpy as jnp
import numpy as np
from jax import lax

D = 4096
HEADS = 4
DK = 384
DV = 768
FF = 11008
SPAN = 64
SEQS = 256


def draw_tokens(key, part):
    base_key = jax.random.fold_in(key, 11)
    rough_key = jax.random.fold_in(key, 12)
    columns = jnp.arange(D, dtype=jnp.float32)
    rising = jnp.exp(jnp.log(3.0) * columns / (D - 1))
    rough = jax.random.uniform(rough_key, (D,), jnp.float32, 0.5, 1.5)
    values = jnp.clip(jax.random.normal(base_key, (SEQS, D), jnp.float32), -6.0, 6.0)
    return (values * rising[None, :] * rough[None, :]).astype(jnp.bfloat16)


def raised(values, stream_key, source, target, shards_of, factor):
    owner, partner = [(jnp.arange(values.shape[position]) // (values.shape[position] // shards_of)).reshape([-1 if axis == position else 1 for axis in range(values.ndim)]) for position in (source, target)]
    chosen = jax.random.permutation(stream_key, shards_of)[partner]
    strong = (owner == chosen) | (owner == (partner + shards_of // 2) % shards_of)
    return jnp.where(strong, factor * values, values)


def levels(key, extent, pieces, low, high):
    gain = 1.0
    for axis_at, shards_of in pieces:
        draws = jax.random.uniform(jax.random.fold_in(jax.random.fold_in(key, 6), axis_at), (shards_of,), jnp.float32, low / len(pieces), high / len(pieces))
        gain = gain * jnp.repeat(jnp.exp(draws), extent[axis_at] // shards_of).reshape((-1,) + (1,) * (len(extent) - 1 - axis_at))
    return gain


def split_up(amount, total, reach, skew):
    loads = [(1 << 20) // math.isqrt(grade ** skew) + 1 for grade in range(2, amount + 1)]
    surplus, holding = total - reach - (amount - 1), [1] * (amount - 1)
    while surplus > 0:
        candidates = [i for i in range(amount - 1) if holding[i] < reach]
        pool, remaining = sum([loads[i] for i in candidates]), surplus
        for i in candidates:
            extra = min(reach - holding[i], max(1, remaining * loads[i] // pool), surplus)
            holding[i] = holding[i] + extra
            surplus = surplus - extra
    return np.array([reach] + holding)


def ragged(stream_key, count, total, bound, lean):
    if count == 2:
        one = jax.random.randint(stream_key, (), max(1, total - bound), min(bound, total - 1) + 1)
        return jnp.stack([one, total - one])
    sizes = jnp.asarray(split_up(count, total, bound, lean), jnp.int32)
    pairs = (count - 1) // 2
    giver, taker = sizes[1:1 + 2 * pairs:2], sizes[2:2 + 2 * pairs:2]
    margin = jnp.minimum(giver - 1, bound - taker)
    shifted = jax.random.randint(jax.random.fold_in(stream_key, 1), (pairs,), 0, 1 << 20) % (margin + 1)
    sizes = sizes.at[1:1 + 2 * pairs:2].set(giver - shifted).at[2:2 + 2 * pairs:2].set(taker + shifted)
    return sizes[jax.random.permutation(jax.random.fold_in(stream_key, 2), count)]


def gaussian(stream_key, extent, spread, most, split=(), held_as=jnp.bfloat16):
    factor_of = levels(stream_key, extent, split, -0.22, 0.18) if split else 1.0
    entries = jax.random.normal(stream_key, extent, jnp.float32) * spread * factor_of
    return jnp.minimum(jnp.maximum(entries, -most), most).astype(held_as)


def bell_draw_with(own_key, extent, width, bound, shards, heavy, kind=jnp.bfloat16):
    drawn = width * jax.random.normal(own_key, extent, jnp.float32)
    if shards:
        drawn = drawn * levels(own_key, extent, shards, -0.22, 0.18)
    return jnp.clip(raised(drawn, jax.random.fold_in(own_key, 3), *heavy), -bound, bound).astype(kind)


def setup_inputs(seed: int = 0) -> dict:
    streams_of = jax.random.split(jax.random.key(seed), 19)
    tokens = draw_tokens(jax.random.fold_in(streams_of[18], 71), 0)
    lengths = ragged(streams_of[1], SEQS, SEQS * SPAN // 4, SPAN, 2).astype(jnp.int32)
    state = gaussian(streams_of[2], (SEQS, HEADS, DK, DV), 1.0, 6.0, ((0, 128), (1, 2)), jnp.float32)
    cache_keys = gaussian(streams_of[3], (SEQS, HEADS, SPAN, DK), 1.0, 6.0, ((0, 128), (1, 2)))
    cache_values = gaussian(streams_of[4], (SEQS, HEADS, SPAN, DV), 1.0, 6.0, ((0, 128), (1, 2)))
    cache_rates = jnp.clip(jnp.exp(math.log(0.3) - 5.0106353 * jax.random.uniform(streams_of[5], (SEQS, HEADS, SPAN, DK), jnp.float32) ** levels(streams_of[5], (SEQS, HEADS, SPAN, DK), ((0, 128), (1, 2)), -0.2, 0.2)), 0.002, 0.3)
    attn_gain = jnp.clip(1.0 + 0.18 * jax.random.normal(streams_of[6], (D,), jnp.float32), 0.099609375, 1.8984375).astype(jnp.bfloat16)
    w_query = gaussian(streams_of[7], (D, HEADS * DK), D ** -0.5, 0.09375, ((0, 32), (1, 2)))
    w_key = gaussian(streams_of[8], (D, HEADS * DK), D ** -0.5, 0.09375, ((0, 32), (1, 2)))
    w_value = gaussian(streams_of[9], (D, HEADS * DV), D ** -0.5, 0.09375, ((0, 32), (1, 2)))
    w_gate = gaussian(streams_of[10], (D, HEADS * DV), D ** -0.5, 0.09375, ((0, 32), (1, 2)))
    w_decay = gaussian(streams_of[11], (D, HEADS * DK), (D // 16) ** -0.5, 0.375, ((0, 32), (1, 2)))
    head_gain = jnp.clip(1.0 + 0.18 * jax.random.normal(streams_of[12], (HEADS, DV), jnp.float32), 0.099609375, 1.8984375).astype(jnp.bfloat16)
    w_out = gaussian(streams_of[13], (HEADS * DV, D), (HEADS * DV) ** -0.5, 0.109375, ((1, 64),))
    mlp_gain = jnp.clip(1.0 + 0.18 * jax.random.normal(streams_of[14], (D,), jnp.float32), 0.099609375, 1.8984375).astype(jnp.bfloat16)
    w_mlp_gate = gaussian(streams_of[15], (D, FF), D ** -0.5, 0.09375, ((1, 64),))
    w_mlp_up = gaussian(streams_of[16], (D, FF), D ** -0.5, 0.09375, ((1, 64),))
    w_mlp_down = bell_draw_with(streams_of[17], (FF, D), FF ** -0.5, 0.15625, ((0, 64),), (0, 1, 64, 4.0))
    return dict(tokens=tokens, lengths=lengths, state=state, cache_keys=cache_keys, cache_values=cache_values, cache_rates=cache_rates, attn_gain=attn_gain, w_query=w_query, w_key=w_key, w_value=w_value, w_gate=w_gate, w_decay=w_decay, head_gain=head_gain, w_out=w_out, mlp_gain=mlp_gain, w_mlp_gate=w_mlp_gate, w_mlp_up=w_mlp_up, w_mlp_down=w_mlp_down)


EPS = 1e-06
GATE_NORM = 16.0
exact_mode = lax.Precision.HIGHEST

def front_part(query, key_new, log_decay, state, cache_keys, cache_rates, lengths):
    span = cache_keys.shape[2]
    live = (jnp.arange(span, dtype=jnp.int32)[None, :] < lengths[:, None]).astype(jnp.float32)
    running = jnp.cumsum(cache_rates * live[:, None, :, None], axis=2)
    total = running[:, :, -1:, :]
    weight = jnp.exp(running - total + log_decay[:, :, None, :])
    scores = jnp.einsum('bhd,bhjd->bhj', query, weight * cache_keys.astype(jnp.float32), precision=exact_mode) * live[:, None, :]
    carried = jnp.einsum('bhd,bhde->bhe', query * jnp.exp(log_decay - total[:, :, 0, :]), state, precision=exact_mode)
    own = lax.optimization_barrier(jnp.sum(query * key_new, axis=-1, keepdims=True))
    return (scores, carried, own)

def back_part(scores, carried, own, value_new, cache_values, gate, head_gain):
    inner = jnp.einsum('bhj,bhje->bhe', scores, cache_values.astype(jnp.float32), precision=exact_mode)
    attended = carried + inner + own * value_new
    normed = attended * lax.rsqrt(lax.optimization_barrier(jnp.mean(attended * attended, axis=-1, keepdims=True)) + EPS)
    normed = normed * head_gain.astype(jnp.float32)
    return (jax.nn.silu(gate) * normed).astype(jnp.bfloat16)

def reference(tokens, lengths, state, cache_keys, cache_values, cache_rates, attn_gain, w_query, w_key, w_value, w_gate, w_decay, head_gain, w_out, mlp_gain, w_mlp_gate, w_mlp_up, w_mlp_down):
    seqs = tokens.shape[0]
    heads_all, key_dim, value_dim = (state.shape[1], state.shape[2], state.shape[3])
    wide = tokens.astype(jnp.float32)
    inv_rms = lax.rsqrt(lax.optimization_barrier(jnp.mean(wide * wide, axis=1, keepdims=True)) + EPS)
    scaled = (wide * attn_gain.astype(jnp.float32)).astype(jnp.bfloat16)

    def project(matrix):
        return jnp.dot(scaled, matrix, preferred_element_type=jnp.float32) * inv_rms
    query = (project(w_query) * key_dim ** (-0.5)).reshape(seqs, heads_all, key_dim)
    key_new = project(w_key).reshape(seqs, heads_all, key_dim)
    log_decay = (jax.nn.log_sigmoid(project(w_decay)) / GATE_NORM).reshape(seqs, heads_all, key_dim)
    value_new = project(w_value).reshape(seqs, heads_all, value_dim)
    gate = project(w_gate).reshape(seqs, heads_all, value_dim)
    scores, carried, own = front_part(query, key_new, log_decay, state, cache_keys, cache_rates, lengths)
    heads = back_part(scores, carried, own, value_new, cache_values, gate, head_gain)
    heads = heads.reshape(seqs, heads_all * value_dim)
    after = (wide + jnp.dot(heads, w_out, preferred_element_type=jnp.float32)).astype(jnp.bfloat16)
    second = after.astype(jnp.float32)
    inv_second = lax.rsqrt(lax.optimization_barrier(jnp.mean(second * second, axis=1, keepdims=True)) + EPS)
    normed = (second * inv_second * mlp_gain.astype(jnp.float32)).astype(jnp.bfloat16)
    gate_ff = jnp.dot(normed, w_mlp_gate, preferred_element_type=jnp.float32)
    up_ff = jnp.dot(normed, w_mlp_up, preferred_element_type=jnp.float32)
    hidden = (jax.nn.silu(gate_ff) * up_ff).astype(jnp.bfloat16)
    return (second + jnp.dot(hidden, w_mlp_down, preferred_element_type=jnp.float32)).astype(jnp.bfloat16)
```

```python
import functools

import jax
import jax.numpy as jnp
from jax import lax
from jax.experimental import pallas as pl
from jax.experimental.pallas import tpu as pltpu
from jax.sharding import PartitionSpec as P

EPS = 1e-06
GATE_NORM = 16.0
NX = 4
LANES = 128
MESH = pl.DeviceIdType.MESH
F32 = jnp.float32
BF16 = jnp.bfloat16


def dot(a, b, dims=((1,), (0,))):
    return lax.dot_general(a, b, (dims, ((), ())), preferred_element_type=F32)


def high_low(a):
    high = a.astype(BF16)
    return high, (a - high.astype(F32)).astype(BF16)


def kernel(
    sizes,
    tokens,
    lengths,
    state,
    cache_keys,
    cache_values,
    cache_rates,
    attn_gain,
    w_query,
    w_key,
    w_value,
    w_gate,
    w_decay,
    head_gain,
    w_out,
    mlp_gain,
    w_mlp_gate,
    w_mlp_up,
    w_mlp_down,
    out,
    tok,
    tokf,
    wq,
    wk,
    wd,
    wv,
    wg,
    st,
    ck,
    cv,
    cr,
    wo,
    wmg,
    wmu,
    wmd,
    x0,
    x1,
    ra0,
    ra1,
    rs0,
    rs1,
    rb0,
    rb1,
    zf,
    zs0,
    zs1,
    zr0,
    zr1,
    memory,
    pack0,
    pack1,
    qe,
    att,
    hg,
    headf,
    headb,
    headsf,
    lhs,
    whole,
    hidden,
    dpart,
    dpeer,
    dx,
    dra,
    drs,
    drb,
    dzs,
    dzr,
    outf,
    lsem,
    psem,
    xsem,
    zsem,
    hz,
    hx,
    hp,
    hr,
    az,
    ax,
    ap,
    ar,
    dsem,
    dzsem,
):
    nz, qb, vb, dk, width = sizes
    rows2 = 2 * nz
    kv = lax.axis_index("kv")
    c = lax.axis_index("tp")
    other = 1 - c
    z = kv // NX
    x = kv % NX
    xr = (x + 1) % NX
    xl = (x + NX - 1) % NX
    xo = (x + 2) % NX
    steps = [((d + 1) // 2) * (1 if d % 2 else -1) for d in range(1, nz)]
    far = [(z + (s % nz)) % nz for s in steps][::-1]
    near = [(z + (s % nz)) % nz for s in steps]
    sides = [(x + d) % NX for d in (2, 1, 3)]

    def local(i, src, dst):
        copy = pltpu.make_async_copy(src, dst, lsem.at[i])
        copy.start()
        return copy

    def remote(src, dst, send, recv, to_kv, to_tp):
        return pltpu.make_async_remote_copy(
            src_ref=src,
            dst_ref=dst,
            send_sem=send,
            recv_sem=recv,
            device_id={"kv": to_kv, "tp": to_tp},
            device_id_type=MESH,
        )

    sent = []

    def send(*args):
        copy = remote(*args)
        copy.start()
        sent.append(copy)

    in_tok = local(0, tokens, tok.at[c])
    in_w = [
        local(1 + i, src, dst)
        for i, (src, dst) in enumerate(
            ((w_query, wq), (w_key, wk), (w_decay, wd), (w_value, wv), (w_gate, wg))
        )
    ]
    in_cache = [
        local(6 + i, src, dst)
        for i, (src, dst) in enumerate(((cache_rates, cr), (cache_keys, ck), (cache_values, cv)))
    ]
    in_state = local(9, state, st)
    in_out = local(10, w_out, wo.at[c])
    in_mlp = [
        local(11 + i, src, dst)
        for i, (src, dst) in enumerate(((w_mlp_gate, wmg), (w_mlp_up, wmu), (w_mlp_down, wmd)))
    ]

    barrier = pltpu.get_barrier_semaphore()

    def greet(to_kv, to_tp):
        pl.semaphore_signal(
            barrier, inc=1, device_id={"kv": to_kv, "tp": to_tp}, device_id_type=MESH
        )

    for zp in far:
        greet(zp * NX + x, c)
        greet(zp * NX + x, other)
    for xp in sides:
        greet(z * NX + xp, c)
    greet(kv, other)
    zf[...] = jnp.zeros_like(zf)
    for h in range(2):
        for b in range(vb // 2):
            hg[h * (vb // 2) + b : h * (vb // 2) + b + 1, :] = head_gain[
                h : h + 1, b * LANES : (b + 1) * LANES
            ].astype(F32)
    pl.semaphore_wait(barrier, 2 * len(far) + len(sides) + 1)

    in_tok.wait()
    send(tok.at[c], tok.at[c], psem.at[0], psem.at[1], kv, other)
    in_out.wait()
    send(wo.at[c], wo.at[c], psem.at[2], psem.at[3], kv, other)
    remote(tok.at[other], tok.at[other], psem.at[0], psem.at[1], kv, other).wait_recv()
    tokf[...] = jnp.concatenate([tok[0].astype(F32), tok[1].astype(F32)], axis=1)
    block = jnp.concatenate(
        [
            tokf[pl.ds(2 * xp + i, nz, stride=2 * NX), :]
            for xp in range(NX)
            for i in range(2)
        ],
        axis=0,
    )
    squares = jnp.sum(block * block, axis=1, keepdims=True)
    scaled = (block * attn_gain[...].astype(F32)).astype(BF16)

    def put(target, b, values):
        half = target.shape[3] // LANES
        at = (b % half) * LANES
        for xp in range(NX):
            target[xp, b // half, :, at : at + LANES] = values[
                xp * rows2 : (xp + 1) * rows2
            ].astype(BF16)

    def project(copy, weight, target, start):
        copy.wait()
        part = dot(scaled, weight[...])
        for b in range(weight.shape[1] // LANES):
            put(target, start + b, part[:, b * LANES : (b + 1) * LANES])

    def x_first(src, first, back, sems, base):
        send(src.at[xo, 0], first.at[0], sems.at[0, base], sems.at[1, base], z * NX + xr, c)
        send(src.at[xo, 1], first.at[1], sems.at[0, base + 1], sems.at[1, base + 1], z * NX + xl, c)
        send(src.at[xr, 1], back.at[0, 1], sems.at[0, base + 2], sems.at[1, base + 2], z * NX + xr, c)
        send(src.at[xl, 0], back.at[1, 0], sems.at[0, base + 3], sems.at[1, base + 3], z * NX + xl, c)

    def x_second(src, first, relay, back, sems, base):
        remote(
            first.at[0], first.at[0], sems.at[0, base], sems.at[1, base], z * NX + xl, c
        ).wait_recv()
        relay[0] = (src[xr, 0].astype(F32) + first[0].astype(F32)).astype(BF16)
        send(relay.at[0], back.at[0, 0], sems.at[0, base + 4], sems.at[1, base + 4], z * NX + xr, c)
        remote(
            first.at[1], first.at[1], sems.at[0, base + 1], sems.at[1, base + 1], z * NX + xr, c
        ).wait_recv()
        relay[1] = (src[xl, 1].astype(F32) + first[1].astype(F32)).astype(BF16)
        send(relay.at[1], back.at[1, 1], sems.at[0, base + 5], sems.at[1, base + 5], z * NX + xl, c)

    def x_wait(back, sems, base, side, half):
        slot = {(0, 1): 2, (1, 0): 3, (0, 0): 4, (1, 1): 5}[(side, half)]
        remote(
            back.at[side, half],
            back.at[side, half],
            sems.at[0, base + slot],
            sems.at[1, base + slot],
            z * NX + (xr if side else xl),
            c,
        ).wait_recv()

    def x_sum(src, back, half):
        return src[x, half].astype(F32) + back[0, half].astype(F32) + back[1, half].astype(F32)

    project(in_w[0], wq, x0, 0)
    project(in_w[1], wk, x0, qb)
    project(in_w[2], wd, x0, 2 * qb)
    put(x0, 3 * qb, jnp.broadcast_to(squares, (squares.shape[0], LANES)))
    for b in range(3 * qb + 1, 2 * (x0.shape[3] // LANES)):
        put(x0, b, jnp.zeros((squares.shape[0], LANES), F32))
    x_first(x0, ra0, rb0, xsem, 0)
    project(in_w[3], wv, x1, 0)
    project(in_w[4], wg, x1, vb)
    x_first(x1, ra1, rb1, xsem, 6)

    span = ck.shape[2]
    hb = vb // 2
    later = (
        lax.broadcasted_iota(jnp.int32, (span, span), 1)
        > lax.broadcasted_iota(jnp.int32, (span, span), 0)
    ).astype(BF16)
    ones = jnp.ones((span, LANES), BF16)
    slots = lax.broadcasted_iota(jnp.int32, (span, 1), 0)

    def fold(i, h):
        live = (slots < lengths[i]).astype(F32)
        rates = cr[i, h] * live
        high, low = high_low(rates)
        rest = dot(later, high) + dot(later, low)
        keys = jnp.exp(-rest) * ck[i, h].astype(F32) * live
        shrink = jnp.exp(-(dot(high, ones, ((0,), (0,))) + dot(low, ones, ((0,), (0,)))))
        high, low = high_low(keys)
        value = cv[i, h]
        inner = dot(high, value, ((0,), (0,))) + dot(low, value, ((0,), (0,)))
        for b in range(hb):
            cols = slice(b * LANES, (b + 1) * LANES)
            memory[i, h, :, cols] = (st[i, h, :, cols] * shrink + inner[:, cols]).astype(BF16)

    for copy in in_cache:
        copy.wait()
    in_state.wait()
    x_second(x0, ra0, rs0, rb0, xsem, 0)
    x_second(x1, ra1, rs1, rb1, xsem, 6)

    slots_row = zf.shape[0] // rows2

    def z_send(src, back, packed, landing, base, sem_base):
        half = src.shape[3] // LANES
        for hh, side in ((1, 0), (0, 1), (0, 0), (1, 1)):
            x_wait(back, xsem, base, side, hh)
        for hh in (0, 1):
            total = x_sum(src, back, hh)
            for b in range(half):
                for i in range(2):
                    zf[pl.ds(i * slots_row + hh * half + b, nz, stride=2 * slots_row), :] = total[
                        i * nz : (i + 1) * nz, b * LANES : (b + 1) * LANES
                    ]
        for zp in range(nz):
            packed[zp] = zf[zp * 2 * slots_row : (zp + 1) * 2 * slots_row, :].astype(BF16)
        for k, zp in enumerate(far):
            send(
                packed.at[zp],
                landing.at[z],
                zsem.at[0, sem_base + k],
                zsem.at[1, sem_base + z],
                zp * NX + x,
                c,
            )

    def z_sum(packed, landing, sem_base):
        for zp in near:
            remote(
                landing.at[zp],
                landing.at[zp],
                zsem.at[0, sem_base],
                zsem.at[1, sem_base + zp],
                zp * NX + x,
                c,
            ).wait_recv()
        total = packed[z].astype(F32)
        for zp in near:
            total = total + landing[zp].astype(F32)
        return total

    z_send(x0, rb0, zs0, zr0, 0, 0)
    z_send(x1, rb1, zs1, zr1, 6, nz)
    for i in range(2):
        for h in range(2):
            fold(i, h)

    pack0[...] = z_sum(zs0, zr0, 0)
    own = []
    inverse = []
    qh = qb // 2
    for i in range(2):
        at = i * slots_row
        inv = lax.rsqrt(pack0[at + 3 * qb : at + 3 * qb + 1, :] * (1.0 / width) + EPS)
        inverse.append(inv)
        query = pack0[at : at + qb, :] * inv * dk ** (-0.5)
        key = pack0[at + qb : at + 2 * qb, :] * inv
        raw = pack0[at + 2 * qb : at + 3 * qb, :] * inv
        decay = (jnp.minimum(raw, 0.0) - jnp.log1p(jnp.exp(-jnp.abs(raw)))) / GATE_NORM
        qe[i * qb : (i + 1) * qb, :] = query * jnp.exp(decay)
        both = query * key
        for h in range(2):
            part = jnp.sum(both[h * qh : (h + 1) * qh, :], axis=0, keepdims=True)
            own.append(jnp.sum(part, axis=1, keepdims=True))
    for i in range(2):
        for h in range(2):
            row = jnp.concatenate(
                [qe[i * qb + h * qh + b : i * qb + h * qh + b + 1, :] for b in range(qh)], axis=1
            )
            high, low = high_low(row)
            got = dot(jnp.concatenate([high, low], axis=0), memory[i, h])
            got = got[0:1] + got[1:2]
            for b in range(hb):
                att[i * vb + h * hb + b : i * vb + h * hb + b + 1, :] = got[
                    :, b * LANES : (b + 1) * LANES
                ]
    pack1[...] = z_sum(zs1, zr1, nz)
    for i in range(2):
        at = i * slots_row
        value = pack1[at : at + vb, :] * inverse[i]
        gate = pack1[at + vb : at + 2 * vb, :] * inverse[i]
        attended = att[i * vb : (i + 1) * vb, :]
        for h in range(2):
            part = slice(h * hb, (h + 1) * hb)
            full = attended[part] + own[2 * i + h] * value[part]
            mean = jnp.sum(jnp.sum(full * full, axis=0, keepdims=True), axis=1, keepdims=True)
            norm = full * lax.rsqrt(mean * (1.0 / (hb * LANES)) + EPS) * hg[part, :]
            g = gate[part]
            headf[i * (headf.shape[0] // 2) + h * hb : i * (headf.shape[0] // 2) + (h + 1) * hb, :] = (
                g / (1.0 + jnp.exp(-g)) * norm
            )
    headb[kv, c] = headf[...].astype(BF16)

    def gather(buf, zs, xs, ps, rs, with_partner):
        mine = buf.at[kv, c]
        for k, zp in enumerate(far):
            send(mine, mine, zs.at[k], rs.at[kv, c], zp * NX + x, c)
        for k, xp in enumerate(sides):
            send(mine, mine, xs.at[z, k], rs.at[kv, c], z * NX + xp, c)
        if with_partner:
            send(mine, mine, ps.at[kv], rs.at[kv, c], kv, other)
        for zp in near:
            origin = zp * NX + x
            slot = buf.at[origin, c]
            remote(slot, slot, zs.at[0], rs.at[origin, c], origin, c).wait_recv()
            for k, xp in enumerate(sides):
                send(slot, slot, xs.at[zp, k], rs.at[origin, c], z * NX + xp, c)
            send(slot, slot, ps.at[origin], rs.at[origin, c], kv, other)
        for zp in [z] + near:
            for xp in sides[::-1]:
                origin = zp * NX + xp
                slot = buf.at[origin, c]
                remote(slot, slot, zs.at[0], rs.at[origin, c], z * NX + xp, c).wait_recv()
                send(slot, slot, ps.at[origin], rs.at[origin, c], kv, other)
        for zp in [z] + near:
            for xp in [x] + sides[::-1]:
                if zp is z and xp is x and not with_partner:
                    continue
                origin = zp * NX + xp
                slot = buf.at[origin, other]
                remote(slot, slot, zs.at[0], rs.at[origin, other], kv, other).wait_recv()

    gather(headb, hz, hx, hp, hr, True)

    n_kv = nz * NX
    hrows = headf.shape[0]
    headsf[...] = headb[...].astype(F32).reshape(headsf.shape)
    for cc in range(2):
        for b in range(vb):
            at = (cc * vb + b) * LANES
            for i in range(2):
                lhs[i * n_kv : (i + 1) * n_kv, at : at + LANES] = headsf[
                    pl.ds(cc * hrows + i * (hrows // 2) + b, n_kv, stride=2 * hrows), :
                ].astype(BF16)
    remote(wo.at[other], wo.at[other], psem.at[2], psem.at[3], kv, other).wait_recv()
    heads = lhs[:, : 2 * vb * LANES]
    projected = jnp.concatenate([dot(heads, wo[0]), dot(heads, wo[1])], axis=1)
    for i in range(2):
        old = tokf[pl.ds(i, n_kv, stride=2), :]
        whole[kv, i] = (old + projected[i * n_kv : (i + 1) * n_kv]).astype(BF16)

    gather(whole, az, ax, ap, ar, False)

    energy = jnp.zeros((2 * n_kv, LANES), F32)
    for k in range(n_kv):
        rows = jnp.concatenate([whole[k, 0], whole[k, 1]], axis=0).astype(F32)
        energy = energy + rows * rows
        cols = slice(k * LANES, (k + 1) * LANES)
        lhs[:, cols] = (rows * mlp_gain[:, cols].astype(F32)).astype(BF16)
    inv = lax.rsqrt(jnp.sum(energy, axis=1, keepdims=True) * (1.0 / width) + EPS)
    in_mlp[0].wait()
    gate = dot(lhs[:, :width], wmg[...]) * inv
    in_mlp[1].wait()
    up = dot(lhs[:, :width], wmu[...]) * inv
    hidden[...] = (gate / (1.0 + jnp.exp(-gate)) * up).astype(BF16)
    in_mlp[2].wait()
    hz_half = nz // 2
    for zh in range(2):
        for zi in range(hz_half):
            zp = zh * hz_half + zi
            part = dot(hidden[...], wmd[:, zp * NX * LANES : (zp + 1) * NX * LANES]).astype(BF16)
            for xp in range(NX):
                for i in range(2):
                    dpart[i, zh, xp, :, zi * LANES : (zi + 1) * LANES] = part[
                        i * n_kv : (i + 1) * n_kv, xp * LANES : (xp + 1) * LANES
                    ]
        send(dpart.at[other, zh], dpeer.at[zh], psem.at[4 + zh], psem.at[6 + zh], kv, other)
    for zh in range(2):
        remote(
            dpeer.at[zh], dpeer.at[zh], psem.at[4 + zh], psem.at[6 + zh], kv, other
        ).wait_recv()
        for xp in (xo, xr, xl, x):
            dx[xp, zh] = (dpart[c, zh, xp].astype(F32) + dpeer[zh, xp].astype(F32)).astype(BF16)
    x_first(dx, dra, drb, dsem, 0)
    x_second(dx, dra, drs, drb, dsem, 0)
    low_lanes = lax.broadcasted_iota(jnp.int32, (n_kv // 2, LANES), 1) < LANES // 2

    def squeeze(rows, right):
        top, bottom = rows[: n_kv // 2], rows[n_kv // 2 :]
        if right:
            top = pltpu.roll(top, LANES // 2, 1)
        else:
            bottom = pltpu.roll(bottom, LANES // 2, 1)
        return jnp.where(low_lanes, top, bottom)

    for hh, side in ((1, 0), (0, 1), (0, 0), (1, 1)):
        x_wait(drb, dsem, 0, side, hh)
    for zh in range(2):
        total = x_sum(dx, drb, zh)
        for zi in range(hz_half):
            rows = total[:, zi * LANES : (zi + 1) * LANES]
            for cc in range(2):
                dzs[zh * hz_half + zi, cc] = squeeze(rows, cc == 1).astype(BF16)
    for k, zp in enumerate(far):
        for q, cc in enumerate((other, c)):
            send(
                dzs.at[zp, cc],
                dzr.at[z, c],
                dzsem.at[0, k, q],
                dzsem.at[1, z, c],
                zp * NX + x,
                cc,
            )
    send(dzs.at[z, other], dzr.at[z, c], dzsem.at[0, nz - 1, 0], dzsem.at[1, z, c], kv, other)
    dzr[z, c] = dzs[z, c]
    for zp in [z] + near:
        for cc in (c, other):
            if zp is z and cc is c:
                continue
            slot = dzr.at[zp, cc]
            remote(
                slot, slot, dzsem.at[0, 0, 0], dzsem.at[1, zp, cc], zp * NX + x, cc
            ).wait_recv()
    for i in range(2):
        rows = whole[kv, i].astype(F32)
        total = jnp.where(c == 1, squeeze(rows, True), squeeze(rows, False))
        for zp in range(nz):
            total = total + dzr[zp, i].astype(F32)
        outf[pl.ds(i, n_kv // 2, stride=2), :] = total
        outf[pl.ds(i + n_kv, n_kv // 2, stride=2), :] = pltpu.roll(total, LANES // 2, 1)
    out[...] = outf[:, : LANES // 2].astype(BF16)
    for copy in sent:
        copy.wait_send()


def shards(
    tokens,
    lengths,
    state,
    cache_keys,
    cache_values,
    cache_rates,
    attn_gain,
    w_query,
    w_key,
    w_value,
    w_gate,
    w_decay,
    head_gain,
    w_out,
    mlp_gain,
    w_mlp_gate,
    w_mlp_up,
    w_mlp_down,
):
    n_kv = lax.axis_size("kv")
    nz = n_kv // NX
    heads, dk, dv = state.shape[1], state.shape[2], state.shape[3]
    width = mlp_gain.shape[0]
    qb, vb = heads * dk // LANES, heads * dv // LANES
    half0, half1 = (3 * qb + 2) // 2, vb
    slots = -(-2 * max(half0, half1) // 8) * 8
    rows2 = 2 * nz
    seqs = 2 * n_kv
    hrows = 2 * (-(-vb // 8) * 8)
    units = w_mlp_down.shape[0]
    cols5 = nz // 2 * LANES
    vmem, dma = pltpu.VMEM, pltpu.SemaphoreType.DMA
    bf, fl = BF16, F32
    scratch = [
        vmem((2, seqs, LANES // 2), bf),
        vmem((seqs, LANES), fl),
        vmem(w_query.shape, bf),
        vmem(w_key.shape, bf),
        vmem(w_decay.shape, bf),
        vmem(w_value.shape, bf),
        vmem(w_gate.shape, bf),
        vmem(state.shape, fl),
        vmem(cache_keys.shape, bf),
        vmem(cache_values.shape, bf),
        vmem(cache_rates.shape, fl),
        vmem((2,) + w_out.shape, bf),
        vmem(w_mlp_gate.shape, bf),
        vmem(w_mlp_up.shape, bf),
        vmem(w_mlp_down.shape, bf),
        vmem((NX, 2, rows2, half0 * LANES), bf),
        vmem((NX, 2, rows2, half1 * LANES), bf),
        vmem((2, rows2, half0 * LANES), bf),
        vmem((2, rows2, half1 * LANES), bf),
        vmem((2, rows2, half0 * LANES), bf),
        vmem((2, rows2, half1 * LANES), bf),
        vmem((2, 2, rows2, half0 * LANES), bf),
        vmem((2, 2, rows2, half1 * LANES), bf),
        vmem((rows2 * slots, LANES), fl),
        vmem((nz, 2 * slots, LANES), bf),
        vmem((nz, 2 * slots, LANES), bf),
        vmem((nz, 2 * slots, LANES), bf),
        vmem((nz, 2 * slots, LANES), bf),
        vmem(state.shape, bf),
        vmem((2 * slots, LANES), fl),
        vmem((2 * slots, LANES), fl),
        vmem((2 * qb, LANES), fl),
        vmem((2 * vb, LANES), fl),
        vmem((vb, LANES), fl),
        vmem((hrows, LANES), fl),
        vmem((n_kv, 2, hrows, LANES), bf),
        vmem((n_kv * 2 * hrows, LANES), fl),
        vmem((seqs, max(width, 2 * vb * LANES)), bf),
        vmem((n_kv, 2, n_kv, LANES), bf),
        vmem((seqs, units), bf),
        vmem((2, 2, NX, n_kv, cols5), bf),
        vmem((2, NX, n_kv, cols5), bf),
        vmem((NX, 2, n_kv, cols5), bf),
        vmem((2, n_kv, cols5), bf),
        vmem((2, n_kv, cols5), bf),
        vmem((2, 2, n_kv, cols5), bf),
        vmem((nz, 2, n_kv // 2, LANES), bf),
        vmem((nz, 2, n_kv // 2, LANES), bf),
        vmem((seqs, LANES), fl),
        dma((14,)),
        dma((8,)),
        dma((2, 12)),
        dma((2, 2 * nz)),
        dma((nz,)),
        dma((nz, NX)),
        dma((n_kv,)),
        dma((n_kv, 2)),
        dma((nz,)),
        dma((nz, NX)),
        dma((n_kv,)),
        dma((n_kv, 2)),
        dma((2, 6)),
        dma((2, nz, 2)),
    ]
    anywhere = pl.BlockSpec(memory_space=pl.ANY)
    in_vmem = pl.BlockSpec(memory_space=pltpu.VMEM)
    in_smem = pl.BlockSpec(memory_space=pltpu.SMEM)
    specs = [anywhere] * 18
    specs[1] = in_smem
    for k in (6, 12, 14):
        specs[k] = in_vmem
    return pl.pallas_call(
        functools.partial(kernel, (nz, qb, vb, dk, width)),
        out_shape=jax.ShapeDtypeStruct(tokens.shape, BF16),
        in_specs=specs,
        out_specs=in_vmem,
        scratch_shapes=scratch,
        compiler_params=pltpu.CompilerParams(collective_id=0, has_side_effects=True),
        name="layer",
    )(
        tokens,
        lengths,
        state,
        cache_keys,
        cache_values,
        cache_rates,
        attn_gain.reshape(1, -1),
        w_query,
        w_key,
        w_value,
        w_gate,
        w_decay,
        head_gain,
        w_out,
        mlp_gain.reshape(1, -1),
        w_mlp_gate,
        w_mlp_up,
        w_mlp_down,
    )


def solution(mesh):
    placed = (
        P("dp", ("kv", "tp")),
        P(("dp", "kv")),
        P(("dp", "kv"), "tp", None, None),
        P(("dp", "kv"), "tp", None, None),
        P(("dp", "kv"), "tp", None, None),
        P(("dp", "kv"), "tp", None, None),
        P("kv"),
        P("kv", "tp"),
        P("kv", "tp"),
        P("kv", "tp"),
        P("kv", "tp"),
        P("kv", "tp"),
        P("tp", None),
        P(None, ("kv", "tp")),
        P(),
        P(None, ("kv", "tp")),
        P(None, ("kv", "tp")),
        P(("kv", "tp"), None),
    )
    return jax.shard_map(
        shards, mesh=mesh, in_specs=placed, out_specs=P("dp", ("kv", "tp")), check_vma=False
    )
```

```python
import functools

import jax
import jax.numpy as jnp
from jax import lax
from jax.experimental import pallas as pl
from jax.experimental.pallas import tpu as pltpu
from jax.sharding import PartitionSpec as P

EPS = 1e-06
GATE_NORM = 16.0
NX = 4
LANES = 128
MESH = pl.DeviceIdType.MESH
F32 = jnp.float32
BF16 = jnp.bfloat16


def dot(a, b, dims=((1,), (0,))):
    return lax.dot_general(a, b, (dims, ((), ())), preferred_element_type=F32)


def high_low(a):
    high = a.astype(BF16)
    return high, (a - high.astype(F32)).astype(BF16)


def kernel(
    sizes,
    tokens,
    lengths,
    state,
    cache_keys,
    cache_values,
    cache_rates,
    attn_gain,
    w_query,
    w_key,
    w_value,
    w_gate,
    w_decay,
    head_gain,
    w_out,
    mlp_gain,
    w_mlp_gate,
    w_mlp_up,
    w_mlp_down,
    out,
    tok,
    tokf,
    wq,
    wk,
    wd,
    wv,
    wg,
    st,
    ck,
    cv,
    cr,
    wo,
    wmg,
    wmu,
    wmd,
    x0,
    x1,
    ra0,
    ra1,
    rs0,
    rs1,
    rb0,
    rb1,
    zf,
    zs0,
    zs1,
    zr0,
    zr1,
    memory,
    pack0,
    pack1,
    qe,
    att,
    hg,
    headf,
    headb,
    headsf,
    lhs,
    whole,
    hidden,
    dpart,
    dpeer,
    dx,
    dra,
    drs,
    drb,
    dzs,
    dzr,
    outf,
    lsem,
    psem,
    xsem,
    zsem,
    hz,
    hx,
    hp,
    hr,
    az,
    ax,
    ap,
    ar,
    dsem,
    dzsem,
):
    nz, qb, vb, dk, width = sizes
    rows2 = 2 * nz
    kv = lax.axis_index("kv")
    c = lax.axis_index("tp")
    other = 1 - c
    z = kv // NX
    x = kv % NX
    xr = (x + 1) % NX
    xl = (x + NX - 1) % NX
    xo = (x + 2) % NX
    steps = [((d + 1) // 2) * (1 if d % 2 else -1) for d in range(1, nz)]
    far = [(z + (s % nz)) % nz for s in steps][::-1]
    near = [(z + (s % nz)) % nz for s in steps]
    sides = [(x + d) % NX for d in (2, 1, 3)]

    def local(i, src, dst):
        copy = pltpu.make_async_copy(src, dst, lsem.at[i])
        copy.start()
        return copy

    def remote(src, dst, send, recv, to_kv, to_tp):
        return pltpu.make_async_remote_copy(
            src_ref=src,
            dst_ref=dst,
            send_sem=send,
            recv_sem=recv,
            device_id={"kv": to_kv, "tp": to_tp},
            device_id_type=MESH,
        )

    scopes = []

    def mark(name=None):
        if scopes:
            scopes.pop().__exit__(None, None, None)
        if name:
            scopes.append(jax.named_scope(name))
            scopes[-1].__enter__()

    sent = []

    def send(*args):
        copy = remote(*args)
        copy.start()
        sent.append(copy)

    mark("load")
    in_tok = local(0, tokens, tok.at[c])
    in_w = [
        local(1 + i, src, dst)
        for i, (src, dst) in enumerate(
            ((w_query, wq), (w_key, wk), (w_decay, wd), (w_value, wv), (w_gate, wg))
        )
    ]
    in_cache = [
        local(6 + i, src, dst)
        for i, (src, dst) in enumerate(((cache_rates, cr), (cache_keys, ck), (cache_values, cv)))
    ]
    in_state = local(9, state, st)
    in_out = local(10, w_out, wo.at[c])
    in_mlp = [
        local(11 + i, src, dst)
        for i, (src, dst) in enumerate(((w_mlp_gate, wmg), (w_mlp_up, wmu), (w_mlp_down, wmd)))
    ]

    mark("barrier")
    barrier = pltpu.get_barrier_semaphore()

    def greet(to_kv, to_tp):
        pl.semaphore_signal(
            barrier, inc=1, device_id={"kv": to_kv, "tp": to_tp}, device_id_type=MESH
        )

    for zp in far:
        greet(zp * NX + x, c)
        greet(zp * NX + x, other)
    for xp in sides:
        greet(z * NX + xp, c)
    greet(kv, other)
    zf[...] = jnp.zeros_like(zf)
    for h in range(2):
        for b in range(vb // 2):
            hg[h * (vb // 2) + b : h * (vb // 2) + b + 1, :] = head_gain[
                h : h + 1, b * LANES : (b + 1) * LANES
            ].astype(F32)
    pl.semaphore_wait(barrier, 2 * len(far) + len(sides) + 1)

    mark("tokens")
    in_tok.wait()
    send(tok.at[c], tok.at[c], psem.at[0], psem.at[1], kv, other)
    in_out.wait()
    send(wo.at[c], wo.at[c], psem.at[2], psem.at[3], kv, other)
    remote(tok.at[other], tok.at[other], psem.at[0], psem.at[1], kv, other).wait_recv()
    tokf[...] = jnp.concatenate([tok[0].astype(F32), tok[1].astype(F32)], axis=1)
    block = jnp.concatenate(
        [
            tokf[pl.ds(2 * xp + i, nz, stride=2 * NX), :]
            for xp in range(NX)
            for i in range(2)
        ],
        axis=0,
    )
    squares = jnp.sum(block * block, axis=1, keepdims=True)
    scaled = (block * attn_gain[...].astype(F32)).astype(BF16)

    def put(target, b, values):
        half = target.shape[3] // LANES
        at = (b % half) * LANES
        for xp in range(NX):
            target[xp, b // half, :, at : at + LANES] = values[
                xp * rows2 : (xp + 1) * rows2
            ].astype(BF16)

    def project(copy, weight, target, start):
        copy.wait()
        part = dot(scaled, weight[...])
        for b in range(weight.shape[1] // LANES):
            put(target, start + b, part[:, b * LANES : (b + 1) * LANES])

    def x_first(src, first, back, sems, base):
        send(src.at[xo, 0], first.at[0], sems.at[0, base], sems.at[1, base], z * NX + xr, c)
        send(src.at[xo, 1], first.at[1], sems.at[0, base + 1], sems.at[1, base + 1], z * NX + xl, c)
        send(src.at[xr, 1], back.at[0, 1], sems.at[0, base + 2], sems.at[1, base + 2], z * NX + xr, c)
        send(src.at[xl, 0], back.at[1, 0], sems.at[0, base + 3], sems.at[1, base + 3], z * NX + xl, c)

    def x_second(src, first, relay, back, sems, base):
        remote(
            first.at[0], first.at[0], sems.at[0, base], sems.at[1, base], z * NX + xl, c
        ).wait_recv()
        relay[0] = (src[xr, 0].astype(F32) + first[0].astype(F32)).astype(BF16)
        send(relay.at[0], back.at[0, 0], sems.at[0, base + 4], sems.at[1, base + 4], z * NX + xr, c)
        remote(
            first.at[1], first.at[1], sems.at[0, base + 1], sems.at[1, base + 1], z * NX + xr, c
        ).wait_recv()
        relay[1] = (src[xl, 1].astype(F32) + first[1].astype(F32)).astype(BF16)
        send(relay.at[1], back.at[1, 1], sems.at[0, base + 5], sems.at[1, base + 5], z * NX + xl, c)

    def x_wait(back, sems, base, side, half):
        slot = {(0, 1): 2, (1, 0): 3, (0, 0): 4, (1, 1): 5}[(side, half)]
        remote(
            back.at[side, half],
            back.at[side, half],
            sems.at[0, base + slot],
            sems.at[1, base + slot],
            z * NX + (xr if side else xl),
            c,
        ).wait_recv()

    def x_sum(src, back, half):
        return src[x, half].astype(F32) + back[0, half].astype(F32) + back[1, half].astype(F32)

    mark("project_a")
    project(in_w[0], wq, x0, 0)
    project(in_w[1], wk, x0, qb)
    project(in_w[2], wd, x0, 2 * qb)
    put(x0, 3 * qb, jnp.broadcast_to(squares, (squares.shape[0], LANES)))
    for b in range(3 * qb + 1, 2 * (x0.shape[3] // LANES)):
        put(x0, b, jnp.zeros((squares.shape[0], LANES), F32))
    x_first(x0, ra0, rb0, xsem, 0)
    mark("project_b")
    project(in_w[3], wv, x1, 0)
    project(in_w[4], wg, x1, vb)
    x_first(x1, ra1, rb1, xsem, 6)

    span = ck.shape[2]
    hb = vb // 2
    later = (
        lax.broadcasted_iota(jnp.int32, (span, span), 1)
        > lax.broadcasted_iota(jnp.int32, (span, span), 0)
    ).astype(BF16)
    ones = jnp.ones((span, LANES), BF16)
    slots = lax.broadcasted_iota(jnp.int32, (span, 1), 0)

    def fold(i, h):
        live = (slots < lengths[i]).astype(F32)
        rates = cr[i, h] * live
        high, low = high_low(rates)
        rest = dot(later, high) + dot(later, low)
        keys = jnp.exp(-rest) * ck[i, h].astype(F32) * live
        shrink = jnp.exp(-(dot(high, ones, ((0,), (0,))) + dot(low, ones, ((0,), (0,)))))
        high, low = high_low(keys)
        value = cv[i, h]
        inner = dot(high, value, ((0,), (0,))) + dot(low, value, ((0,), (0,)))
        for b in range(hb):
            cols = slice(b * LANES, (b + 1) * LANES)
            memory[i, h, :, cols] = (st[i, h, :, cols] * shrink + inner[:, cols]).astype(BF16)

    mark("x_second")
    for copy in in_cache:
        copy.wait()
    in_state.wait()
    x_second(x0, ra0, rs0, rb0, xsem, 0)
    x_second(x1, ra1, rs1, rb1, xsem, 6)

    slots_row = zf.shape[0] // rows2

    def z_send(src, back, packed, landing, base, sem_base):
        half = src.shape[3] // LANES
        for hh, side in ((1, 0), (0, 1), (0, 0), (1, 1)):
            x_wait(back, xsem, base, side, hh)
        for hh in (0, 1):
            total = x_sum(src, back, hh)
            for b in range(half):
                for i in range(2):
                    zf[pl.ds(i * slots_row + hh * half + b, nz, stride=2 * slots_row), :] = total[
                        i * nz : (i + 1) * nz, b * LANES : (b + 1) * LANES
                    ]
        for zp in range(nz):
            packed[zp] = zf[zp * 2 * slots_row : (zp + 1) * 2 * slots_row, :].astype(BF16)
        for k, zp in enumerate(far):
            send(
                packed.at[zp],
                landing.at[z],
                zsem.at[0, sem_base + k],
                zsem.at[1, sem_base + z],
                zp * NX + x,
                c,
            )

    def z_sum(packed, landing, sem_base):
        for zp in near:
            remote(
                landing.at[zp],
                landing.at[zp],
                zsem.at[0, sem_base],
                zsem.at[1, sem_base + zp],
                zp * NX + x,
                c,
            ).wait_recv()
        total = packed[z].astype(F32)
        for zp in near:
            total = total + landing[zp].astype(F32)
        return total

    mark("z_send_a")
    z_send(x0, rb0, zs0, zr0, 0, 0)
    mark("z_send_b")
    z_send(x1, rb1, zs1, zr1, 6, nz)
    mark("fold")
    for i in range(2):
        for h in range(2):
            fold(i, h)

    mark("z_wait_a")
    pack0[...] = z_sum(zs0, zr0, 0)
    mark("heads_a")
    own = []
    inverse = []
    qh = qb // 2
    for i in range(2):
        at = i * slots_row
        inv = lax.rsqrt(pack0[at + 3 * qb : at + 3 * qb + 1, :] * (1.0 / width) + EPS)
        inverse.append(inv)
        query = pack0[at : at + qb, :] * inv * dk ** (-0.5)
        key = pack0[at + qb : at + 2 * qb, :] * inv
        raw = pack0[at + 2 * qb : at + 3 * qb, :] * inv
        decay = (jnp.minimum(raw, 0.0) - jnp.log1p(jnp.exp(-jnp.abs(raw)))) / GATE_NORM
        qe[i * qb : (i + 1) * qb, :] = query * jnp.exp(decay)
        both = query * key
        for h in range(2):
            part = jnp.sum(both[h * qh : (h + 1) * qh, :], axis=0, keepdims=True)
            own.append(jnp.sum(part, axis=1, keepdims=True))
    for i in range(2):
        for h in range(2):
            row = jnp.concatenate(
                [qe[i * qb + h * qh + b : i * qb + h * qh + b + 1, :] for b in range(qh)], axis=1
            )
            high, low = high_low(row)
            got = dot(jnp.concatenate([high, low], axis=0), memory[i, h])
            got = got[0:1] + got[1:2]
            for b in range(hb):
                att[i * vb + h * hb + b : i * vb + h * hb + b + 1, :] = got[
                    :, b * LANES : (b + 1) * LANES
                ]
    mark("z_wait_b")
    pack1[...] = z_sum(zs1, zr1, nz)
    for i in range(2):
        at = i * slots_row
        if i == 0:
            mark("heads_b")
        value = pack1[at : at + vb, :] * inverse[i]
        gate = pack1[at + vb : at + 2 * vb, :] * inverse[i]
        attended = att[i * vb : (i + 1) * vb, :]
        for h in range(2):
            part = slice(h * hb, (h + 1) * hb)
            full = attended[part] + own[2 * i + h] * value[part]
            mean = jnp.sum(jnp.sum(full * full, axis=0, keepdims=True), axis=1, keepdims=True)
            norm = full * lax.rsqrt(mean * (1.0 / (hb * LANES)) + EPS) * hg[part, :]
            g = gate[part]
            headf[i * (headf.shape[0] // 2) + h * hb : i * (headf.shape[0] // 2) + (h + 1) * hb, :] = (
                g / (1.0 + jnp.exp(-g)) * norm
            )
    headb[kv, c] = headf[...].astype(BF16)

    def gather(buf, zs, xs, ps, rs, with_partner):
        mine = buf.at[kv, c]
        for k, zp in enumerate(far):
            send(mine, mine, zs.at[k], rs.at[kv, c], zp * NX + x, c)
        for k, xp in enumerate(sides):
            send(mine, mine, xs.at[z, k], rs.at[kv, c], z * NX + xp, c)
        if with_partner:
            send(mine, mine, ps.at[kv], rs.at[kv, c], kv, other)
        for zp in near:
            origin = zp * NX + x
            slot = buf.at[origin, c]
            remote(slot, slot, zs.at[0], rs.at[origin, c], origin, c).wait_recv()
            for k, xp in enumerate(sides):
                send(slot, slot, xs.at[zp, k], rs.at[origin, c], z * NX + xp, c)
            send(slot, slot, ps.at[origin], rs.at[origin, c], kv, other)
        for zp in [z] + near:
            for xp in sides[::-1]:
                origin = zp * NX + xp
                slot = buf.at[origin, c]
                remote(slot, slot, zs.at[0], rs.at[origin, c], z * NX + xp, c).wait_recv()
                send(slot, slot, ps.at[origin], rs.at[origin, c], kv, other)
        for zp in [z] + near:
            for xp in [x] + sides[::-1]:
                if zp is z and xp is x and not with_partner:
                    continue
                origin = zp * NX + xp
                slot = buf.at[origin, other]
                remote(slot, slot, zs.at[0], rs.at[origin, other], kv, other).wait_recv()

    mark("gather_heads")
    gather(headb, hz, hx, hp, hr, True)

    mark("project_out")
    n_kv = nz * NX
    hrows = headf.shape[0]
    headsf[...] = headb[...].astype(F32).reshape(headsf.shape)
    for cc in range(2):
        for b in range(vb):
            at = (cc * vb + b) * LANES
            for i in range(2):
                lhs[i * n_kv : (i + 1) * n_kv, at : at + LANES] = headsf[
                    pl.ds(cc * hrows + i * (hrows // 2) + b, n_kv, stride=2 * hrows), :
                ].astype(BF16)
    remote(wo.at[other], wo.at[other], psem.at[2], psem.at[3], kv, other).wait_recv()
    heads = lhs[:, : 2 * vb * LANES]
    projected = dot(heads, wo[...].reshape(LANES, 2 * vb * LANES), ((1,), (1,)))
    for i in range(2):
        old = tokf[pl.ds(i, n_kv, stride=2), :]
        whole[kv, i] = (old + projected[i * n_kv : (i + 1) * n_kv]).astype(BF16)

    mark("gather_after")
    gather(whole, az, ax, ap, ar, False)

    mark("mlp_in")
    energy = jnp.zeros((2 * n_kv, LANES), F32)
    for k in range(n_kv):
        rows = jnp.concatenate([whole[k, 0], whole[k, 1]], axis=0).astype(F32)
        energy = energy + rows * rows
        cols = slice(k * LANES, (k + 1) * LANES)
        lhs[:, cols] = (rows * mlp_gain[k : k + 1, :].astype(F32)).astype(BF16)
    inv = lax.rsqrt(jnp.sum(energy, axis=1, keepdims=True) * (1.0 / width) + EPS)
    in_mlp[0].wait()
    gate = dot(lhs[:, :width], wmg[...], ((1,), (1,))) * inv
    in_mlp[1].wait()
    up = dot(lhs[:, :width], wmu[...], ((1,), (1,))) * inv
    hidden[...] = (gate / (1.0 + jnp.exp(-gate)) * up).astype(BF16)
    mark("mlp_down")
    in_mlp[2].wait()
    hz_half = nz // 2
    for zh in range(2):
        for zi in range(hz_half):
            zp = zh * hz_half + zi
            part = dot(hidden[...], wmd[:, zp * NX * LANES : (zp + 1) * NX * LANES]).astype(BF16)
            for xp in range(NX):
                for i in range(2):
                    dpart[i, zh, xp, :, zi * LANES : (zi + 1) * LANES] = part[
                        i * n_kv : (i + 1) * n_kv, xp * LANES : (xp + 1) * LANES
                    ]
        send(dpart.at[other, zh], dpeer.at[zh], psem.at[4 + zh], psem.at[6 + zh], kv, other)
    mark("down_peer")
    for zh in range(2):
        remote(
            dpeer.at[zh], dpeer.at[zh], psem.at[4 + zh], psem.at[6 + zh], kv, other
        ).wait_recv()
        for xp in (xo, xr, xl, x):
            dx[xp, zh] = (dpart[c, zh, xp].astype(F32) + dpeer[zh, xp].astype(F32)).astype(BF16)
    mark("down_x")
    x_first(dx, dra, drb, dsem, 0)
    x_second(dx, dra, drs, drb, dsem, 0)
    low_lanes = lax.broadcasted_iota(jnp.int32, (n_kv // 2, LANES), 1) < LANES // 2

    def squeeze(rows, right):
        top, bottom = rows[: n_kv // 2], rows[n_kv // 2 :]
        if right:
            top = pltpu.roll(top, LANES // 2, 1)
        else:
            bottom = pltpu.roll(bottom, LANES // 2, 1)
        return jnp.where(low_lanes, top, bottom)

    mark("down_x2")
    for hh, side in ((1, 0), (0, 1), (0, 0), (1, 1)):
        x_wait(drb, dsem, 0, side, hh)
    mark("down_pack")
    for zh in range(2):
        total = x_sum(dx, drb, zh)
        for zi in range(hz_half):
            rows = total[:, zi * LANES : (zi + 1) * LANES]
            for cc in range(2):
                dzs[zh * hz_half + zi, cc] = squeeze(rows, cc == 1).astype(BF16)
    for k, zp in enumerate(far):
        for q, cc in enumerate((other, c)):
            send(
                dzs.at[zp, cc],
                dzr.at[z, c],
                dzsem.at[0, k, q],
                dzsem.at[1, z, c],
                zp * NX + x,
                cc,
            )
    send(dzs.at[z, other], dzr.at[z, c], dzsem.at[0, nz - 1, 0], dzsem.at[1, z, c], kv, other)
    dzr[z, c] = dzs[z, c]
    mark("down_z")
    for zp in [z] + near:
        for cc in (c, other):
            if zp is z and cc is c:
                continue
            slot = dzr.at[zp, cc]
            remote(
                slot, slot, dzsem.at[0, 0, 0], dzsem.at[1, zp, cc], zp * NX + x, cc
            ).wait_recv()
    mark("finish")
    for i in range(2):
        rows = whole[kv, i].astype(F32)
        total = jnp.where(c == 1, squeeze(rows, True), squeeze(rows, False))
        for zp in range(nz):
            total = total + dzr[zp, i].astype(F32)
        outf[pl.ds(i, n_kv // 2, stride=2), :] = total
        outf[pl.ds(i + n_kv, n_kv // 2, stride=2), :] = pltpu.roll(total, LANES // 2, 1)
    out[...] = outf[:, : LANES // 2].astype(BF16)
    mark("drain")
    for copy in sent:
        copy.wait_send()
    mark()


def shards(
    tokens,
    lengths,
    state,
    cache_keys,
    cache_values,
    cache_rates,
    attn_gain,
    w_query,
    w_key,
    w_value,
    w_gate,
    w_decay,
    head_gain,
    w_out,
    mlp_gain,
    w_mlp_gate,
    w_mlp_up,
    w_mlp_down,
):
    n_kv = lax.axis_size("kv")
    nz = n_kv // NX
    heads, dk, dv = state.shape[1], state.shape[2], state.shape[3]
    width = mlp_gain.shape[0]
    qb, vb = heads * dk // LANES, heads * dv // LANES
    half0, half1 = (3 * qb + 2) // 2, vb
    slots = -(-2 * max(half0, half1) // 8) * 8
    rows2 = 2 * nz
    seqs = 2 * n_kv
    hrows = 2 * (-(-vb // 8) * 8)
    units = w_mlp_down.shape[0]
    cols5 = nz // 2 * LANES
    vmem, dma = pltpu.VMEM, pltpu.SemaphoreType.DMA
    bf, fl = BF16, F32
    scratch = [
        vmem((2, seqs, LANES // 2), bf),
        vmem((seqs, LANES), fl),
        vmem(w_query.shape, bf),
        vmem(w_key.shape, bf),
        vmem(w_decay.shape, bf),
        vmem(w_value.shape, bf),
        vmem(w_gate.shape, bf),
        vmem(state.shape, fl),
        vmem(cache_keys.shape, bf),
        vmem(cache_values.shape, bf),
        vmem(cache_rates.shape, fl),
        vmem((2,) + w_out.shape[::-1], bf),
        vmem(w_mlp_gate.shape[::-1], bf),
        vmem(w_mlp_up.shape[::-1], bf),
        vmem(w_mlp_down.shape, bf),
        vmem((NX, 2, rows2, half0 * LANES), bf),
        vmem((NX, 2, rows2, half1 * LANES), bf),
        vmem((2, rows2, half0 * LANES), bf),
        vmem((2, rows2, half1 * LANES), bf),
        vmem((2, rows2, half0 * LANES), bf),
        vmem((2, rows2, half1 * LANES), bf),
        vmem((2, 2, rows2, half0 * LANES), bf),
        vmem((2, 2, rows2, half1 * LANES), bf),
        vmem((rows2 * slots, LANES), fl),
        vmem((nz, 2 * slots, LANES), bf),
        vmem((nz, 2 * slots, LANES), bf),
        vmem((nz, 2 * slots, LANES), bf),
        vmem((nz, 2 * slots, LANES), bf),
        vmem(state.shape, bf),
        vmem((2 * slots, LANES), fl),
        vmem((2 * slots, LANES), fl),
        vmem((2 * qb, LANES), fl),
        vmem((2 * vb, LANES), fl),
        vmem((vb, LANES), fl),
        vmem((hrows, LANES), fl),
        vmem((n_kv, 2, hrows, LANES), bf),
        vmem((n_kv * 2 * hrows, LANES), fl),
        vmem((seqs, max(width, 2 * vb * LANES)), bf),
        vmem((n_kv, 2, n_kv, LANES), bf),
        vmem((seqs, units), bf),
        vmem((2, 2, NX, n_kv, cols5), bf),
        vmem((2, NX, n_kv, cols5), bf),
        vmem((NX, 2, n_kv, cols5), bf),
        vmem((2, n_kv, cols5), bf),
        vmem((2, n_kv, cols5), bf),
        vmem((2, 2, n_kv, cols5), bf),
        vmem((nz, 2, n_kv // 2, LANES), bf),
        vmem((nz, 2, n_kv // 2, LANES), bf),
        vmem((seqs, LANES), fl),
        dma((14,)),
        dma((8,)),
        dma((2, 12)),
        dma((2, 2 * nz)),
        dma((nz,)),
        dma((nz, NX)),
        dma((n_kv,)),
        dma((n_kv, 2)),
        dma((nz,)),
        dma((nz, NX)),
        dma((n_kv,)),
        dma((n_kv, 2)),
        dma((2, 6)),
        dma((2, nz, 2)),
    ]
    anywhere = pl.BlockSpec(memory_space=pl.ANY)
    in_vmem = pl.BlockSpec(memory_space=pltpu.VMEM)
    in_smem = pl.BlockSpec(memory_space=pltpu.SMEM)
    specs = [anywhere] * 18
    specs[1] = in_smem
    for k in (6, 12, 14):
        specs[k] = in_vmem
    return pl.pallas_call(
        functools.partial(kernel, (nz, qb, vb, dk, width)),
        out_shape=jax.ShapeDtypeStruct(tokens.shape, BF16),
        in_specs=specs,
        out_specs=in_vmem,
        scratch_shapes=scratch,
        compiler_params=pltpu.CompilerParams(collective_id=0, has_side_effects=True),
        name="layer",
    )(
        tokens,
        lengths,
        state,
        cache_keys,
        cache_values,
        cache_rates,
        attn_gain.reshape(1, -1),
        w_query,
        w_key,
        w_value,
        w_gate,
        w_decay,
        head_gain,
        w_out.T,
        mlp_gain.reshape(-1, LANES),
        w_mlp_gate.T,
        w_mlp_up.T,
        w_mlp_down,
    )


def solution(mesh):
    placed = (
        P("dp", ("kv", "tp")),
        P(("dp", "kv")),
        P(("dp", "kv"), "tp", None, None),
        P(("dp", "kv"), "tp", None, None),
        P(("dp", "kv"), "tp", None, None),
        P(("dp", "kv"), "tp", None, None),
        P("kv"),
        P("kv", "tp"),
        P("kv", "tp"),
        P("kv", "tp"),
        P("kv", "tp"),
        P("kv", "tp"),
        P("tp", None),
        P(None, ("kv", "tp")),
        P(),
        P(None, ("kv", "tp")),
        P(None, ("kv", "tp")),
        P(("kv", "tp"), None),
    )
    return jax.shard_map(
        shards, mesh=mesh, in_specs=placed, out_specs=P("dp", ("kv", "tp")), check_vma=False
    )
```

```python
import functools

import jax
import jax.numpy as jnp
from jax import lax
from jax.experimental import pallas as pl
from jax.experimental.pallas import tpu as pltpu
from jax.sharding import PartitionSpec as P

EPS = 1e-06
GATE_NORM = 16.0
NX = 4
LANES = 128
MESH = pl.DeviceIdType.MESH
F32 = jnp.float32
BF16 = jnp.bfloat16


def dot(a, b, dims=((1,), (0,))):
    return lax.dot_general(a, b, (dims, ((), ())), preferred_element_type=F32)


def high_low(a):
    high = a.astype(BF16)
    return high, (a - high.astype(F32)).astype(BF16)


def kernel(
    sizes,
    tokens,
    lengths,
    state,
    cache_keys,
    cache_values,
    cache_rates,
    attn_gain,
    w_query,
    w_key,
    w_value,
    w_gate,
    w_decay,
    head_gain,
    w_out,
    mlp_gain,
    w_mlp_gate,
    w_mlp_up,
    w_mlp_down,
    out,
    tok,
    tokf,
    wq,
    wk,
    wd,
    wv,
    wg,
    st,
    ck,
    cv,
    cr,
    wo,
    wmg,
    wmu,
    wmd,
    x0,
    x1,
    ra0,
    ra1,
    rs0,
    rs1,
    rb0,
    rb1,
    zf,
    zs0,
    zs1,
    zr0,
    zr1,
    memory,
    pack0,
    pack1,
    qe,
    att,
    hg,
    headf,
    headb,
    headsf,
    lhs,
    whole,
    hidden,
    dpart,
    dpeer,
    dx,
    dra,
    drs,
    drb,
    dzs,
    dzr,
    outf,
    again,
    hgain,
    mgain,
    mgainf,
    lens,
    lsem,
    psem,
    xsem,
    zsem,
    hsem,
    asem,
    dzsem,
):
    nz, qb, vb, dk, width = sizes
    rows2 = 2 * nz
    kv = lax.axis_index("kv")
    c = lax.axis_index("tp")
    other = 1 - c
    z = kv // NX
    x = kv % NX
    xr = (x + 1) % NX
    xl = (x + NX - 1) % NX
    xo = (x + 2) % NX
    steps = [((d + 1) // 2) * (1 if d % 2 else -1) for d in range(1, nz)]
    far = [(z + (s % nz)) % nz for s in steps][::-1]
    near = [(z + (s % nz)) % nz for s in steps]
    sides = [(x + d) % NX for d in (2, 1, 3)]

    def local(i, src, dst):
        copy = pltpu.make_async_copy(src, dst, lsem.at[i])
        copy.start()
        return copy

    def remote(src, dst, send, recv, to_kv, to_tp):
        return pltpu.make_async_remote_copy(
            src_ref=src,
            dst_ref=dst,
            send_sem=send,
            recv_sem=recv,
            device_id={"kv": to_kv, "tp": to_tp},
            device_id_type=MESH,
        )

    scopes = []

    def mark(name=None):
        if scopes:
            scopes.pop().__exit__(None, None, None)
        if name:
            scopes.append(jax.named_scope(name))
            scopes[-1].__enter__()

    def send(*args):
        remote(*args).start()

    mark("load")
    in_tok = local(0, tokens, tok.at[c])
    in_small = [
        local(14 + i, src, dst)
        for i, (src, dst) in enumerate(
            ((attn_gain, again), (head_gain, hgain), (mlp_gain, mgain), (lengths, lens))
        )
    ]
    in_w = [
        local(1 + i, src, dst)
        for i, (src, dst) in enumerate(
            ((w_query, wq), (w_key, wk), (w_decay, wd), (w_value, wv), (w_gate, wg))
        )
    ]
    in_cache = [
        local(6 + i, src, dst)
        for i, (src, dst) in enumerate(((cache_rates, cr), (cache_keys, ck), (cache_values, cv)))
    ]
    in_state = local(9, state, st)
    in_out = local(10, w_out, wo.at[c])
    in_mlp = [
        local(11 + i, src, dst)
        for i, (src, dst) in enumerate(((w_mlp_gate, wmg), (w_mlp_up, wmu), (w_mlp_down, wmd)))
    ]

    mark("barrier")
    barrier = pltpu.get_barrier_semaphore()

    def greet(to_kv, to_tp):
        pl.semaphore_signal(
            barrier, inc=1, device_id={"kv": to_kv, "tp": to_tp}, device_id_type=MESH
        )

    for zp in far:
        greet(zp * NX + x, c)
        greet(zp * NX + x, other)
    for xp in sides:
        greet(z * NX + xp, c)
    greet(kv, other)
    zf[...] = jnp.zeros_like(zf)
    for copy in in_small:
        copy.wait()
    mgainf[...] = mgain[...].astype(F32)
    for h in range(2):
        for b in range(vb // 2):
            hg[h * (vb // 2) + b : h * (vb // 2) + b + 1, :] = hgain[
                h : h + 1, b * LANES : (b + 1) * LANES
            ].astype(F32)
    pl.semaphore_wait(barrier, 2 * len(far) + len(sides) + 1)

    mark("tokens")
    in_tok.wait()
    send(tok.at[c], tok.at[c], psem.at[0], psem.at[1], kv, other)
    in_out.wait()
    send(wo.at[c], wo.at[c], psem.at[2], psem.at[3], kv, other)
    remote(tok.at[other], tok.at[other], psem.at[0], psem.at[1], kv, other).wait_recv()
    tokf[...] = jnp.concatenate([tok[0].astype(F32), tok[1].astype(F32)], axis=1)
    block = jnp.concatenate(
        [
            tokf[pl.ds(2 * xp + i, nz, stride=2 * NX), :]
            for xp in range(NX)
            for i in range(2)
        ],
        axis=0,
    )
    squares = jnp.sum(block * block, axis=1, keepdims=True)
    scaled = (block * again[...].astype(F32)).astype(BF16)

    def put(target, b, values):
        half = target.shape[2] // LANES
        at = (b % half) * LANES
        for xp in range(NX):
            target[2 * xp + b // half, :, at : at + LANES] = values[
                xp * rows2 : (xp + 1) * rows2
            ].astype(BF16)

    def project(copy, weight, target, start):
        copy.wait()
        part = dot(scaled, weight[...])
        for b in range(weight.shape[1] // LANES):
            put(target, start + b, part[:, b * LANES : (b + 1) * LANES])

    left, right = z * NX + xl, z * NX + xr

    def x_first(src, first, back, stage):
        out_sem, in_left, in_right, in_back = [xsem.at[stage, k] for k in range(4)]
        send(src.at[2 * xo], first.at[0], out_sem, in_left, right, c)
        send(src.at[2 * xo + 1], first.at[1], out_sem, in_right, left, c)
        send(src.at[2 * xr + 1], back.at[1], out_sem, in_back, right, c)
        send(src.at[2 * xl], back.at[2], out_sem, in_back, left, c)

    def x_second(src, first, relay, back, stage):
        out_sem, in_left, in_right, in_back = [xsem.at[stage, k] for k in range(4)]
        remote(first.at[0], first.at[0], out_sem, in_left, left, c).wait_recv()
        relay[0] = (src[2 * xr].astype(F32) + first[0].astype(F32)).astype(BF16)
        send(relay.at[0], back.at[0], out_sem, in_back, right, c)
        remote(first.at[1], first.at[1], out_sem, in_right, right, c).wait_recv()
        relay[1] = (src[2 * xl + 1].astype(F32) + first[1].astype(F32)).astype(BF16)
        send(relay.at[1], back.at[3], out_sem, in_back, left, c)

    def x_wait(back, stage):
        remote(back, back, xsem.at[stage, 0], xsem.at[stage, 3], left, c).wait_recv()

    def x_drain(src, stage):
        part = src.at[pl.ds(0, 6)]
        remote(part, part, xsem.at[stage, 0], xsem.at[stage, 3], left, c).wait_send()

    def x_sum(src, back, half):
        return (
            src[2 * x + half].astype(F32) + back[half].astype(F32) + back[2 + half].astype(F32)
        )

    project(in_w[0], wq, x0, 0)
    project(in_w[1], wk, x0, qb)
    project(in_w[2], wd, x0, 2 * qb)
    put(x0, 3 * qb, jnp.broadcast_to(squares, (squares.shape[0], LANES)))
    for b in range(3 * qb + 1, 2 * (x0.shape[2] // LANES)):
        put(x0, b, jnp.zeros((squares.shape[0], LANES), F32))
    x_first(x0, ra0, rb0, 0)
    mark("project_b")
    project(in_w[3], wv, x1, 0)
    project(in_w[4], wg, x1, vb)
    x_first(x1, ra1, rb1, 1)

    span = ck.shape[2]
    hb = vb // 2
    later = (
        lax.broadcasted_iota(jnp.int32, (span, span), 1)
        > lax.broadcasted_iota(jnp.int32, (span, span), 0)
    ).astype(BF16)
    ones = jnp.ones((span, LANES), BF16)
    slots = lax.broadcasted_iota(jnp.int32, (span, 1), 0)

    def fold(i, h):
        live = (slots < lens[i]).astype(F32)
        rates = cr[i, h] * live
        high, low = high_low(rates)
        rest = dot(later, high) + dot(later, low)
        keys = jnp.exp(-rest) * ck[i, h].astype(F32) * live
        shrink = jnp.exp(-(dot(high, ones, ((0,), (0,))) + dot(low, ones, ((0,), (0,)))))
        high, low = high_low(keys)
        value = cv[i, h]
        inner = dot(high, value, ((0,), (0,))) + dot(low, value, ((0,), (0,)))
        for b in range(hb):
            cols = slice(b * LANES, (b + 1) * LANES)
            memory[i, h, :, cols] = (st[i, h, :, cols] * shrink + inner[:, cols]).astype(BF16)

    mark("x_second")
    for copy in in_cache:
        copy.wait()
    in_state.wait()
    x_second(x0, ra0, rs0, rb0, 0)
    x_second(x1, ra1, rs1, rb1, 1)

    slots_row = zf.shape[0] // rows2

    def z_send(src, back, packed, landing, stage):
        half = src.shape[2] // LANES
        x_wait(back, stage)
        for hh in (0, 1):
            total = x_sum(src, back, hh)
            for b in range(half):
                for i in range(2):
                    zf[pl.ds(i * slots_row + hh * half + b, nz, stride=2 * slots_row), :] = total[
                        i * nz : (i + 1) * nz, b * LANES : (b + 1) * LANES
                    ]
        for zp in range(nz):
            packed[zp] = zf[zp * 2 * slots_row : (zp + 1) * 2 * slots_row, :].astype(BF16)
        for zp in far:
            send(
                packed.at[zp], landing.at[z], zsem.at[stage, 0], zsem.at[stage, 1], zp * NX + x, c
            )

    def z_sum(packed, landing, stage):
        part = landing.at[pl.ds(0, nz - 1)]
        remote(part, part, zsem.at[stage, 0], zsem.at[stage, 1], left, c).wait_recv()
        total = packed[z].astype(F32)
        for zp in near:
            total = total + landing[zp].astype(F32)
        return total

    mark("z_send_a")
    z_send(x0, rb0, zs0, zr0, 0)
    mark("z_send_b")
    z_send(x1, rb1, zs1, zr1, 1)
    mark("fold")
    for i in range(2):
        for h in range(2):
            fold(i, h)

    mark("z_wait_a")
    pack0[...] = z_sum(zs0, zr0, 0)
    mark("heads_a")
    own = []
    inverse = []
    qh = qb // 2
    for i in range(2):
        at = i * slots_row
        inv = lax.rsqrt(pack0[at + 3 * qb : at + 3 * qb + 1, :] * (1.0 / width) + EPS)
        inverse.append(inv)
        query = pack0[at : at + qb, :] * inv * dk ** (-0.5)
        key = pack0[at + qb : at + 2 * qb, :] * inv
        raw = pack0[at + 2 * qb : at + 3 * qb, :] * inv
        decay = (jnp.minimum(raw, 0.0) - jnp.log1p(jnp.exp(-jnp.abs(raw)))) / GATE_NORM
        qe[i * qb : (i + 1) * qb, :] = query * jnp.exp(decay)
        both = query * key
        for h in range(2):
            part = jnp.sum(both[h * qh : (h + 1) * qh, :], axis=0, keepdims=True)
            own.append(jnp.sum(part, axis=1, keepdims=True))
    for i in range(2):
        for h in range(2):
            row = jnp.concatenate(
                [qe[i * qb + h * qh + b : i * qb + h * qh + b + 1, :] for b in range(qh)], axis=1
            )
            high, low = high_low(row)
            got = dot(jnp.concatenate([high, low], axis=0), memory[i, h])
            got = got[0:1] + got[1:2]
            for b in range(hb):
                att[i * vb + h * hb + b : i * vb + h * hb + b + 1, :] = got[
                    :, b * LANES : (b + 1) * LANES
                ]
    mark("z_wait_b")
    pack1[...] = z_sum(zs1, zr1, 1)
    for i in range(2):
        at = i * slots_row
        if i == 0:
            mark("heads_b")
        value = pack1[at : at + vb, :] * inverse[i]
        gate = pack1[at + vb : at + 2 * vb, :] * inverse[i]
        attended = att[i * vb : (i + 1) * vb, :]
        for h in range(2):
            part = slice(h * hb, (h + 1) * hb)
            full = attended[part] + own[2 * i + h] * value[part]
            mean = jnp.sum(jnp.sum(full * full, axis=0, keepdims=True), axis=1, keepdims=True)
            norm = full * lax.rsqrt(mean * (1.0 / (hb * LANES)) + EPS) * hg[part, :]
            g = gate[part]
            headf[i * (headf.shape[0] // 2) + h * hb : i * (headf.shape[0] // 2) + (h + 1) * hb, :] = (
                g / (1.0 + jnp.exp(-g)) * norm
            )
    headb[2 * kv + c] = headf[...].astype(BF16)

    def gather(buf, sems, with_partner, consume):
        out_sem = sems.at[0]
        mine = buf.at[2 * kv + c]
        for zp in far:
            send(mine, mine, out_sem, sems.at[1 + z], zp * NX + x, c)
        for xp in sides:
            send(mine, mine, out_sem, sems.at[1 + nz + z], z * NX + xp, c)
        if with_partner:
            send(mine, mine, out_sem, sems.at[1 + 2 * nz + z], kv, other)
        for zp in near:
            origin = zp * NX + x
            slot = buf.at[2 * origin + c]
            remote(slot, slot, out_sem, sems.at[1 + zp], origin, c).wait_recv()
            for xp in sides:
                send(slot, slot, out_sem, sems.at[1 + nz + zp], z * NX + xp, c)
            send(slot, slot, out_sem, sems.at[1 + 2 * nz + zp], kv, other)
        order = [z] + near

        def finish(zp):
            part = buf.at[pl.ds(0, NX - (zp is z and not with_partner))]
            remote(part, part, out_sem, sems.at[1 + 2 * nz + zp], kv, other).wait_recv()
            consume(zp)

        for n, zp in enumerate(order):
            part = buf.at[pl.ds(0, NX - 1)]
            remote(part, part, out_sem, sems.at[1 + nz + zp], left, c).wait_recv()
            for xp in sides[::-1]:
                slot = buf.at[2 * (zp * NX + xp) + c]
                send(slot, slot, out_sem, sems.at[1 + 2 * nz + zp], kv, other)
            if n:
                finish(order[n - 1])
        finish(order[-1])

    def gather_drain(buf, sems, with_partner):
        part = buf.at[pl.ds(0, 2 * nz * NX - 1 - (not with_partner))]
        remote(part, part, sems.at[0], sems.at[1], left, c).wait_send()

    n_kv = nz * NX
    hrows = headf.shape[0]

    def widen(zp):
        for k in range(2 * NX):
            slot = 2 * NX * zp + k
            headsf[pl.ds(pl.multiple_of(slot * hrows, 8), hrows), :] = headb[slot].astype(F32)

    mark("gather_heads")
    gather(headb, hsem, True, widen)

    mark("project_out")
    for cc in range(2):
        for b in range(vb):
            at = (cc * vb + b) * LANES
            for i in range(2):
                lhs[i * n_kv : (i + 1) * n_kv, at : at + LANES] = headsf[
                    pl.ds(cc * hrows + i * (hrows // 2) + b, n_kv, stride=2 * hrows), :
                ].astype(BF16)
    remote(wo.at[other], wo.at[other], psem.at[2], psem.at[3], kv, other).wait_recv()
    projected = dot(lhs[...], wo[...].reshape(LANES, 2 * vb * LANES), ((1,), (1,)))
    for i in range(2):
        old = tokf[pl.ds(i, n_kv, stride=2), :]
        whole[2 * kv + i] = (old + projected[i * n_kv : (i + 1) * n_kv]).astype(BF16)

    mark("gather_after")
    in_mlp[0].wait()
    in_mlp[1].wait()
    sums = [
        jnp.zeros((2 * n_kv, LANES), F32),
        jnp.zeros(hidden.shape, F32),
        jnp.zeros(hidden.shape, F32),
    ]

    def multiply(zp):
        parts = []
        for xp in range(NX):
            k = zp * NX + xp
            rows = jnp.concatenate([whole[2 * k], whole[2 * k + 1]], axis=0).astype(F32)
            sums[0] = sums[0] + rows * rows
            parts.append((rows * mgainf[pl.ds(k, 1), :]).astype(BF16))
        rows = jnp.concatenate(parts, axis=1)
        cols = pl.ds(pl.multiple_of(zp * NX * LANES, LANES), NX * LANES)
        sums[1] = sums[1] + dot(rows, wmg[:, cols], ((1,), (1,)))
        sums[2] = sums[2] + dot(rows, wmu[:, cols], ((1,), (1,)))

    gather(whole, asem, False, multiply)

    mark("mlp_in")
    inv = lax.rsqrt(jnp.sum(sums[0], axis=1, keepdims=True) * (1.0 / width) + EPS)
    gate = sums[1] * inv
    up = sums[2] * inv
    hidden[...] = (gate / (1.0 + jnp.exp(-gate)) * up).astype(BF16)
    mark("mlp_down")
    in_mlp[2].wait()
    hz_half = nz // 2
    for zh in range(2):
        for zi in range(hz_half):
            zp = zh * hz_half + zi
            part = dot(hidden[...], wmd[:, zp * NX * LANES : (zp + 1) * NX * LANES]).astype(BF16)
            for xp in range(NX):
                for i in range(2):
                    dpart[i, zh, xp, :, zi * LANES : (zi + 1) * LANES] = part[
                        i * n_kv : (i + 1) * n_kv, xp * LANES : (xp + 1) * LANES
                    ]
        send(dpart.at[other, zh], dpeer.at[zh], psem.at[4], psem.at[5 + zh], kv, other)
    mark("down_peer")
    for zh in range(2):
        remote(
            dpeer.at[zh], dpeer.at[zh], psem.at[4], psem.at[5 + zh], kv, other
        ).wait_recv()
        for xp in (xo, xr, xl, x):
            dx[2 * xp + zh] = (dpart[c, zh, xp].astype(F32) + dpeer[zh, xp].astype(F32)).astype(BF16)
    mark("down_x")
    x_first(dx, dra, drb, 2)
    x_second(dx, dra, drs, drb, 2)
    low_lanes = lax.broadcasted_iota(jnp.int32, (n_kv // 2, LANES), 1) < LANES // 2

    def squeeze(rows, right):
        top, bottom = rows[: n_kv // 2], rows[n_kv // 2 :]
        if right:
            top = pltpu.roll(top, LANES // 2, 1)
        else:
            bottom = pltpu.roll(bottom, LANES // 2, 1)
        return jnp.where(low_lanes, top, bottom)

    mark("down_x2")
    x_wait(drb, 2)
    mark("down_pack")
    for zh in range(2):
        total = x_sum(dx, drb, zh)
        for zi in range(hz_half):
            rows = total[:, zi * LANES : (zi + 1) * LANES]
            for cc in range(2):
                dzs[2 * (zh * hz_half + zi) + cc] = squeeze(rows, cc == 1).astype(BF16)
    for zp in far:
        for cc in (other, c):
            send(
                dzs.at[2 * zp + cc],
                dzr.at[2 * z + c],
                dzsem.at[0],
                dzsem.at[1],
                zp * NX + x,
                cc,
            )
    send(dzs.at[2 * z + other], dzr.at[2 * z + c], dzsem.at[0], dzsem.at[1], kv, other)
    dzr[2 * z + c] = dzs[2 * z + c]
    mark("down_z")
    part = dzr.at[pl.ds(0, 2 * nz - 1)]
    remote(part, part, dzsem.at[0], dzsem.at[1], kv, other).wait_recv()
    mark("finish")
    for i in range(2):
        rows = whole[2 * kv + i].astype(F32)
        total = jnp.where(c == 1, squeeze(rows, True), squeeze(rows, False))
        for zp in range(nz):
            total = total + dzr[2 * zp + i].astype(F32)
        outf[pl.ds(i, n_kv // 2, stride=2), :] = total
        outf[pl.ds(i + n_kv, n_kv // 2, stride=2), :] = pltpu.roll(total, LANES // 2, 1)
    out[...] = outf[:, : LANES // 2].astype(BF16)
    mark("drain")
    remote(tok.at[c], tok.at[c], psem.at[0], psem.at[1], kv, other).wait_send()
    remote(wo.at[c], wo.at[c], psem.at[2], psem.at[3], kv, other).wait_send()
    x_drain(x0, 0)
    x_drain(x1, 1)
    for stage, landing in enumerate((zr0, zr1)):
        part = landing.at[pl.ds(0, nz - 1)]
        remote(part, part, zsem.at[stage, 0], zsem.at[stage, 1], left, c).wait_send()
    gather_drain(headb, hsem, True)
    gather_drain(whole, asem, False)
    remote(dpeer, dpeer, psem.at[4], psem.at[5], kv, other).wait_send()
    x_drain(dx, 2)
    part = dzr.at[pl.ds(0, 2 * nz - 1)]
    remote(part, part, dzsem.at[0], dzsem.at[1], kv, other).wait_send()
    mark()


def shards(
    tokens,
    lengths,
    state,
    cache_keys,
    cache_values,
    cache_rates,
    attn_gain,
    w_query,
    w_key,
    w_value,
    w_gate,
    w_decay,
    head_gain,
    w_out,
    mlp_gain,
    w_mlp_gate,
    w_mlp_up,
    w_mlp_down,
):
    n_kv = lax.axis_size("kv")
    nz = n_kv // NX
    heads, dk, dv = state.shape[1], state.shape[2], state.shape[3]
    width = mlp_gain.shape[0]
    qb, vb = heads * dk // LANES, heads * dv // LANES
    half0, half1 = (3 * qb + 2) // 2, vb
    slots = -(-2 * max(half0, half1) // 8) * 8
    rows2 = 2 * nz
    seqs = 2 * n_kv
    hrows = 2 * vb
    units = w_mlp_down.shape[0]
    cols5 = nz // 2 * LANES
    vmem, dma = pltpu.VMEM, pltpu.SemaphoreType.DMA
    bf, fl = BF16, F32
    scratch = [
        vmem((2, seqs, LANES // 2), bf),
        vmem((seqs, LANES), fl),
        vmem(w_query.shape, bf),
        vmem(w_key.shape, bf),
        vmem(w_decay.shape, bf),
        vmem(w_value.shape, bf),
        vmem(w_gate.shape, bf),
        vmem(state.shape, fl),
        vmem(cache_keys.shape, bf),
        vmem(cache_values.shape, bf),
        vmem(cache_rates.shape, fl),
        vmem((2,) + w_out.shape[::-1], bf),
        vmem(w_mlp_gate.shape[::-1], bf),
        vmem(w_mlp_up.shape[::-1], bf),
        vmem(w_mlp_down.shape, bf),
        vmem((NX * 2, rows2, half0 * LANES), bf),
        vmem((NX * 2, rows2, half1 * LANES), bf),
        vmem((2, rows2, half0 * LANES), bf),
        vmem((2, rows2, half1 * LANES), bf),
        vmem((2, rows2, half0 * LANES), bf),
        vmem((2, rows2, half1 * LANES), bf),
        vmem((4, rows2, half0 * LANES), bf),
        vmem((4, rows2, half1 * LANES), bf),
        vmem((rows2 * slots, LANES), fl),
        vmem((nz, 2 * slots, LANES), bf),
        vmem((nz, 2 * slots, LANES), bf),
        vmem((nz, 2 * slots, LANES), bf),
        vmem((nz, 2 * slots, LANES), bf),
        vmem(state.shape, bf),
        vmem((2 * slots, LANES), fl),
        vmem((2 * slots, LANES), fl),
        vmem((2 * qb, LANES), fl),
        vmem((2 * vb, LANES), fl),
        vmem((vb, LANES), fl),
        vmem((hrows, LANES), fl),
        vmem((2 * n_kv, hrows, LANES), bf),
        vmem((n_kv * 2 * hrows, LANES), fl),
        vmem((seqs, 2 * vb * LANES), bf),
        vmem((2 * n_kv, n_kv, LANES), bf),
        vmem((seqs, units), bf),
        vmem((2, 2, NX, n_kv, cols5), bf),
        vmem((2, NX, n_kv, cols5), bf),
        vmem((NX * 2, n_kv, cols5), bf),
        vmem((2, n_kv, cols5), bf),
        vmem((2, n_kv, cols5), bf),
        vmem((4, n_kv, cols5), bf),
        vmem((2 * nz, n_kv // 2, LANES), bf),
        vmem((2 * nz, n_kv // 2, LANES), bf),
        vmem((seqs, LANES), fl),
        vmem((1, LANES), bf),
        vmem((heads, dv), bf),
        vmem((n_kv, LANES), bf),
        vmem((n_kv, LANES), fl),
        pltpu.SMEM((2,), jnp.int32),
        dma((18,)),
        dma((7,)),
        dma((3, 4)),
        dma((2, 2)),
        dma((1 + 3 * nz,)),
        dma((1 + 3 * nz,)),
        dma((2,)),
    ]
    anywhere = pl.BlockSpec(memory_space=pl.ANY)
    in_vmem = pl.BlockSpec(memory_space=pltpu.VMEM)
    specs = [anywhere] * 18
    return pl.pallas_call(
        functools.partial(kernel, (nz, qb, vb, dk, width)),
        out_shape=jax.ShapeDtypeStruct(tokens.shape, BF16),
        in_specs=specs,
        out_specs=in_vmem,
        scratch_shapes=scratch,
        compiler_params=pltpu.CompilerParams(collective_id=0, has_side_effects=True),
        name="layer",
    )(
        tokens,
        lengths,
        state,
        cache_keys,
        cache_values,
        cache_rates,
        attn_gain.reshape(1, -1),
        w_query,
        w_key,
        w_value,
        w_gate,
        w_decay,
        head_gain,
        w_out.T,
        mlp_gain.reshape(-1, LANES),
        w_mlp_gate.T,
        w_mlp_up.T,
        w_mlp_down,
    )


def solution(mesh):
    placed = (
        P("dp", ("kv", "tp")),
        P(("dp", "kv")),
        P(("dp", "kv"), "tp", None, None),
        P(("dp", "kv"), "tp", None, None),
        P(("dp", "kv"), "tp", None, None),
        P(("dp", "kv"), "tp", None, None),
        P("kv"),
        P("kv", "tp"),
        P("kv", "tp"),
        P("kv", "tp"),
        P("kv", "tp"),
        P("kv", "tp"),
        P("tp", None),
        P(None, ("kv", "tp")),
        P(),
        P(None, ("kv", "tp")),
        P(None, ("kv", "tp")),
        P(("kv", "tp"), None),
    )
    return jax.shard_map(
        shards, mesh=mesh, in_specs=placed, out_specs=P("dp", ("kv", "tp")), check_vma=False
    )
```

```python
import functools

import jax
import jax.numpy as jnp
from jax import lax
from jax.experimental import pallas as pl
from jax.experimental.pallas import tpu as pltpu
from jax.sharding import PartitionSpec as P

EPS = 1e-06
GATE_NORM = 16.0
NX = 4
LANES = 128
MESH = pl.DeviceIdType.MESH
F32 = jnp.float32
BF16 = jnp.bfloat16


def dot(a, b, dims=((1,), (0,))):
    return lax.dot_general(a, b, (dims, ((), ())), preferred_element_type=F32)


def high_low(a):
    high = a.astype(BF16)
    return high, (a - high.astype(F32)).astype(BF16)


def kernel(
    sizes,
    tokens,
    lengths,
    state,
    cache_keys,
    cache_values,
    cache_rates,
    attn_gain,
    w_query,
    w_key,
    w_value,
    w_gate,
    w_decay,
    head_gain,
    w_out,
    mlp_gain,
    w_mlp_gate,
    w_mlp_up,
    w_mlp_down,
    out,
    tok,
    tokf,
    wq,
    wk,
    wd,
    wv,
    wg,
    st,
    ck,
    cv,
    cr,
    wo,
    wmg,
    wmu,
    wmd,
    xa,
    xb,
    xfa,
    xfb,
    xsa,
    xsb,
    xba,
    xbb,
    zf,
    zs,
    zr,
    memory,
    pack0,
    pack1,
    qe,
    att,
    hg,
    headf,
    headb,
    headsf,
    lhs,
    whole,
    hidden,
    dpart,
    dpeer,
    dx,
    dra,
    drs,
    drb,
    dzs,
    dzr,
    outf,
    again,
    hgain,
    mgain,
    mgainf,
    lens,
    lsem,
    psem,
    xsem,
    zsem,
    hsem,
    asem,
    dzsem,
):
    nz, qb, vb, dk, width = sizes
    nh = nz // 2
    kv = lax.axis_index("kv")
    c = lax.axis_index("tp")
    other = 1 - c
    z = kv // NX
    x = kv % NX
    xr = (x + 1) % NX
    xl = (x + NX - 1) % NX
    xo = (x + 2) % NX
    steps = [((d + 1) // 2) * (1 if d % 2 else -1) for d in range(1, nz)]
    far = [(z + (s % nz)) % nz for s in steps][::-1]
    near = [(z + (s % nz)) % nz for s in steps]
    sides = [(x + d) % NX for d in (2, 1, 3)]
    last = near[-1]

    def turn(g, j):
        return (nz // 4 + g * nh + j) % nz

    def zrel(g, j):
        return (z + turn(g, j)) % nz

    def by_distance(g):
        return sorted(range(nh), key=lambda j: -min(turn(g, j), nz - turn(g, j)))

    self_g, self_j = divmod((nz - nz // 4) % nz, nh)

    def local(i, src, dst):
        copy = pltpu.make_async_copy(src, dst, lsem.at[i])
        copy.start()
        return copy

    def remote(src, dst, send, recv, to_kv, to_tp):
        return pltpu.make_async_remote_copy(
            src_ref=src,
            dst_ref=dst,
            send_sem=send,
            recv_sem=recv,
            device_id={"kv": to_kv, "tp": to_tp},
            device_id_type=MESH,
        )

    scopes = []

    def mark(name=None):
        if scopes:
            scopes.pop().__exit__(None, None, None)
        if name:
            scopes.append(jax.named_scope(name))
            scopes[-1].__enter__()

    def send(*args):
        remote(*args).start()

    mark("load")
    in_tok = local(0, tokens, tok.at[c])
    in_small = [
        local(14 + i, src, dst)
        for i, (src, dst) in enumerate(
            ((attn_gain, again), (head_gain, hgain), (mlp_gain, mgain), (lengths, lens))
        )
    ]
    in_w = [
        local(1 + i, src, dst)
        for i, (src, dst) in enumerate(
            ((w_query, wq), (w_key, wk), (w_decay, wd), (w_value, wv), (w_gate, wg))
        )
    ]
    in_cache = [
        local(6 + i, src, dst)
        for i, (src, dst) in enumerate(((cache_rates, cr), (cache_keys, ck), (cache_values, cv)))
    ]
    in_state = local(9, state, st)
    in_out = local(10, w_out, wo.at[c])
    in_mlp = [
        local(11 + i, src, dst)
        for i, (src, dst) in enumerate(((w_mlp_gate, wmg), (w_mlp_up, wmu), (w_mlp_down, wmd)))
    ]

    mark("barrier")
    barrier = pltpu.get_barrier_semaphore()

    def greet(to_kv, to_tp):
        pl.semaphore_signal(
            barrier, inc=1, device_id={"kv": to_kv, "tp": to_tp}, device_id_type=MESH
        )

    for zp in far:
        greet(zp * NX + x, c)
        greet(zp * NX + x, other)
    for xp in sides:
        greet(z * NX + xp, c)
        greet(last * NX + xp, c)
    greet(kv, other)
    zf[...] = jnp.zeros_like(zf)
    for copy in in_small:
        copy.wait()
    mgainf[...] = mgain[...].astype(F32)
    for h in range(2):
        for b in range(vb // 2):
            hg[h * (vb // 2) + b : h * (vb // 2) + b + 1, :] = hgain[
                h : h + 1, b * LANES : (b + 1) * LANES
            ].astype(F32)
    pl.semaphore_wait(barrier, 2 * len(far) + 2 * len(sides) + 1)

    mark("tokens")
    in_tok.wait()
    send(tok.at[c], tok.at[c], psem.at[0], psem.at[1], kv, other)
    in_out.wait()
    send(wo.at[c], wo.at[c], psem.at[2], psem.at[3], kv, other)
    remote(tok.at[other], tok.at[other], psem.at[0], psem.at[1], kv, other).wait_recv()
    tokf[...] = jnp.concatenate([tok[0].astype(F32), tok[1].astype(F32)], axis=1)
    block = []
    for xp in range(NX):
        pair = [
            pltpu.roll(
                tokf[pl.ds(2 * xp + i, nz, stride=2 * NX), :], (2 * nz - z - nz // 4) % nz, 0
            )
            for i in range(2)
        ]
        for g in range(2):
            block += [rows[g * nh : (g + 1) * nh] for rows in pair]
    block = jnp.concatenate(block, axis=0)
    squares = jnp.sum(block * block, axis=1, keepdims=True)
    scaled = (block * again[...].astype(F32)).astype(BF16)

    def put(target, b, values):
        half = target.shape[3] // LANES
        at = (b % half) * LANES
        for xp in range(NX):
            for g in range(2):
                row = (2 * xp + g) * nz
                target[g, 2 * xp + b // half, :, at : at + LANES] = values[row : row + nz].astype(
                    BF16
                )

    def project(copy, weight, target, start):
        copy.wait()
        part = dot(scaled, weight[...])
        for b in range(weight.shape[1] // LANES):
            put(target, start + b, part[:, b * LANES : (b + 1) * LANES])

    left, right = z * NX + xl, z * NX + xr

    def x_first(src, first, back, stage):
        out_sem, in_left, in_right, in_back = [xsem.at[stage, k] for k in range(4)]
        send(src.at[2 * xo], first.at[0], out_sem, in_left, right, c)
        send(src.at[2 * xo + 1], first.at[1], out_sem, in_right, left, c)

    def x_direct(src, first, back, stage):
        out_sem, in_left, in_right, in_back = [xsem.at[stage, k] for k in range(4)]
        send(src.at[2 * xr + 1], back.at[1], out_sem, in_back, right, c)
        send(src.at[2 * xl], back.at[2], out_sem, in_back, left, c)

    def x_second(src, first, relay, back, stage):
        out_sem, in_left, in_right, in_back = [xsem.at[stage, k] for k in range(4)]
        remote(first.at[0], first.at[0], out_sem, in_left, left, c).wait_recv()
        relay[0] = (src[2 * xr].astype(F32) + first[0].astype(F32)).astype(BF16)
        send(relay.at[0], back.at[0], out_sem, in_back, right, c)
        remote(first.at[1], first.at[1], out_sem, in_right, right, c).wait_recv()
        relay[1] = (src[2 * xl + 1].astype(F32) + first[1].astype(F32)).astype(BF16)
        send(relay.at[1], back.at[3], out_sem, in_back, left, c)

    def x_wait(back, stage):
        remote(back, back, xsem.at[stage, 0], xsem.at[stage, 3], left, c).wait_recv()

    def x_drain(src, stage):
        part = src.at[pl.ds(0, 6)]
        remote(part, part, xsem.at[stage, 0], xsem.at[stage, 3], left, c).wait_send()

    def x_sum(src, back, half):
        return (
            src[2 * x + half].astype(F32) + back[half].astype(F32) + back[2 + half].astype(F32)
        )

    def x_stage(g, col):
        src, first, relay, back = ((xa, xfa, xsa, xba), (xb, xfb, xsb, xbb))[col]
        return src.at[g], first.at[g], relay.at[g], back.at[g], 2 * g + col

    def x_one(g, col):
        src, first, relay, back, stage = x_stage(g, col)
        x_first(src, first, back, stage)

    def x_ind(g, col):
        src, first, relay, back, stage = x_stage(g, col)
        x_direct(src, first, back, stage)

    project(in_w[0], wq, xa, 0)
    project(in_w[1], wk, xa, qb)
    project(in_w[2], wd, xa, 2 * qb)
    put(xa, 3 * qb, jnp.broadcast_to(squares, (squares.shape[0], LANES)))
    for b in range(3 * qb + 1, 2 * (xa.shape[3] // LANES)):
        put(xa, b, jnp.zeros((squares.shape[0], LANES), F32))
    x_one(0, 0)
    mark("project_b")
    project(in_w[3], wv, xb, 0)
    project(in_w[4], wg, xb, vb)
    x_one(0, 1)
    x_ind(0, 0)
    x_ind(0, 1)
    x_one(1, 0)
    x_one(1, 1)

    span = ck.shape[2]
    hb = vb // 2
    later = (
        lax.broadcasted_iota(jnp.int32, (span, span), 1)
        > lax.broadcasted_iota(jnp.int32, (span, span), 0)
    ).astype(BF16)
    ones = jnp.ones((span, LANES), BF16)
    slots = lax.broadcasted_iota(jnp.int32, (span, 1), 0)

    def fold(i, h):
        live = (slots < lens[i]).astype(F32)
        rates = cr[i, h] * live
        high, low = high_low(rates)
        rest = dot(later, high) + dot(later, low)
        keys = jnp.exp(-rest) * ck[i, h].astype(F32) * live
        shrink = jnp.exp(-(dot(high, ones, ((0,), (0,))) + dot(low, ones, ((0,), (0,)))))
        high, low = high_low(keys)
        value = cv[i, h]
        inner = dot(high, value, ((0,), (0,))) + dot(low, value, ((0,), (0,)))
        for b in range(hb):
            cols = slice(b * LANES, (b + 1) * LANES)
            memory[i, h, :, cols] = (st[i, h, :, cols] * shrink + inner[:, cols]).astype(BF16)

    mark("fold_a")
    for copy in in_cache:
        copy.wait()
    in_state.wait()
    for h in range(2):
        fold(0, h)
    mark("x_second_a")
    x_second(*x_stage(0, 0))
    x_second(*x_stage(0, 1))
    mark("x_second_b")
    x_ind(1, 0)
    x_ind(1, 1)
    x_second(*x_stage(1, 0))
    x_second(*x_stage(1, 1))

    slots_row = zf.shape[0] // (2 * nh)

    def z_send(g, col):
        src, first, relay, back, stage = x_stage(g, col)
        half = src.shape[2] // LANES
        x_wait(back, stage)
        for hh in (0, 1):
            total = x_sum(src, back, hh)
            for b in range(half):
                for i in range(2):
                    zf[pl.ds(i * slots_row + hh * half + b, nh, stride=2 * slots_row), :] = total[
                        i * nh : (i + 1) * nh, b * LANES : (b + 1) * LANES
                    ]
        for j in by_distance(g):
            zs[stage, j] = zf[j * 2 * slots_row : (j + 1) * 2 * slots_row, :].astype(BF16)
            if (g, j) != (self_g, self_j):
                send(
                    zs.at[stage, j],
                    zr.at[stage, j],
                    zsem.at[stage, 0],
                    zsem.at[stage, 1],
                    zrel(g, j) * NX + x,
                    c,
                )

    def z_part(g, col):
        return zr.at[2 * g + col, pl.ds(0, nh - (g == self_g))]

    def z_sum(col):
        for g in range(2):
            part = z_part(g, col)
            stage = 2 * g + col
            remote(part, part, zsem.at[stage, 0], zsem.at[stage, 1], left, c).wait_recv()
        total = zs[2 * self_g + col, self_j].astype(F32)
        for g in range(2):
            for j in range(nh):
                if (g, j) != (self_g, self_j):
                    total = total + zr[2 * g + col, j].astype(F32)
        return total

    mark("z_send_a")
    z_send(0, 0)
    z_send(0, 1)
    mark("fold_b")
    for h in range(2):
        fold(1, h)
    mark("z_send_b")
    z_send(1, 0)
    z_send(1, 1)

    mark("z_wait_a")
    pack0[...] = z_sum(0)
    mark("heads_a")
    own = []
    inverse = []
    qh = qb // 2
    for i in range(2):
        at = i * slots_row
        inv = lax.rsqrt(pack0[at + 3 * qb : at + 3 * qb + 1, :] * (1.0 / width) + EPS)
        inverse.append(inv)
        query = pack0[at : at + qb, :] * inv * dk ** (-0.5)
        key = pack0[at + qb : at + 2 * qb, :] * inv
        raw = pack0[at + 2 * qb : at + 3 * qb, :] * inv
        decay = (jnp.minimum(raw, 0.0) - jnp.log1p(jnp.exp(-jnp.abs(raw)))) / GATE_NORM
        qe[i * qb : (i + 1) * qb, :] = query * jnp.exp(decay)
        both = query * key
        for h in range(2):
            part = jnp.sum(both[h * qh : (h + 1) * qh, :], axis=0, keepdims=True)
            own.append(jnp.sum(part, axis=1, keepdims=True))
    for i in range(2):
        for h in range(2):
            row = jnp.concatenate(
                [qe[i * qb + h * qh + b : i * qb + h * qh + b + 1, :] for b in range(qh)], axis=1
            )
            high, low = high_low(row)
            got = dot(jnp.concatenate([high, low], axis=0), memory[i, h])
            got = got[0:1] + got[1:2]
            for b in range(hb):
                att[i * vb + h * hb + b : i * vb + h * hb + b + 1, :] = got[
                    :, b * LANES : (b + 1) * LANES
                ]
    mark("z_wait_b")
    pack1[...] = z_sum(1)
    for i in range(2):
        at = i * slots_row
        if i == 0:
            mark("heads_b")
        value = pack1[at : at + vb, :] * inverse[i]
        gate = pack1[at + vb : at + 2 * vb, :] * inverse[i]
        attended = att[i * vb : (i + 1) * vb, :]
        for h in range(2):
            part = slice(h * hb, (h + 1) * hb)
            full = attended[part] + own[2 * i + h] * value[part]
            mean = jnp.sum(jnp.sum(full * full, axis=0, keepdims=True), axis=1, keepdims=True)
            norm = full * lax.rsqrt(mean * (1.0 / (hb * LANES)) + EPS) * hg[part, :]
            g = gate[part]
            headf[i * (headf.shape[0] // 2) + h * hb : i * (headf.shape[0] // 2) + (h + 1) * hb, :] = (
                g / (1.0 + jnp.exp(-g)) * norm
            )
    headb[2 * kv + c] = headf[...].astype(BF16)

    def gather(buf, sems, with_partner, consume):
        out_sem = sems.at[0]
        mine = buf.at[2 * kv + c]

        def in_z(zp):
            return sems.at[1 + zp]

        def in_x(zp):
            return sems.at[1 + nz + zp]

        def in_peer(zp):
            return sems.at[1 + 2 * nz + zp]

        for xp in sides:
            send(mine, mine, out_sem, in_x(z), last * NX + xp, c)
        for zp in far:
            send(mine, mine, out_sem, in_z(z), zp * NX + x, c)
        for xp in sides:
            send(mine, mine, out_sem, in_x(z), z * NX + xp, c)
        if with_partner:
            send(mine, mine, out_sem, in_peer(z), kv, other)

        def take_z(zp):
            origin = zp * NX + x
            slot = buf.at[2 * origin + c]
            remote(slot, slot, out_sem, in_z(zp), origin, c).wait_recv()
            if zp is not last:
                for xp in sides:
                    send(slot, slot, out_sem, in_x(zp), z * NX + xp, c)
            send(slot, slot, out_sem, in_peer(zp), kv, other)

        def take_x(zp):
            part = buf.at[pl.ds(0, NX - 1)]
            remote(part, part, out_sem, in_x(zp), left, c).wait_recv()
            for xp in sides[::-1]:
                slot = buf.at[2 * (zp * NX + xp) + c]
                send(slot, slot, out_sem, in_peer(zp), kv, other)

        def finish(zp):
            part = buf.at[pl.ds(0, NX - (zp is z and not with_partner))]
            remote(part, part, out_sem, in_peer(zp), kv, other).wait_recv()
            consume(zp)

        for n, zp in enumerate(near):
            take_z(zp)
            if n == len(near) // 2:
                take_x(z)
        mark("take_x")
        finish(z)
        order = near[:-1][:4] + [last] + near[:-1][4:]
        for n, zp in enumerate(order):
            take_x(zp)
            if n >= 3:
                finish(order[n - 3])
        mark("take_peer")
        for zp in order[-min(3, len(order)) :]:
            finish(zp)

    def gather_drain(buf, sems, with_partner):
        part = buf.at[pl.ds(0, 2 * nz * NX - 1 - (not with_partner))]
        remote(part, part, sems.at[0], sems.at[1], left, c).wait_send()

    n_kv = nz * NX
    hrows = headf.shape[0]

    def widen(zp):
        for k in range(2 * NX):
            slot = 2 * NX * zp + k
            headsf[pl.ds(pl.multiple_of(slot * hrows, 8), hrows), :] = headb[slot].astype(F32)

    mark("gather_heads")
    gather(headb, hsem, True, widen)

    mark("project_out")
    for cc in range(2):
        for b in range(vb):
            at = (cc * vb + b) * LANES
            for i in range(2):
                lhs[i * n_kv : (i + 1) * n_kv, at : at + LANES] = headsf[
                    pl.ds(cc * hrows + i * (hrows // 2) + b, n_kv, stride=2 * hrows), :
                ].astype(BF16)
    remote(wo.at[other], wo.at[other], psem.at[2], psem.at[3], kv, other).wait_recv()
    projected = dot(lhs[...], wo[...].reshape(LANES, 2 * vb * LANES), ((1,), (1,)))
    for i in range(2):
        old = tokf[pl.ds(i, n_kv, stride=2), :]
        whole[2 * kv + i] = (old + projected[i * n_kv : (i + 1) * n_kv]).astype(BF16)

    mark("gather_after")
    in_mlp[0].wait()
    in_mlp[1].wait()
    sums = [
        jnp.zeros((2 * n_kv, LANES), F32),
        jnp.zeros(hidden.shape, F32),
        jnp.zeros(hidden.shape, F32),
    ]

    def multiply(zp):
        parts = []
        for xp in range(NX):
            k = zp * NX + xp
            rows = jnp.concatenate([whole[2 * k], whole[2 * k + 1]], axis=0).astype(F32)
            sums[0] = sums[0] + rows * rows
            parts.append((rows * mgainf[pl.ds(k, 1), :]).astype(BF16))
        rows = jnp.concatenate(parts, axis=1)
        cols = pl.ds(pl.multiple_of(zp * NX * LANES, LANES), NX * LANES)
        sums[1] = sums[1] + dot(rows, wmg[:, cols], ((1,), (1,)))
        sums[2] = sums[2] + dot(rows, wmu[:, cols], ((1,), (1,)))

    gather(whole, asem, False, multiply)

    mark("mlp_in")
    inv = lax.rsqrt(jnp.sum(sums[0], axis=1, keepdims=True) * (1.0 / width) + EPS)
    gate = sums[1] * inv
    up = sums[2] * inv
    hidden[...] = (gate / (1.0 + jnp.exp(-gate)) * up).astype(BF16)
    mark("mlp_down")
    in_mlp[2].wait()
    for g in range(2):
        for j in range(nh):
            cols = pl.ds(pl.multiple_of(zrel(g, j) * NX * LANES, LANES), NX * LANES)
            part = dot(hidden[...], wmd[:, cols]).astype(BF16)
            for xp in range(NX):
                for k in range(4):
                    dpart[k // 2, g, 2 * xp + k % 2, :, j * LANES : (j + 1) * LANES] = part[
                        k * n_kv // 2 : (k + 1) * n_kv // 2, xp * LANES : (xp + 1) * LANES
                    ]
        send(dpart.at[other, g], dpeer.at[g], psem.at[4], psem.at[5 + g], kv, other)
    mark("down_peer")

    def d_stage(g):
        return dx.at[g], dra.at[g], drs.at[g], drb.at[g], 4 + g

    for g in range(2):
        remote(dpeer.at[g], dpeer.at[g], psem.at[4], psem.at[5 + g], kv, other).wait_recv()
        for xp in (xo, xr, xl, x):
            for k in range(2):
                dx[g, 2 * xp + k] = (
                    dpart[c, g, 2 * xp + k].astype(F32) + dpeer[g, 2 * xp + k].astype(F32)
                ).astype(BF16)
        x_first(dx.at[g], dra.at[g], drb.at[g], 4 + g)
        x_direct(dx.at[g], dra.at[g], drb.at[g], 4 + g)
    mark("down_x")
    for g in range(2):
        x_second(*d_stage(g))
    low_lanes = lax.broadcasted_iota(jnp.int32, (n_kv // 2, LANES), 1) < LANES // 2

    def squeeze(top, bottom, right):
        if right:
            top = pltpu.roll(top, LANES // 2, 1)
        else:
            bottom = pltpu.roll(bottom, LANES // 2, 1)
        return jnp.where(low_lanes, top, bottom)

    mark("down_x2")
    for g in range(2):
        x_wait(drb.at[g], 4 + g)
        top, bottom = [x_sum(dx.at[g], drb.at[g], k) for k in range(2)]
        for j in by_distance(g):
            cols = slice(j * LANES, (j + 1) * LANES)
            slot = 2 * (g * nh + j)
            for cc in range(2):
                dzs[slot + cc] = squeeze(top[:, cols], bottom[:, cols], cc == 1).astype(BF16)
            if (g, j) == (self_g, self_j):
                dzr[slot + c] = dzs[slot + c]
                send(dzs.at[slot + other], dzr.at[slot + c], dzsem.at[0], dzsem.at[1], kv, other)
            else:
                for cc in (other, c):
                    send(
                        dzs.at[slot + cc],
                        dzr.at[slot + c],
                        dzsem.at[0],
                        dzsem.at[1],
                        zrel(g, j) * NX + x,
                        cc,
                    )
    mark("down_z")
    part = dzr.at[pl.ds(0, 2 * nz - 1)]
    remote(part, part, dzsem.at[0], dzsem.at[1], kv, other).wait_recv()
    mark("finish")
    for i in range(2):
        rows = whole[2 * kv + i].astype(F32)
        halves = rows[: n_kv // 2], rows[n_kv // 2 :]
        total = jnp.where(c == 1, squeeze(*halves, True), squeeze(*halves, False))
        for zp in range(nz):
            total = total + dzr[2 * zp + i].astype(F32)
        outf[pl.ds(i, n_kv // 2, stride=2), :] = total
        outf[pl.ds(i + n_kv, n_kv // 2, stride=2), :] = pltpu.roll(total, LANES // 2, 1)
    out[...] = outf[:, : LANES // 2].astype(BF16)
    mark("drain")
    remote(tok.at[c], tok.at[c], psem.at[0], psem.at[1], kv, other).wait_send()
    remote(wo.at[c], wo.at[c], psem.at[2], psem.at[3], kv, other).wait_send()
    for g in range(2):
        for col in range(2):
            stage = 2 * g + col
            x_drain((xa, xb)[col].at[g], stage)
            part = z_part(g, col)
            remote(part, part, zsem.at[stage, 0], zsem.at[stage, 1], left, c).wait_send()
        x_drain(dx.at[g], 4 + g)
    gather_drain(headb, hsem, True)
    gather_drain(whole, asem, False)
    remote(dpeer, dpeer, psem.at[4], psem.at[5], kv, other).wait_send()
    part = dzr.at[pl.ds(0, 2 * nz - 1)]
    remote(part, part, dzsem.at[0], dzsem.at[1], kv, other).wait_send()
    mark()


def shards(
    tokens,
    lengths,
    state,
    cache_keys,
    cache_values,
    cache_rates,
    attn_gain,
    w_query,
    w_key,
    w_value,
    w_gate,
    w_decay,
    head_gain,
    w_out,
    mlp_gain,
    w_mlp_gate,
    w_mlp_up,
    w_mlp_down,
):
    n_kv = lax.axis_size("kv")
    nz = n_kv // NX
    heads, dk, dv = state.shape[1], state.shape[2], state.shape[3]
    width = mlp_gain.shape[0]
    qb, vb = heads * dk // LANES, heads * dv // LANES
    half0, half1 = (3 * qb + 2) // 2, vb
    slots = -(-2 * max(half0, half1) // 8) * 8
    nh = nz // 2
    seqs = 2 * n_kv
    hrows = 2 * vb
    units = w_mlp_down.shape[0]
    cols5 = nh * LANES
    vmem, dma = pltpu.VMEM, pltpu.SemaphoreType.DMA
    bf, fl = BF16, F32
    scratch = [
        vmem((2, seqs, LANES // 2), bf),
        vmem((seqs, LANES), fl),
        vmem(w_query.shape, bf),
        vmem(w_key.shape, bf),
        vmem(w_decay.shape, bf),
        vmem(w_value.shape, bf),
        vmem(w_gate.shape, bf),
        vmem(state.shape, fl),
        vmem(cache_keys.shape, bf),
        vmem(cache_values.shape, bf),
        vmem(cache_rates.shape, fl),
        vmem((2,) + w_out.shape[::-1], bf),
        vmem(w_mlp_gate.shape[::-1], bf),
        vmem(w_mlp_up.shape[::-1], bf),
        vmem(w_mlp_down.shape, bf),
        vmem((2, NX * 2, nz, half0 * LANES), bf),
        vmem((2, NX * 2, nz, half1 * LANES), bf),
        vmem((2, 2, nz, half0 * LANES), bf),
        vmem((2, 2, nz, half1 * LANES), bf),
        vmem((2, 2, nz, half0 * LANES), bf),
        vmem((2, 2, nz, half1 * LANES), bf),
        vmem((2, 4, nz, half0 * LANES), bf),
        vmem((2, 4, nz, half1 * LANES), bf),
        vmem((nz * slots, LANES), fl),
        vmem((4, nh, 2 * slots, LANES), bf),
        vmem((4, nh, 2 * slots, LANES), bf),
        vmem(state.shape, bf),
        vmem((2 * slots, LANES), fl),
        vmem((2 * slots, LANES), fl),
        vmem((2 * qb, LANES), fl),
        vmem((2 * vb, LANES), fl),
        vmem((vb, LANES), fl),
        vmem((hrows, LANES), fl),
        vmem((2 * n_kv, hrows, LANES), bf),
        vmem((n_kv * 2 * hrows, LANES), fl),
        vmem((seqs, 2 * vb * LANES), bf),
        vmem((2 * n_kv, n_kv, LANES), bf),
        vmem((seqs, units), bf),
        vmem((2, 2, NX * 2, n_kv // 2, cols5), bf),
        vmem((2, NX * 2, n_kv // 2, cols5), bf),
        vmem((2, NX * 2, n_kv // 2, cols5), bf),
        vmem((2, 2, n_kv // 2, cols5), bf),
        vmem((2, 2, n_kv // 2, cols5), bf),
        vmem((2, 4, n_kv // 2, cols5), bf),
        vmem((2 * nz, n_kv // 2, LANES), bf),
        vmem((2 * nz, n_kv // 2, LANES), bf),
        vmem((seqs, LANES), fl),
        vmem((1, LANES), bf),
        vmem((heads, dv), bf),
        vmem((n_kv, LANES), bf),
        vmem((n_kv, LANES), fl),
        pltpu.SMEM((2,), jnp.int32),
        dma((18,)),
        dma((7,)),
        dma((6, 4)),
        dma((4, 2)),
        dma((1 + 3 * nz,)),
        dma((1 + 3 * nz,)),
        dma((2,)),
    ]
    anywhere = pl.BlockSpec(memory_space=pl.ANY)
    in_vmem = pl.BlockSpec(memory_space=pltpu.VMEM)
    specs = [anywhere] * 18
    return pl.pallas_call(
        functools.partial(kernel, (nz, qb, vb, dk, width)),
        out_shape=jax.ShapeDtypeStruct(tokens.shape, BF16),
        in_specs=specs,
        out_specs=in_vmem,
        scratch_shapes=scratch,
        compiler_params=pltpu.CompilerParams(collective_id=0, has_side_effects=True),
        name="layer",
    )(
        tokens,
        lengths,
        state,
        cache_keys,
        cache_values,
        cache_rates,
        attn_gain.reshape(1, -1),
        w_query,
        w_key,
        w_value,
        w_gate,
        w_decay,
        head_gain,
        w_out.T,
        mlp_gain.reshape(-1, LANES),
        w_mlp_gate.T,
        w_mlp_up.T,
        w_mlp_down,
    )


def solution(mesh):
    placed = (
        P("dp", ("kv", "tp")),
        P(("dp", "kv")),
        P(("dp", "kv"), "tp", None, None),
        P(("dp", "kv"), "tp", None, None),
        P(("dp", "kv"), "tp", None, None),
        P(("dp", "kv"), "tp", None, None),
        P("kv"),
        P("kv", "tp"),
        P("kv", "tp"),
        P("kv", "tp"),
        P("kv", "tp"),
        P("kv", "tp"),
        P("tp", None),
        P(None, ("kv", "tp")),
        P(),
        P(None, ("kv", "tp")),
        P(None, ("kv", "tp")),
        P(("kv", "tp"), None),
    )
    return jax.shard_map(
        shards, mesh=mesh, in_specs=placed, out_specs=P("dp", ("kv", "tp")), check_vma=False
    )
```

```python
import functools

import jax
import jax.numpy as jnp
from jax import lax
from jax.experimental import pallas as pl
from jax.experimental.pallas import tpu as pltpu
from jax.sharding import PartitionSpec as P

EPS = 1e-06
GATE_NORM = 16.0
NX = 4
LANES = 128
MESH = pl.DeviceIdType.MESH
F32 = jnp.float32
BF16 = jnp.bfloat16


def dot(a, b, dims=((1,), (0,))):
    return lax.dot_general(a, b, (dims, ((), ())), preferred_element_type=F32)


def high_low(a):
    high = a.astype(BF16)
    return high, (a - high.astype(F32)).astype(BF16)


def kernel(
    sizes,
    tokens,
    lengths,
    state,
    cache_keys,
    cache_values,
    cache_rates,
    attn_gain,
    w_query,
    w_key,
    w_value,
    w_gate,
    w_decay,
    head_gain,
    w_out,
    mlp_gain,
    w_mlp_gate,
    w_mlp_up,
    w_mlp_down,
    out,
    tok,
    tokf,
    wq,
    wk,
    wd,
    wv,
    wg,
    st,
    ck,
    cv,
    cr,
    wo,
    wmg,
    wmu,
    wmd,
    xa,
    xb,
    xfa,
    xfb,
    xsa,
    xsb,
    xba,
    xbb,
    zf,
    zs,
    zr,
    memory,
    pack0,
    pack1,
    qe,
    att,
    hg,
    headf,
    headb,
    headsf,
    lhs,
    whole,
    hidden,
    dpart,
    dpeer,
    dx,
    drb,
    dzs,
    dzr,
    outf,
    again,
    hgain,
    mgain,
    mgainf,
    lens,
    lsem,
    psem,
    xsem,
    zsem,
    hsem,
    asem,
    dxsem,
    dzsem,
):
    nz, qb, vb, dk, width = sizes
    nh = nz // 2
    kv = lax.axis_index("kv")
    c = lax.axis_index("tp")
    other = 1 - c
    z = kv // NX
    x = kv % NX
    xr = (x + 1) % NX
    xl = (x + NX - 1) % NX
    xo = (x + 2) % NX
    steps = [((d + 1) // 2) * (1 if d % 2 else -1) for d in range(1, nz)]
    far = [(z + (s % nz)) % nz for s in steps][::-1]
    near = [(z + (s % nz)) % nz for s in steps]
    sides = [(x + d) % NX for d in (2, 1, 3)]

    def turn(g, j):
        return (nz // 4 + g * nh + j) % nz

    def zrel(g, j):
        return (z + turn(g, j)) % nz

    def by_distance(g):
        return sorted(range(nh), key=lambda j: -min(turn(g, j), nz - turn(g, j)))

    self_g, self_j = divmod((nz - nz // 4) % nz, nh)

    def local(i, src, dst):
        copy = pltpu.make_async_copy(src, dst, lsem.at[i])
        copy.start()
        return copy

    def remote(src, dst, send, recv, to_kv, to_tp):
        return pltpu.make_async_remote_copy(
            src_ref=src,
            dst_ref=dst,
            send_sem=send,
            recv_sem=recv,
            device_id={"kv": to_kv, "tp": to_tp},
            device_id_type=MESH,
        )

    scopes = []

    def mark(name=None):
        if scopes:
            scopes.pop().__exit__(None, None, None)
        if name:
            scopes.append(jax.named_scope(name))
            scopes[-1].__enter__()

    def send(*args):
        remote(*args).start()

    mark("barrier")
    barrier = pltpu.get_barrier_semaphore()

    def greet(to_kv, to_tp):
        pl.semaphore_signal(
            barrier, inc=1, device_id={"kv": to_kv, "tp": to_tp}, device_id_type=MESH
        )

    for zp in far:
        greet(zp * NX + x, c)
        greet(zp * NX + x, other)
    for xp in sides:
        greet(z * NX + xp, c)
    greet(kv, other)
    mark("load")
    in_tok = local(0, tokens, tok.at[c])
    in_small = [
        local(14 + i, src, dst)
        for i, (src, dst) in enumerate(
            ((attn_gain, again), (head_gain, hgain), (mlp_gain, mgain), (lengths, lens))
        )
    ]
    in_w = [
        local(1 + i, src, dst)
        for i, (src, dst) in enumerate(
            ((w_query, wq), (w_key, wk), (w_decay, wd), (w_value, wv), (w_gate, wg))
        )
    ]
    in_cache = [
        local(6 + i, src, dst)
        for i, (src, dst) in enumerate(((cache_rates, cr), (cache_keys, ck), (cache_values, cv)))
    ]
    in_state = local(9, state, st)
    in_out = local(10, w_out, wo.at[c])
    in_mlp = [
        local(11 + i, src, dst)
        for i, (src, dst) in enumerate(((w_mlp_gate, wmg), (w_mlp_up, wmu), (w_mlp_down, wmd)))
    ]

    zf[...] = jnp.zeros_like(zf)
    pl.semaphore_wait(barrier, 2 * len(far) + len(sides) + 1)

    mark("tokens")
    in_tok.wait()
    send(tok.at[c], tok.at[c], psem.at[0], psem.at[1], kv, other)
    in_out.wait()
    send(wo.at[c], wo.at[c], psem.at[2], psem.at[3], kv, other)
    remote(tok.at[other], tok.at[other], psem.at[0], psem.at[1], kv, other).wait_recv()
    tokf[...] = jnp.concatenate([tok[0].astype(F32), tok[1].astype(F32)], axis=1)
    block = []
    for xp in range(NX):
        pair = [
            pltpu.roll(
                tokf[pl.ds(2 * xp + i, nz, stride=2 * NX), :], (2 * nz - z - nz // 4) % nz, 0
            )
            for i in range(2)
        ]
        for g in range(2):
            block += [rows[g * nh : (g + 1) * nh] for rows in pair]
    block = jnp.concatenate(block, axis=0)
    in_small[0].wait()
    squares = jnp.sum(block * block, axis=1, keepdims=True)
    scaled = (block * again[...].astype(F32)).astype(BF16)

    def put(target, b, values):
        half = target.shape[3] // LANES
        at = (b % half) * LANES
        for xp in range(NX):
            for g in range(2):
                row = (2 * xp + g) * nz
                target[g, 2 * xp + b // half, :, at : at + LANES] = values[row : row + nz].astype(
                    BF16
                )

    def project(copy, weight, target, start):
        copy.wait()
        part = dot(scaled, weight[...])
        for b in range(weight.shape[1] // LANES):
            put(target, start + b, part[:, b * LANES : (b + 1) * LANES])

    left, right = z * NX + xl, z * NX + xr

    def x_first(src, first, back, stage):
        out_sem, in_left, in_right, in_back = [xsem.at[stage, k] for k in range(4)]
        send(src.at[2 * xo], first.at[0], out_sem, in_left, right, c)
        send(src.at[2 * xo + 1], first.at[1], out_sem, in_right, left, c)

    def x_direct(src, first, back, stage):
        out_sem, in_left, in_right, in_back = [xsem.at[stage, k] for k in range(4)]
        send(src.at[2 * xr + 1], back.at[1], out_sem, in_back, right, c)
        send(src.at[2 * xl], back.at[2], out_sem, in_back, left, c)

    def x_second(src, first, relay, back, stage):
        out_sem, in_left, in_right, in_back = [xsem.at[stage, k] for k in range(4)]
        remote(first.at[0], first.at[0], out_sem, in_left, left, c).wait_recv()
        relay[0] = (src[2 * xr].astype(F32) + first[0].astype(F32)).astype(BF16)
        send(relay.at[0], back.at[0], out_sem, in_back, right, c)
        remote(first.at[1], first.at[1], out_sem, in_right, right, c).wait_recv()
        relay[1] = (src[2 * xl + 1].astype(F32) + first[1].astype(F32)).astype(BF16)
        send(relay.at[1], back.at[3], out_sem, in_back, left, c)

    def x_wait(back, stage):
        remote(back, back, xsem.at[stage, 0], xsem.at[stage, 3], left, c).wait_recv()

    def x_drain(src, stage):
        part = src.at[pl.ds(0, 6)]
        remote(part, part, xsem.at[stage, 0], xsem.at[stage, 3], left, c).wait_send()

    def x_sum(src, back, half):
        return (
            src[2 * x + half].astype(F32) + back[half].astype(F32) + back[2 + half].astype(F32)
        )

    def x_stage(g, col):
        src, first, relay, back = ((xa, xfa, xsa, xba), (xb, xfb, xsb, xbb))[col]
        return src.at[g], first.at[g], relay.at[g], back.at[g], 2 * g + col

    def x_one(g, col):
        src, first, relay, back, stage = x_stage(g, col)
        x_first(src, first, back, stage)

    def x_ind(g, col):
        src, first, relay, back, stage = x_stage(g, col)
        x_direct(src, first, back, stage)

    project(in_w[0], wq, xa, 0)
    project(in_w[1], wk, xa, qb)
    project(in_w[2], wd, xa, 2 * qb)
    put(xa, 3 * qb, jnp.broadcast_to(squares, (squares.shape[0], LANES)))
    for b in range(3 * qb + 1, 2 * (xa.shape[3] // LANES)):
        put(xa, b, jnp.zeros((squares.shape[0], LANES), F32))
    x_one(0, 0)
    mark("project_b")
    project(in_w[3], wv, xb, 0)
    project(in_w[4], wg, xb, vb)
    x_one(0, 1)
    x_ind(0, 0)
    x_ind(0, 1)
    x_one(1, 0)
    x_one(1, 1)

    span = ck.shape[2]
    hb = vb // 2
    later = (
        lax.broadcasted_iota(jnp.int32, (span, span), 1)
        > lax.broadcasted_iota(jnp.int32, (span, span), 0)
    ).astype(BF16)
    ones = jnp.ones((span, LANES), BF16)
    slots = lax.broadcasted_iota(jnp.int32, (span, 1), 0)

    def fold(i, h):
        live = (slots < lens[i]).astype(F32)
        rates = cr[i, h] * live
        high, low = high_low(rates)
        rest = dot(later, high) + dot(later, low)
        keys = jnp.exp(-rest) * ck[i, h].astype(F32) * live
        shrink = jnp.exp(-(dot(high, ones, ((0,), (0,))) + dot(low, ones, ((0,), (0,)))))
        high, low = high_low(keys)
        value = cv[i, h]
        inner = dot(high, value, ((0,), (0,))) + dot(low, value, ((0,), (0,)))
        for b in range(hb):
            cols = slice(b * LANES, (b + 1) * LANES)
            memory[i, h, :, cols] = (st[i, h, :, cols] * shrink + inner[:, cols]).astype(BF16)

    mark("fold_a")
    for copy in in_small[1:]:
        copy.wait()
    mgainf[...] = mgain[...].astype(F32)
    for h in range(2):
        for b in range(hb):
            hg[h * hb + b : h * hb + b + 1, :] = hgain[
                h : h + 1, b * LANES : (b + 1) * LANES
            ].astype(F32)
    for copy in in_cache:
        copy.wait()
    in_state.wait()
    for h in range(2):
        fold(0, h)
    mark("x_second_a")
    x_second(*x_stage(0, 0))
    x_second(*x_stage(0, 1))
    mark("x_second_b")
    x_ind(1, 0)
    x_ind(1, 1)
    x_second(*x_stage(1, 0))
    x_second(*x_stage(1, 1))

    slots_row = zf.shape[0] // (2 * nh)

    def z_send(g, col):
        src, first, relay, back, stage = x_stage(g, col)
        half = src.shape[2] // LANES
        x_wait(back, stage)
        for hh in (0, 1):
            total = x_sum(src, back, hh)
            for b in range(half):
                for i in range(2):
                    zf[pl.ds(i * slots_row + hh * half + b, nh, stride=2 * slots_row), :] = total[
                        i * nh : (i + 1) * nh, b * LANES : (b + 1) * LANES
                    ]
        for j in by_distance(g):
            zs[stage, j] = zf[j * 2 * slots_row : (j + 1) * 2 * slots_row, :].astype(BF16)
            if (g, j) != (self_g, self_j):
                send(
                    zs.at[stage, j],
                    zr.at[stage, j],
                    zsem.at[stage, 0],
                    zsem.at[stage, 1],
                    zrel(g, j) * NX + x,
                    c,
                )

    def z_part(g, col):
        return zr.at[2 * g + col, pl.ds(0, nh - (g == self_g))]

    def z_sum(col):
        for g in range(2):
            part = z_part(g, col)
            stage = 2 * g + col
            remote(part, part, zsem.at[stage, 0], zsem.at[stage, 1], left, c).wait_recv()
        total = zs[2 * self_g + col, self_j].astype(F32)
        for g in range(2):
            for j in range(nh):
                if (g, j) != (self_g, self_j):
                    total = total + zr[2 * g + col, j].astype(F32)
        return total

    mark("z_send_a")
    z_send(0, 0)
    z_send(0, 1)
    mark("fold_b")
    for h in range(2):
        fold(1, h)
    mark("z_send_b")
    z_send(1, 0)
    z_send(1, 1)

    mark("z_wait_a")
    pack0[...] = z_sum(0)
    mark("heads_a")
    own = []
    inverse = []
    qh = qb // 2
    for i in range(2):
        at = i * slots_row
        inv = lax.rsqrt(pack0[at + 3 * qb : at + 3 * qb + 1, :] * (1.0 / width) + EPS)
        inverse.append(inv)
        query = pack0[at : at + qb, :] * inv * dk ** (-0.5)
        key = pack0[at + qb : at + 2 * qb, :] * inv
        raw = pack0[at + 2 * qb : at + 3 * qb, :] * inv
        decay = (jnp.minimum(raw, 0.0) - jnp.log1p(jnp.exp(-jnp.abs(raw)))) / GATE_NORM
        qe[i * qb : (i + 1) * qb, :] = query * jnp.exp(decay)
        both = query * key
        for h in range(2):
            part = jnp.sum(both[h * qh : (h + 1) * qh, :], axis=0, keepdims=True)
            own.append(jnp.sum(part, axis=1, keepdims=True))
    for i in range(2):
        for h in range(2):
            row = jnp.concatenate(
                [qe[i * qb + h * qh + b : i * qb + h * qh + b + 1, :] for b in range(qh)], axis=1
            )
            high, low = high_low(row)
            got = dot(jnp.concatenate([high, low], axis=0), memory[i, h])
            got = got[0:1] + got[1:2]
            for b in range(hb):
                att[i * vb + h * hb + b : i * vb + h * hb + b + 1, :] = got[
                    :, b * LANES : (b + 1) * LANES
                ]
    mark("z_wait_b")
    pack1[...] = z_sum(1)
    for i in range(2):
        at = i * slots_row
        if i == 0:
            mark("heads_b")
        value = pack1[at : at + vb, :] * inverse[i]
        gate = pack1[at + vb : at + 2 * vb, :] * inverse[i]
        attended = att[i * vb : (i + 1) * vb, :]
        for h in range(2):
            part = slice(h * hb, (h + 1) * hb)
            full = attended[part] + own[2 * i + h] * value[part]
            mean = jnp.sum(jnp.sum(full * full, axis=0, keepdims=True), axis=1, keepdims=True)
            norm = full * lax.rsqrt(mean * (1.0 / (hb * LANES)) + EPS) * hg[part, :]
            g = gate[part]
            headf[i * (headf.shape[0] // 2) + h * hb : i * (headf.shape[0] // 2) + (h + 1) * hb, :] = (
                g / (1.0 + jnp.exp(-g)) * norm
            )
    headb[2 * kv + c] = headf[...].astype(BF16)

    def gather(buf, sems, with_partner, consume):
        out_sem = sems.at[0]
        mine = buf.at[2 * kv + c]

        def in_z(zp):
            return sems.at[1 + zp]

        def in_x(zp):
            return sems.at[1 + nz + zp]

        def in_peer(zp):
            return sems.at[1 + 2 * nz + zp]

        for zp in far:
            send(mine, mine, out_sem, in_z(z), zp * NX + x, c)
        for xp in sides:
            send(mine, mine, out_sem, in_x(z), z * NX + xp, c)
        if with_partner:
            send(mine, mine, out_sem, in_peer(z), kv, other)

        def take_z(zp):
            origin = zp * NX + x
            slot = buf.at[2 * origin + c]
            remote(slot, slot, out_sem, in_z(zp), origin, c).wait_recv()
            for xp in sides:
                send(slot, slot, out_sem, in_x(zp), z * NX + xp, c)
            send(slot, slot, out_sem, in_peer(zp), kv, other)

        def take_x(zp):
            part = buf.at[pl.ds(0, NX - 1)]
            remote(part, part, out_sem, in_x(zp), left, c).wait_recv()
            for xp in sides[::-1]:
                slot = buf.at[2 * (zp * NX + xp) + c]
                send(slot, slot, out_sem, in_peer(zp), kv, other)

        def finish(zp):
            part = buf.at[pl.ds(0, NX - (zp is z and not with_partner))]
            remote(part, part, out_sem, in_peer(zp), kv, other).wait_recv()
            consume(zp)

        for zp in near:
            take_z(zp)
        mark("take_x")
        split = (len(near) + 1) // 2
        for zp in [z] + near[:split]:
            take_x(zp)
        finish(z)
        for zp in near[: split // 2]:
            finish(zp)
        for zp in near[split:]:
            take_x(zp)
        mark("take_peer")
        for zp in near[split // 2 :]:
            finish(zp)

    def gather_drain(buf, sems, with_partner):
        part = buf.at[pl.ds(0, 2 * nz * NX - 1 - (not with_partner))]
        remote(part, part, sems.at[0], sems.at[1], left, c).wait_send()

    n_kv = nz * NX
    hrows = headf.shape[0]

    def widen(zp):
        for k in range(2 * NX):
            slot = 2 * NX * zp + k
            headsf[pl.ds(pl.multiple_of(slot * hrows, 8), hrows), :] = headb[slot].astype(F32)

    mark("gather_heads")
    gather(headb, hsem, True, widen)

    mark("project_out")
    for cc in range(2):
        for b in range(vb):
            at = (cc * vb + b) * LANES
            for i in range(2):
                lhs[i * n_kv : (i + 1) * n_kv, at : at + LANES] = headsf[
                    pl.ds(cc * hrows + i * (hrows // 2) + b, n_kv, stride=2 * hrows), :
                ].astype(BF16)
    remote(wo.at[other], wo.at[other], psem.at[2], psem.at[3], kv, other).wait_recv()
    projected = dot(lhs[...], wo[...].reshape(LANES, 2 * vb * LANES), ((1,), (1,)))
    for i in range(2):
        old = tokf[pl.ds(i, n_kv, stride=2), :]
        whole[2 * kv + i] = (old + projected[i * n_kv : (i + 1) * n_kv]).astype(BF16)

    mark("gather_after")
    in_mlp[0].wait()
    in_mlp[1].wait()
    sums = [
        jnp.zeros((2 * n_kv, LANES), F32),
        jnp.zeros(hidden.shape, F32),
        jnp.zeros(hidden.shape, F32),
    ]

    def multiply(zp):
        parts = []
        for xp in range(NX):
            k = zp * NX + xp
            rows = jnp.concatenate([whole[2 * k], whole[2 * k + 1]], axis=0).astype(F32)
            sums[0] = sums[0] + rows * rows
            parts.append((rows * mgainf[pl.ds(k, 1), :]).astype(BF16))
        rows = jnp.concatenate(parts, axis=1)
        cols = pl.ds(pl.multiple_of(zp * NX * LANES, LANES), NX * LANES)
        sums[1] = sums[1] + dot(rows, wmg[:, cols], ((1,), (1,)))
        sums[2] = sums[2] + dot(rows, wmu[:, cols], ((1,), (1,)))

    gather(whole, asem, False, multiply)

    mark("mlp_in")
    inv = lax.rsqrt(jnp.sum(sums[0], axis=1, keepdims=True) * (1.0 / width) + EPS)
    gate = sums[1] * inv
    up = sums[2] * inv
    hidden[...] = (gate / (1.0 + jnp.exp(-gate)) * up).astype(BF16)
    mark("mlp_down")
    in_mlp[2].wait()
    for g in range(2):
        for j in range(nh):
            cols = pl.ds(pl.multiple_of(zrel(g, j) * NX * LANES, LANES), NX * LANES)
            part = dot(hidden[...], wmd[:, cols]).astype(BF16)
            for xp in range(NX):
                for k in range(4):
                    dpart[k // 2, g, 2 * xp + k % 2, :, j * LANES : (j + 1) * LANES] = part[
                        k * n_kv // 2 : (k + 1) * n_kv // 2, xp * LANES : (xp + 1) * LANES
                    ]
        send(dpart.at[other, g], dpeer.at[g], psem.at[4], psem.at[5 + g], kv, other)
    mark("down_peer")

    for g in range(2):
        remote(dpeer.at[g], dpeer.at[g], psem.at[4], psem.at[5 + g], kv, other).wait_recv()
        for n, xp in enumerate(sides + [x]):
            for k in range(2):
                dx[g, 2 * xp + k] = (
                    dpart[c, g, 2 * xp + k].astype(F32) + dpeer[g, 2 * xp + k].astype(F32)
                ).astype(BF16)
            if n < NX - 1:
                send(
                    dx.at[g, pl.ds(2 * xp, 2)],
                    drb.at[g, pl.ds(2 * n, 2)],
                    dxsem.at[g, 0],
                    dxsem.at[g, 1],
                    z * NX + xp,
                    c,
                )
    low_lanes = lax.broadcasted_iota(jnp.int32, (n_kv // 2, LANES), 1) < LANES // 2

    def squeeze(top, bottom, right):
        if right:
            top = pltpu.roll(top, LANES // 2, 1)
        else:
            bottom = pltpu.roll(bottom, LANES // 2, 1)
        return jnp.where(low_lanes, top, bottom)

    mark("down_x2")
    for g in range(2):
        part = drb.at[g]
        remote(part, part, dxsem.at[g, 0], dxsem.at[g, 1], left, c).wait_recv()
        top, bottom = [
            dx[g, 2 * x + k].astype(F32)
            + sum(drb[g, 2 * n + k].astype(F32) for n in range(NX - 1))
            for k in range(2)
        ]
        for j in by_distance(g):
            cols = slice(j * LANES, (j + 1) * LANES)
            slot = 2 * (g * nh + j)
            for cc in range(2):
                dzs[slot + cc] = squeeze(top[:, cols], bottom[:, cols], cc == 1).astype(BF16)
            if (g, j) == (self_g, self_j):
                dzr[slot + c] = dzs[slot + c]
                send(dzs.at[slot + other], dzr.at[slot + c], dzsem.at[0], dzsem.at[1], kv, other)
            else:
                for cc in (other, c):
                    send(
                        dzs.at[slot + cc],
                        dzr.at[slot + c],
                        dzsem.at[0],
                        dzsem.at[1],
                        zrel(g, j) * NX + x,
                        cc,
                    )
    mark("down_z")
    part = dzr.at[pl.ds(0, 2 * nz - 1)]
    remote(part, part, dzsem.at[0], dzsem.at[1], kv, other).wait_recv()
    mark("finish")
    for i in range(2):
        rows = whole[2 * kv + i].astype(F32)
        halves = rows[: n_kv // 2], rows[n_kv // 2 :]
        total = jnp.where(c == 1, squeeze(*halves, True), squeeze(*halves, False))
        for zp in range(nz):
            total = total + dzr[2 * zp + i].astype(F32)
        outf[pl.ds(i, n_kv // 2, stride=2), :] = total
        outf[pl.ds(i + n_kv, n_kv // 2, stride=2), :] = pltpu.roll(total, LANES // 2, 1)
    out[...] = outf[:, : LANES // 2].astype(BF16)
    mark("drain")
    remote(tok.at[c], tok.at[c], psem.at[0], psem.at[1], kv, other).wait_send()
    remote(wo.at[c], wo.at[c], psem.at[2], psem.at[3], kv, other).wait_send()
    for g in range(2):
        for col in range(2):
            stage = 2 * g + col
            x_drain((xa, xb)[col].at[g], stage)
            part = z_part(g, col)
            remote(part, part, zsem.at[stage, 0], zsem.at[stage, 1], left, c).wait_send()
        part = drb.at[g]
        remote(part, part, dxsem.at[g, 0], dxsem.at[g, 1], left, c).wait_send()
    gather_drain(headb, hsem, True)
    gather_drain(whole, asem, False)
    remote(dpeer, dpeer, psem.at[4], psem.at[5], kv, other).wait_send()
    part = dzr.at[pl.ds(0, 2 * nz - 1)]
    remote(part, part, dzsem.at[0], dzsem.at[1], kv, other).wait_send()
    mark()


def shards(
    tokens,
    lengths,
    state,
    cache_keys,
    cache_values,
    cache_rates,
    attn_gain,
    w_query,
    w_key,
    w_value,
    w_gate,
    w_decay,
    head_gain,
    w_out,
    mlp_gain,
    w_mlp_gate,
    w_mlp_up,
    w_mlp_down,
):
    n_kv = lax.axis_size("kv")
    nz = n_kv // NX
    heads, dk, dv = state.shape[1], state.shape[2], state.shape[3]
    width = mlp_gain.shape[0]
    qb, vb = heads * dk // LANES, heads * dv // LANES
    half0, half1 = (3 * qb + 2) // 2, vb
    slots = -(-2 * max(half0, half1) // 8) * 8
    nh = nz // 2
    seqs = 2 * n_kv
    hrows = 2 * vb
    units = w_mlp_down.shape[0]
    cols5 = nh * LANES
    vmem, dma = pltpu.VMEM, pltpu.SemaphoreType.DMA
    bf, fl = BF16, F32
    scratch = [
        vmem((2, seqs, LANES // 2), bf),
        vmem((seqs, LANES), fl),
        vmem(w_query.shape, bf),
        vmem(w_key.shape, bf),
        vmem(w_decay.shape, bf),
        vmem(w_value.shape, bf),
        vmem(w_gate.shape, bf),
        vmem(state.shape, fl),
        vmem(cache_keys.shape, bf),
        vmem(cache_values.shape, bf),
        vmem(cache_rates.shape, fl),
        vmem((2,) + w_out.shape[::-1], bf),
        vmem(w_mlp_gate.shape[::-1], bf),
        vmem(w_mlp_up.shape[::-1], bf),
        vmem(w_mlp_down.shape, bf),
        vmem((2, NX * 2, nz, half0 * LANES), bf),
        vmem((2, NX * 2, nz, half1 * LANES), bf),
        vmem((2, 2, nz, half0 * LANES), bf),
        vmem((2, 2, nz, half1 * LANES), bf),
        vmem((2, 2, nz, half0 * LANES), bf),
        vmem((2, 2, nz, half1 * LANES), bf),
        vmem((2, 4, nz, half0 * LANES), bf),
        vmem((2, 4, nz, half1 * LANES), bf),
        vmem((nz * slots, LANES), fl),
        vmem((4, nh, 2 * slots, LANES), bf),
        vmem((4, nh, 2 * slots, LANES), bf),
        vmem(state.shape, bf),
        vmem((2 * slots, LANES), fl),
        vmem((2 * slots, LANES), fl),
        vmem((2 * qb, LANES), fl),
        vmem((2 * vb, LANES), fl),
        vmem((vb, LANES), fl),
        vmem((hrows, LANES), fl),
        vmem((2 * n_kv, hrows, LANES), bf),
        vmem((n_kv * 2 * hrows, LANES), fl),
        vmem((seqs, 2 * vb * LANES), bf),
        vmem((2 * n_kv, n_kv, LANES), bf),
        vmem((seqs, units), bf),
        vmem((2, 2, NX * 2, n_kv // 2, cols5), bf),
        vmem((2, NX * 2, n_kv // 2, cols5), bf),
        vmem((2, NX * 2, n_kv // 2, cols5), bf),
        vmem((2, 2 * (NX - 1), n_kv // 2, cols5), bf),
        vmem((2 * nz, n_kv // 2, LANES), bf),
        vmem((2 * nz, n_kv // 2, LANES), bf),
        vmem((seqs, LANES), fl),
        vmem((1, LANES), bf),
        vmem((heads, dv), bf),
        vmem((n_kv, LANES), bf),
        vmem((n_kv, LANES), fl),
        pltpu.SMEM((2,), jnp.int32),
        dma((18,)),
        dma((7,)),
        dma((4, 4)),
        dma((4, 2)),
        dma((1 + 3 * nz,)),
        dma((1 + 3 * nz,)),
        dma((2, 2)),
        dma((2,)),
    ]
    anywhere = pl.BlockSpec(memory_space=pl.ANY)
    in_vmem = pl.BlockSpec(memory_space=pltpu.VMEM)
    specs = [anywhere] * 18
    return pl.pallas_call(
        functools.partial(kernel, (nz, qb, vb, dk, width)),
        out_shape=jax.ShapeDtypeStruct(tokens.shape, BF16),
        in_specs=specs,
        out_specs=in_vmem,
        scratch_shapes=scratch,
        compiler_params=pltpu.CompilerParams(collective_id=0, has_side_effects=True),
        name="layer",
    )(
        tokens,
        lengths,
        state,
        cache_keys,
        cache_values,
        cache_rates,
        attn_gain.reshape(1, -1),
        w_query,
        w_key,
        w_value,
        w_gate,
        w_decay,
        head_gain,
        w_out.T,
        mlp_gain.reshape(-1, LANES),
        w_mlp_gate.T,
        w_mlp_up.T,
        w_mlp_down,
    )


def solution(mesh):
    placed = (
        P("dp", ("kv", "tp")),
        P(("dp", "kv")),
        P(("dp", "kv"), "tp", None, None),
        P(("dp", "kv"), "tp", None, None),
        P(("dp", "kv"), "tp", None, None),
        P(("dp", "kv"), "tp", None, None),
        P("kv"),
        P("kv", "tp"),
        P("kv", "tp"),
        P("kv", "tp"),
        P("kv", "tp"),
        P("kv", "tp"),
        P("tp", None),
        P(None, ("kv", "tp")),
        P(),
        P(None, ("kv", "tp")),
        P(None, ("kv", "tp")),
        P(("kv", "tp"), None),
    )
    return jax.shard_map(
        shards, mesh=mesh, in_specs=placed, out_specs=P("dp", ("kv", "tp")), check_vma=False
    )
```

```python
import functools

import jax
import jax.numpy as jnp
from jax import lax
from jax.experimental import pallas as pl
from jax.experimental.pallas import tpu as pltpu
from jax.sharding import PartitionSpec as P

EPS = 1e-06
GATE_NORM = 16.0
NX = 4
LANES = 128
MESH = pl.DeviceIdType.MESH
F32 = jnp.float32
BF16 = jnp.bfloat16


def dot(a, b, dims=((1,), (0,))):
    return lax.dot_general(a, b, (dims, ((), ())), preferred_element_type=F32)


def high_low(a):
    high = a.astype(BF16)
    return high, (a - high.astype(F32)).astype(BF16)


def kernel(
    sizes,
    tokens,
    lengths,
    state,
    cache_keys,
    cache_values,
    cache_rates,
    attn_gain,
    w_query,
    w_key,
    w_value,
    w_gate,
    w_decay,
    head_gain,
    w_out,
    mlp_gain,
    w_mlp_gate,
    w_mlp_up,
    w_mlp_down,
    out,
    tok,
    tokf,
    wq,
    wk,
    wd,
    wv,
    wg,
    st,
    ck,
    cv,
    cr,
    wo,
    wmg,
    wmu,
    wmd,
    xa,
    xb,
    xfa,
    xfb,
    xsa,
    xsb,
    xba,
    xbb,
    zf,
    zs,
    zr,
    memory,
    pack0,
    pack1,
    qe,
    att,
    hg,
    headf,
    headb,
    headsf,
    lhs,
    whole,
    hidden,
    dpart,
    dpeer,
    dx,
    drb,
    dzs,
    dzr,
    outf,
    again,
    hgain,
    mgain,
    mgainf,
    lens,
    lsem,
    psem,
    xsem,
    zsem,
    hsem,
    asem,
    dxsem,
    dzsem,
    csem,
):
    nz, qb, vb, dk, width = sizes
    nh = nz // 2
    kv = lax.axis_index("kv")
    c = lax.axis_index("tp")
    other = 1 - c
    z = kv // NX
    x = kv % NX
    xr = (x + 1) % NX
    xl = (x + NX - 1) % NX
    xo = (x + 2) % NX
    steps = [((d + 1) // 2) * (1 if d % 2 else -1) for d in range(1, nz)]
    far = [(z + (s % nz)) % nz for s in steps][::-1]
    near = [(z + (s % nz)) % nz for s in steps]
    sides = [(x + d) % NX for d in (2, 1, 3)]

    def turn(g, j):
        return (nz // 4 + g * nh + j) % nz

    def zrel(g, j):
        return (z + turn(g, j)) % nz

    def by_distance(g):
        return sorted(range(nh), key=lambda j: -min(turn(g, j), nz - turn(g, j)))

    self_g, self_j = divmod((nz - nz // 4) % nz, nh)

    def local(i, src, dst):
        copy = pltpu.make_async_copy(src, dst, lsem.at[i])
        copy.start()
        return copy

    def remote(src, dst, send, recv, to_kv, to_tp):
        return pltpu.make_async_remote_copy(
            src_ref=src,
            dst_ref=dst,
            send_sem=send,
            recv_sem=recv,
            device_id={"kv": to_kv, "tp": to_tp},
            device_id_type=MESH,
        )

    scopes = []

    def mark(name=None):
        if scopes:
            scopes.pop().__exit__(None, None, None)
        if name:
            scopes.append(jax.named_scope(name))
            scopes[-1].__enter__()

    def send(*args):
        remote(*args).start()

    mark("barrier")
    barrier = pltpu.get_barrier_semaphore()

    def greet(to_kv, to_tp):
        pl.semaphore_signal(
            barrier, inc=1, device_id={"kv": to_kv, "tp": to_tp}, device_id_type=MESH
        )

    up, down = (z + 1) % nz, (z + nz - 1) % nz
    beside = [up, down][: nz - 1]
    for zp in beside:
        greet(zp * NX + x, c)
    for xp in (xr, xl):
        greet(z * NX + xp, c)
    greet(kv, other)
    mark("load")
    in_tok = local(0, tokens, tok.at[c])
    in_small = [
        local(14 + i, src, dst)
        for i, (src, dst) in enumerate(
            ((attn_gain, again), (head_gain, hgain), (mlp_gain, mgain), (lengths, lens))
        )
    ]
    in_w = [
        local(1 + i, src, dst)
        for i, (src, dst) in enumerate(
            ((w_query, wq), (w_key, wk), (w_decay, wd), (w_value, wv), (w_gate, wg))
        )
    ]
    in_cache = [
        local(6 + i, src, dst)
        for i, (src, dst) in enumerate(((cache_rates, cr), (cache_keys, ck), (cache_values, cv)))
    ]
    in_state = local(9, state, st)
    in_out = local(10, w_out, wo.at[c])
    in_mlp = [
        local(11 + i, src, dst)
        for i, (src, dst) in enumerate(((w_mlp_gate, wmg), (w_mlp_up, wmu), (w_mlp_down, wmd)))
    ]

    mark("meet")
    pl.semaphore_wait(barrier, len(beside) + 3)

    rounds = nz // 2 - 1

    def chain_send(r):
        if r < rounds:
            device = {"kv": up * NX + x, "tp": c}
            pl.semaphore_signal(csem.at[2 * r], inc=1, device_id=device, device_id_type=MESH)
            if r + 2 <= (nz - 1) // 2:
                device = {"kv": down * NX + x, "tp": c}
                pl.semaphore_signal(
                    csem.at[2 * r + 1], inc=1, device_id=device, device_id_type=MESH
                )

    def chain_wait(r):
        if r < rounds:
            pl.semaphore_wait(csem.at[2 * r], 1)
            if r + 2 <= (nz - 1) // 2:
                pl.semaphore_wait(csem.at[2 * r + 1], 1)

    chain_send(0)

    mark("tokens")
    in_tok.wait()
    send(tok.at[c], tok.at[c], psem.at[0], psem.at[1], kv, other)
    in_out.wait()
    send(wo.at[c], wo.at[c], psem.at[2], psem.at[3], kv, other)
    remote(tok.at[other], tok.at[other], psem.at[0], psem.at[1], kv, other).wait_recv()
    tokf[...] = jnp.concatenate([tok[0].astype(F32), tok[1].astype(F32)], axis=1)
    block = []
    for xp in range(NX):
        pair = [
            pltpu.roll(
                tokf[pl.ds(2 * xp + i, nz, stride=2 * NX), :], (2 * nz - z - nz // 4) % nz, 0
            )
            for i in range(2)
        ]
        for g in range(2):
            block += [rows[g * nh : (g + 1) * nh] for rows in pair]
    block = jnp.concatenate(block, axis=0)
    in_small[0].wait()
    squares = jnp.sum(block * block, axis=1, keepdims=True)
    scaled = (block * again[...].astype(F32)).astype(BF16)

    def put(target, b, values):
        half = target.shape[3] // LANES
        at = (b % half) * LANES
        for xp in range(NX):
            for g in range(2):
                row = (2 * xp + g) * nz
                target[g, 2 * xp + b // half, :, at : at + LANES] = values[row : row + nz].astype(
                    BF16
                )

    def project(copy, weight, target, start):
        copy.wait()
        part = dot(scaled, weight[...])
        for b in range(weight.shape[1] // LANES):
            put(target, start + b, part[:, b * LANES : (b + 1) * LANES])

    left, right = z * NX + xl, z * NX + xr

    def x_first(src, first, back, stage):
        out_sem, in_left, in_right, in_back = [xsem.at[stage, k] for k in range(4)]
        send(src.at[2 * xo], first.at[0], out_sem, in_left, right, c)
        send(src.at[2 * xo + 1], first.at[1], out_sem, in_right, left, c)

    def x_direct(src, first, back, stage):
        out_sem, in_left, in_right, in_back = [xsem.at[stage, k] for k in range(4)]
        send(src.at[2 * xr + 1], back.at[1], out_sem, in_back, right, c)
        send(src.at[2 * xl], back.at[2], out_sem, in_back, left, c)

    def x_second(src, first, relay, back, stage):
        out_sem, in_left, in_right, in_back = [xsem.at[stage, k] for k in range(4)]
        remote(first.at[0], first.at[0], out_sem, in_left, left, c).wait_recv()
        relay[0] = (src[2 * xr].astype(F32) + first[0].astype(F32)).astype(BF16)
        send(relay.at[0], back.at[0], out_sem, in_back, right, c)
        remote(first.at[1], first.at[1], out_sem, in_right, right, c).wait_recv()
        relay[1] = (src[2 * xl + 1].astype(F32) + first[1].astype(F32)).astype(BF16)
        send(relay.at[1], back.at[3], out_sem, in_back, left, c)

    def x_wait(back, stage):
        remote(back, back, xsem.at[stage, 0], xsem.at[stage, 3], left, c).wait_recv()

    def x_drain(src, stage):
        part = src.at[pl.ds(0, 6)]
        remote(part, part, xsem.at[stage, 0], xsem.at[stage, 3], left, c).wait_send()

    def x_sum(src, back, half):
        return (
            src[2 * x + half].astype(F32) + back[half].astype(F32) + back[2 + half].astype(F32)
        )

    def x_stage(g, col):
        src, first, relay, back = ((xa, xfa, xsa, xba), (xb, xfb, xsb, xbb))[col]
        return src.at[g], first.at[g], relay.at[g], back.at[g], 2 * g + col

    def x_one(g, col):
        src, first, relay, back, stage = x_stage(g, col)
        x_first(src, first, back, stage)

    def x_ind(g, col):
        src, first, relay, back, stage = x_stage(g, col)
        x_direct(src, first, back, stage)

    project(in_w[0], wq, xa, 0)
    project(in_w[1], wk, xa, qb)
    project(in_w[2], wd, xa, 2 * qb)
    put(xa, 3 * qb, jnp.broadcast_to(squares, (squares.shape[0], LANES)))
    for b in range(3 * qb + 1, 2 * (xa.shape[3] // LANES)):
        put(xa, b, jnp.zeros((squares.shape[0], LANES), F32))
    x_one(0, 0)
    chain_wait(0)
    chain_send(1)
    mark("project_b")
    project(in_w[3], wv, xb, 0)
    project(in_w[4], wg, xb, vb)
    x_one(0, 1)
    x_ind(0, 0)
    x_ind(0, 1)
    x_one(1, 0)
    x_one(1, 1)

    span = ck.shape[2]
    hb = vb // 2
    later = (
        lax.broadcasted_iota(jnp.int32, (span, span), 1)
        > lax.broadcasted_iota(jnp.int32, (span, span), 0)
    ).astype(BF16)
    ones = jnp.ones((span, LANES), BF16)
    slots = lax.broadcasted_iota(jnp.int32, (span, 1), 0)

    def fold(i, h):
        live = (slots < lens[i]).astype(F32)
        rates = cr[i, h] * live
        high, low = high_low(rates)
        rest = dot(later, high) + dot(later, low)
        keys = jnp.exp(-rest) * ck[i, h].astype(F32) * live
        shrink = jnp.exp(-(dot(high, ones, ((0,), (0,))) + dot(low, ones, ((0,), (0,)))))
        high, low = high_low(keys)
        value = cv[i, h]
        inner = dot(high, value, ((0,), (0,))) + dot(low, value, ((0,), (0,)))
        for b in range(hb):
            cols = slice(b * LANES, (b + 1) * LANES)
            memory[i, h, :, cols] = (st[i, h, :, cols] * shrink + inner[:, cols]).astype(BF16)

    mark("fold_a")
    zf[...] = jnp.zeros_like(zf)
    for copy in in_small[1:]:
        copy.wait()
    mgainf[...] = mgain[...].astype(F32)
    for h in range(2):
        for b in range(hb):
            hg[h * hb + b : h * hb + b + 1, :] = hgain[
                h : h + 1, b * LANES : (b + 1) * LANES
            ].astype(F32)
    for copy in in_cache:
        copy.wait()
    in_state.wait()
    for h in range(2):
        fold(0, h)
    chain_wait(1)
    chain_send(2)
    mark("x_second_a")
    x_second(*x_stage(0, 0))
    x_second(*x_stage(0, 1))
    mark("x_second_b")
    x_ind(1, 0)
    x_ind(1, 1)
    x_second(*x_stage(1, 0))
    x_second(*x_stage(1, 1))

    slots_row = zf.shape[0] // (2 * nh)

    def z_send(g, col):
        src, first, relay, back, stage = x_stage(g, col)
        half = src.shape[2] // LANES
        x_wait(back, stage)
        for hh in (0, 1):
            total = x_sum(src, back, hh)
            for b in range(half):
                for i in range(2):
                    zf[pl.ds(i * slots_row + hh * half + b, nh, stride=2 * slots_row), :] = total[
                        i * nh : (i + 1) * nh, b * LANES : (b + 1) * LANES
                    ]
        for j in by_distance(g):
            zs[stage, j] = zf[j * 2 * slots_row : (j + 1) * 2 * slots_row, :].astype(BF16)
            if (g, j) != (self_g, self_j):
                send(
                    zs.at[stage, j],
                    zr.at[stage, j],
                    zsem.at[stage, 0],
                    zsem.at[stage, 1],
                    zrel(g, j) * NX + x,
                    c,
                )

    def z_part(g, col):
        return zr.at[2 * g + col, pl.ds(0, nh - (g == self_g))]

    def z_sum(col):
        for g in range(2):
            part = z_part(g, col)
            stage = 2 * g + col
            remote(part, part, zsem.at[stage, 0], zsem.at[stage, 1], left, c).wait_recv()
        total = zs[2 * self_g + col, self_j].astype(F32)
        for g in range(2):
            for j in range(nh):
                if (g, j) != (self_g, self_j):
                    total = total + zr[2 * g + col, j].astype(F32)
        return total

    chain_wait(2)
    mark("z_send_a")
    z_send(0, 0)
    z_send(0, 1)
    mark("fold_b")
    for h in range(2):
        fold(1, h)
    mark("z_send_b")
    z_send(1, 0)
    z_send(1, 1)

    mark("z_wait_a")
    pack0[...] = z_sum(0)
    mark("heads_a")
    own = []
    inverse = []
    qh = qb // 2
    for i in range(2):
        at = i * slots_row
        inv = lax.rsqrt(pack0[at + 3 * qb : at + 3 * qb + 1, :] * (1.0 / width) + EPS)
        inverse.append(inv)
        query = pack0[at : at + qb, :] * inv * dk ** (-0.5)
        key = pack0[at + qb : at + 2 * qb, :] * inv
        raw = pack0[at + 2 * qb : at + 3 * qb, :] * inv
        decay = (jnp.minimum(raw, 0.0) - jnp.log1p(jnp.exp(-jnp.abs(raw)))) / GATE_NORM
        qe[i * qb : (i + 1) * qb, :] = query * jnp.exp(decay)
        both = query * key
        for h in range(2):
            part = jnp.sum(both[h * qh : (h + 1) * qh, :], axis=0, keepdims=True)
            own.append(jnp.sum(part, axis=1, keepdims=True))
    for i in range(2):
        for h in range(2):
            row = jnp.concatenate(
                [qe[i * qb + h * qh + b : i * qb + h * qh + b + 1, :] for b in range(qh)], axis=1
            )
            high, low = high_low(row)
            got = dot(jnp.concatenate([high, low], axis=0), memory[i, h])
            got = got[0:1] + got[1:2]
            for b in range(hb):
                att[i * vb + h * hb + b : i * vb + h * hb + b + 1, :] = got[
                    :, b * LANES : (b + 1) * LANES
                ]
    mark("z_wait_b")
    pack1[...] = z_sum(1)
    for i in range(2):
        at = i * slots_row
        if i == 0:
            mark("heads_b")
        value = pack1[at : at + vb, :] * inverse[i]
        gate = pack1[at + vb : at + 2 * vb, :] * inverse[i]
        attended = att[i * vb : (i + 1) * vb, :]
        for h in range(2):
            part = slice(h * hb, (h + 1) * hb)
            full = attended[part] + own[2 * i + h] * value[part]
            mean = jnp.sum(jnp.sum(full * full, axis=0, keepdims=True), axis=1, keepdims=True)
            norm = full * lax.rsqrt(mean * (1.0 / (hb * LANES)) + EPS) * hg[part, :]
            g = gate[part]
            headf[i * (headf.shape[0] // 2) + h * hb : i * (headf.shape[0] // 2) + (h + 1) * hb, :] = (
                g / (1.0 + jnp.exp(-g)) * norm
            )
    headb[2 * kv + c] = headf[...].astype(BF16)

    def gather(buf, sems, with_partner, consume):
        out_sem = sems.at[0]
        mine = buf.at[2 * kv + c]

        def in_z(zp):
            return sems.at[1 + zp]

        def in_x(zp):
            return sems.at[1 + nz + zp]

        def in_peer(zp):
            return sems.at[1 + 2 * nz + zp]

        for zp in far:
            send(mine, mine, out_sem, in_z(z), zp * NX + x, c)
        for xp in sides:
            send(mine, mine, out_sem, in_x(z), z * NX + xp, c)
        if with_partner:
            send(mine, mine, out_sem, in_peer(z), kv, other)

        def take_z(zp):
            origin = zp * NX + x
            slot = buf.at[2 * origin + c]
            remote(slot, slot, out_sem, in_z(zp), origin, c).wait_recv()
            for xp in sides:
                send(slot, slot, out_sem, in_x(zp), z * NX + xp, c)
            send(slot, slot, out_sem, in_peer(zp), kv, other)

        def take_x(zp):
            part = buf.at[pl.ds(0, NX - 1)]
            remote(part, part, out_sem, in_x(zp), left, c).wait_recv()
            for xp in sides[::-1]:
                slot = buf.at[2 * (zp * NX + xp) + c]
                send(slot, slot, out_sem, in_peer(zp), kv, other)

        def finish(zp):
            part = buf.at[pl.ds(0, NX - (zp is z and not with_partner))]
            remote(part, part, out_sem, in_peer(zp), kv, other).wait_recv()
            consume(zp)

        for zp in near:
            take_z(zp)
        mark("take_x")
        split = (len(near) + 1) // 2
        for zp in [z] + near[:split]:
            take_x(zp)
        finish(z)
        for zp in near[: split // 2]:
            finish(zp)
        for zp in near[split:]:
            take_x(zp)
        mark("take_peer")
        for zp in near[split // 2 :]:
            finish(zp)

    def gather_drain(buf, sems, with_partner):
        part = buf.at[pl.ds(0, 2 * nz * NX - 1 - (not with_partner))]
        remote(part, part, sems.at[0], sems.at[1], left, c).wait_send()

    n_kv = nz * NX
    hrows = headf.shape[0]

    def widen(zp):
        for k in range(2 * NX):
            slot = 2 * NX * zp + k
            headsf[pl.ds(pl.multiple_of(slot * hrows, 8), hrows), :] = headb[slot].astype(F32)

    mark("gather_heads")
    gather(headb, hsem, True, widen)

    mark("project_out")
    for cc in range(2):
        for b in range(vb):
            at = (cc * vb + b) * LANES
            for i in range(2):
                lhs[i * n_kv : (i + 1) * n_kv, at : at + LANES] = headsf[
                    pl.ds(cc * hrows + i * (hrows // 2) + b, n_kv, stride=2 * hrows), :
                ].astype(BF16)
    remote(wo.at[other], wo.at[other], psem.at[2], psem.at[3], kv, other).wait_recv()
    projected = dot(lhs[...], wo[...].reshape(LANES, 2 * vb * LANES), ((1,), (1,)))
    for i in range(2):
        old = tokf[pl.ds(i, n_kv, stride=2), :]
        whole[2 * kv + i] = (old + projected[i * n_kv : (i + 1) * n_kv]).astype(BF16)

    mark("gather_after")
    in_mlp[0].wait()
    in_mlp[1].wait()
    sums = [
        jnp.zeros((2 * n_kv, LANES), F32),
        jnp.zeros(hidden.shape, F32),
        jnp.zeros(hidden.shape, F32),
    ]

    def multiply(zp):
        parts = []
        for xp in range(NX):
            k = zp * NX + xp
            rows = jnp.concatenate([whole[2 * k], whole[2 * k + 1]], axis=0).astype(F32)
            sums[0] = sums[0] + rows * rows
            parts.append((rows * mgainf[pl.ds(k, 1), :]).astype(BF16))
        rows = jnp.concatenate(parts, axis=1)
        cols = pl.ds(pl.multiple_of(zp * NX * LANES, LANES), NX * LANES)
        sums[1] = sums[1] + dot(rows, wmg[:, cols], ((1,), (1,)))
        sums[2] = sums[2] + dot(rows, wmu[:, cols], ((1,), (1,)))

    gather(whole, asem, False, multiply)

    mark("mlp_in")
    inv = lax.rsqrt(jnp.sum(sums[0], axis=1, keepdims=True) * (1.0 / width) + EPS)
    gate = sums[1] * inv
    up = sums[2] * inv
    hidden[...] = (gate / (1.0 + jnp.exp(-gate)) * up).astype(BF16)
    mark("mlp_down")
    in_mlp[2].wait()
    for g in range(2):
        for j in range(nh):
            cols = pl.ds(pl.multiple_of(zrel(g, j) * NX * LANES, LANES), NX * LANES)
            part = dot(hidden[...], wmd[:, cols]).astype(BF16)
            for xp in range(NX):
                for k in range(4):
                    dpart[k // 2, g, 2 * xp + k % 2, :, j * LANES : (j + 1) * LANES] = part[
                        k * n_kv // 2 : (k + 1) * n_kv // 2, xp * LANES : (xp + 1) * LANES
                    ]
        send(dpart.at[other, g], dpeer.at[g], psem.at[4], psem.at[5 + g], kv, other)
    mark("down_peer")

    for g in range(2):
        remote(dpeer.at[g], dpeer.at[g], psem.at[4], psem.at[5 + g], kv, other).wait_recv()
        for n, xp in enumerate(sides + [x]):
            for k in range(2):
                dx[g, 2 * xp + k] = (
                    dpart[c, g, 2 * xp + k].astype(F32) + dpeer[g, 2 * xp + k].astype(F32)
                ).astype(BF16)
            if n < NX - 1:
                send(
                    dx.at[g, pl.ds(2 * xp, 2)],
                    drb.at[g, pl.ds(2 * n, 2)],
                    dxsem.at[g, 0],
                    dxsem.at[g, 1],
                    z * NX + xp,
                    c,
                )
    low_lanes = lax.broadcasted_iota(jnp.int32, (n_kv // 2, LANES), 1) < LANES // 2

    def squeeze(top, bottom, right):
        if right:
            top = pltpu.roll(top, LANES // 2, 1)
        else:
            bottom = pltpu.roll(bottom, LANES // 2, 1)
        return jnp.where(low_lanes, top, bottom)

    mark("down_x2")
    for g in range(2):
        part = drb.at[g]
        remote(part, part, dxsem.at[g, 0], dxsem.at[g, 1], left, c).wait_recv()
        top, bottom = [
            dx[g, 2 * x + k].astype(F32)
            + sum(drb[g, 2 * n + k].astype(F32) for n in range(NX - 1))
            for k in range(2)
        ]
        for j in by_distance(g):
            cols = slice(j * LANES, (j + 1) * LANES)
            slot = 2 * (g * nh + j)
            for cc in range(2):
                dzs[slot + cc] = squeeze(top[:, cols], bottom[:, cols], cc == 1).astype(BF16)
            if (g, j) == (self_g, self_j):
                dzr[slot + c] = dzs[slot + c]
                send(dzs.at[slot + other], dzr.at[slot + c], dzsem.at[0], dzsem.at[1], kv, other)
            else:
                for cc in (other, c):
                    send(
                        dzs.at[slot + cc],
                        dzr.at[slot + c],
                        dzsem.at[0],
                        dzsem.at[1],
                        zrel(g, j) * NX + x,
                        cc,
                    )
    mark("down_z")
    part = dzr.at[pl.ds(0, 2 * nz - 1)]
    remote(part, part, dzsem.at[0], dzsem.at[1], kv, other).wait_recv()
    mark("finish")
    for i in range(2):
        rows = whole[2 * kv + i].astype(F32)
        halves = rows[: n_kv // 2], rows[n_kv // 2 :]
        total = jnp.where(c == 1, squeeze(*halves, True), squeeze(*halves, False))
        for zp in range(nz):
            total = total + dzr[2 * zp + i].astype(F32)
        outf[pl.ds(i, n_kv // 2, stride=2), :] = total
        outf[pl.ds(i + n_kv, n_kv // 2, stride=2), :] = pltpu.roll(total, LANES // 2, 1)
    out[...] = outf[:, : LANES // 2].astype(BF16)
    mark("drain")
    remote(tok.at[c], tok.at[c], psem.at[0], psem.at[1], kv, other).wait_send()
    remote(wo.at[c], wo.at[c], psem.at[2], psem.at[3], kv, other).wait_send()
    for g in range(2):
        for col in range(2):
            stage = 2 * g + col
            x_drain((xa, xb)[col].at[g], stage)
            part = z_part(g, col)
            remote(part, part, zsem.at[stage, 0], zsem.at[stage, 1], left, c).wait_send()
        part = drb.at[g]
        remote(part, part, dxsem.at[g, 0], dxsem.at[g, 1], left, c).wait_send()
    gather_drain(headb, hsem, True)
    gather_drain(whole, asem, False)
    remote(dpeer, dpeer, psem.at[4], psem.at[5], kv, other).wait_send()
    part = dzr.at[pl.ds(0, 2 * nz - 1)]
    remote(part, part, dzsem.at[0], dzsem.at[1], kv, other).wait_send()
    mark()


def shards(
    tokens,
    lengths,
    state,
    cache_keys,
    cache_values,
    cache_rates,
    attn_gain,
    w_query,
    w_key,
    w_value,
    w_gate,
    w_decay,
    head_gain,
    w_out,
    mlp_gain,
    w_mlp_gate,
    w_mlp_up,
    w_mlp_down,
):
    n_kv = lax.axis_size("kv")
    nz = n_kv // NX
    heads, dk, dv = state.shape[1], state.shape[2], state.shape[3]
    width = mlp_gain.shape[0]
    qb, vb = heads * dk // LANES, heads * dv // LANES
    half0, half1 = (3 * qb + 2) // 2, vb
    slots = -(-2 * max(half0, half1) // 8) * 8
    nh = nz // 2
    seqs = 2 * n_kv
    hrows = 2 * vb
    units = w_mlp_down.shape[0]
    cols5 = nh * LANES
    vmem, dma = pltpu.VMEM, pltpu.SemaphoreType.DMA
    bf, fl = BF16, F32
    scratch = [
        vmem((2, seqs, LANES // 2), bf),
        vmem((seqs, LANES), fl),
        vmem(w_query.shape, bf),
        vmem(w_key.shape, bf),
        vmem(w_decay.shape, bf),
        vmem(w_value.shape, bf),
        vmem(w_gate.shape, bf),
        vmem(state.shape, fl),
        vmem(cache_keys.shape, bf),
        vmem(cache_values.shape, bf),
        vmem(cache_rates.shape, fl),
        vmem((2,) + w_out.shape[::-1], bf),
        vmem(w_mlp_gate.shape[::-1], bf),
        vmem(w_mlp_up.shape[::-1], bf),
        vmem(w_mlp_down.shape, bf),
        vmem((2, NX * 2, nz, half0 * LANES), bf),
        vmem((2, NX * 2, nz, half1 * LANES), bf),
        vmem((2, 2, nz, half0 * LANES), bf),
        vmem((2, 2, nz, half1 * LANES), bf),
        vmem((2, 2, nz, half0 * LANES), bf),
        vmem((2, 2, nz, half1 * LANES), bf),
        vmem((2, 4, nz, half0 * LANES), bf),
        vmem((2, 4, nz, half1 * LANES), bf),
        vmem((nz * slots, LANES), fl),
        vmem((4, nh, 2 * slots, LANES), bf),
        vmem((4, nh, 2 * slots, LANES), bf),
        vmem(state.shape, bf),
        vmem((2 * slots, LANES), fl),
        vmem((2 * slots, LANES), fl),
        vmem((2 * qb, LANES), fl),
        vmem((2 * vb, LANES), fl),
        vmem((vb, LANES), fl),
        vmem((hrows, LANES), fl),
        vmem((2 * n_kv, hrows, LANES), bf),
        vmem((n_kv * 2 * hrows, LANES), fl),
        vmem((seqs, 2 * vb * LANES), bf),
        vmem((2 * n_kv, n_kv, LANES), bf),
        vmem((seqs, units), bf),
        vmem((2, 2, NX * 2, n_kv // 2, cols5), bf),
        vmem((2, NX * 2, n_kv // 2, cols5), bf),
        vmem((2, NX * 2, n_kv // 2, cols5), bf),
        vmem((2, 2 * (NX - 1), n_kv // 2, cols5), bf),
        vmem((2 * nz, n_kv // 2, LANES), bf),
        vmem((2 * nz, n_kv // 2, LANES), bf),
        vmem((seqs, LANES), fl),
        vmem((1, LANES), bf),
        vmem((heads, dv), bf),
        vmem((n_kv, LANES), bf),
        vmem((n_kv, LANES), fl),
        pltpu.SMEM((2,), jnp.int32),
        dma((18,)),
        dma((7,)),
        dma((4, 4)),
        dma((4, 2)),
        dma((1 + 3 * nz,)),
        dma((1 + 3 * nz,)),
        dma((2, 2)),
        dma((2,)),
        pltpu.SemaphoreType.REGULAR((max(1, 2 * (nz // 2) - 3),)),
    ]
    anywhere = pl.BlockSpec(memory_space=pl.ANY)
    in_vmem = pl.BlockSpec(memory_space=pltpu.VMEM)
    specs = [anywhere] * 18
    return pl.pallas_call(
        functools.partial(kernel, (nz, qb, vb, dk, width)),
        out_shape=jax.ShapeDtypeStruct(tokens.shape, BF16),
        in_specs=specs,
        out_specs=in_vmem,
        scratch_shapes=scratch,
        compiler_params=pltpu.CompilerParams(collective_id=0, has_side_effects=True),
        name="layer",
    )(
        tokens,
        lengths,
        state,
        cache_keys,
        cache_values,
        cache_rates,
        attn_gain.reshape(1, -1),
        w_query,
        w_key,
        w_value,
        w_gate,
        w_decay,
        head_gain,
        w_out.T,
        mlp_gain.reshape(-1, LANES),
        w_mlp_gate.T,
        w_mlp_up.T,
        w_mlp_down,
    )


def solution(mesh):
    placed = (
        P("dp", ("kv", "tp")),
        P(("dp", "kv")),
        P(("dp", "kv"), "tp", None, None),
        P(("dp", "kv"), "tp", None, None),
        P(("dp", "kv"), "tp", None, None),
        P(("dp", "kv"), "tp", None, None),
        P("kv"),
        P("kv", "tp"),
        P("kv", "tp"),
        P("kv", "tp"),
        P("kv", "tp"),
        P("kv", "tp"),
        P("tp", None),
        P(None, ("kv", "tp")),
        P(),
        P(None, ("kv", "tp")),
        P(None, ("kv", "tp")),
        P(("kv", "tp"), None),
    )
    return jax.shard_map(
        shards, mesh=mesh, in_specs=placed, out_specs=P("dp", ("kv", "tp")), check_vma=False
    )
```

```python
import functools

import jax
import jax.numpy as jnp
from jax import lax
from jax.experimental import pallas as pl
from jax.experimental.pallas import tpu as pltpu
from jax.sharding import PartitionSpec as P

EPS = 1e-06
GATE_NORM = 16.0
NX = 4
LANES = 128
MESH = pl.DeviceIdType.MESH
F32 = jnp.float32
BF16 = jnp.bfloat16


def dot(a, b, dims=((1,), (0,))):
    return lax.dot_general(a, b, (dims, ((), ())), preferred_element_type=F32)


def high_low(a):
    high = a.astype(BF16)
    return high, (a - high.astype(F32)).astype(BF16)


def kernel(
    sizes,
    tokens,
    lengths,
    state,
    cache_keys,
    cache_values,
    cache_rates,
    attn_gain,
    w_query,
    w_key,
    w_value,
    w_gate,
    w_decay,
    head_gain,
    w_out,
    mlp_gain,
    w_mlp_gate,
    w_mlp_up,
    w_mlp_down,
    out,
    tok,
    tokf,
    wq,
    wk,
    wd,
    wv,
    wg,
    st,
    ck,
    cv,
    cr,
    wo,
    wm,
    xa,
    xb,
    xfa,
    xfb,
    xsa,
    xsb,
    xba,
    xbb,
    zf,
    zs,
    zr,
    memory,
    pack0,
    pack1,
    qe,
    att,
    hg,
    headf,
    headb,
    headsf,
    lhs,
    whole,
    hidden,
    partial,
    kept,
    dx,
    drb,
    dzs,
    dzr,
    outf,
    again,
    hgain,
    mgain,
    mgainf,
    lens,
    lsem,
    psem,
    xsem,
    zsem,
    hsem,
    asem,
    dxsem,
    dzsem,
    csem,
):
    nz, qb, vb, dk, width = sizes
    nh = nz // 2
    kv = lax.axis_index("kv")
    c = lax.axis_index("tp")
    other = 1 - c
    z = kv // NX
    x = kv % NX
    xr = (x + 1) % NX
    xl = (x + NX - 1) % NX
    xo = (x + 2) % NX
    steps = [((d + 1) // 2) * (1 if d % 2 else -1) for d in range(1, nz)]
    far = [(z + (s % nz)) % nz for s in steps][::-1]
    near = [(z + (s % nz)) % nz for s in steps]
    sides = [(x + d) % NX for d in (2, 1, 3)]

    def turn(g, j):
        return (nz // 4 + g * nh + j) % nz

    def zrel(g, j):
        return (z + turn(g, j)) % nz

    def by_distance(g):
        return sorted(range(nh), key=lambda j: -min(turn(g, j), nz - turn(g, j)))

    self_g, self_j = divmod((nz - nz // 4) % nz, nh)

    def local(i, src, dst):
        copy = pltpu.make_async_copy(src, dst, lsem.at[i])
        copy.start()
        return copy

    def remote(src, dst, send, recv, to_kv, to_tp):
        return pltpu.make_async_remote_copy(
            src_ref=src,
            dst_ref=dst,
            send_sem=send,
            recv_sem=recv,
            device_id={"kv": to_kv, "tp": to_tp},
            device_id_type=MESH,
        )

    scopes = []

    def mark(name=None):
        if scopes:
            scopes.pop().__exit__(None, None, None)
        if name:
            scopes.append(jax.named_scope(name))
            scopes[-1].__enter__()

    def send(*args):
        remote(*args).start()

    mark("barrier")
    barrier = pltpu.get_barrier_semaphore()

    def greet(to_kv, to_tp):
        pl.semaphore_signal(
            barrier, inc=1, device_id={"kv": to_kv, "tp": to_tp}, device_id_type=MESH
        )

    up, down = (z + 1) % nz, (z + nz - 1) % nz
    beside = [up, down][: nz - 1]
    for zp in beside:
        greet(zp * NX + x, c)
    for xp in (xr, xl):
        greet(z * NX + xp, c)
    greet(kv, other)
    mark("load")
    in_tok = local(0, tokens, tok.at[c])
    in_small = [
        local(12 + i, src, dst)
        for i, (src, dst) in enumerate(
            ((attn_gain, again), (head_gain, hgain), (mlp_gain, mgain), (lengths, lens))
        )
    ]
    in_w = [
        local(1 + i, src, dst)
        for i, (src, dst) in enumerate(
            ((w_query, wq), (w_key, wk), (w_decay, wd), (w_value, wv), (w_gate, wg))
        )
    ]
    in_cache = [
        local(6 + i, src, dst)
        for i, (src, dst) in enumerate(((cache_rates, cr), (cache_keys, ck), (cache_values, cv)))
    ]
    in_state = local(9, state, st)
    in_out = local(10, w_out, wo.at[c])
    in_mlp = [
        pltpu.make_async_copy(src, wm.at[c, i], lsem.at[11])
        for i, src in enumerate((w_mlp_gate, w_mlp_up, w_mlp_down))
    ]
    for copy in in_mlp:
        copy.start()

    mark("meet")
    pl.semaphore_wait(barrier, len(beside) + 3)

    rounds = nz // 2 - 1

    def chain_send(r):
        if r < rounds:
            device = {"kv": up * NX + x, "tp": c}
            pl.semaphore_signal(csem.at[2 * r], inc=1, device_id=device, device_id_type=MESH)
            if r + 2 <= (nz - 1) // 2:
                device = {"kv": down * NX + x, "tp": c}
                pl.semaphore_signal(
                    csem.at[2 * r + 1], inc=1, device_id=device, device_id_type=MESH
                )

    def chain_wait(r):
        if r < rounds:
            pl.semaphore_wait(csem.at[2 * r], 1)
            if r + 2 <= (nz - 1) // 2:
                pl.semaphore_wait(csem.at[2 * r + 1], 1)

    chain_send(0)

    mark("tokens")
    in_tok.wait()
    send(tok.at[c], tok.at[c], psem.at[0], psem.at[1], kv, other)
    remote(tok.at[other], tok.at[other], psem.at[0], psem.at[1], kv, other).wait_recv()
    tokf[...] = jnp.concatenate([tok[0].astype(F32), tok[1].astype(F32)], axis=1)
    block = []
    for xp in range(NX):
        pair = [
            pltpu.roll(
                tokf[pl.ds(2 * xp + i, nz, stride=2 * NX), :], (2 * nz - z - nz // 4) % nz, 0
            )
            for i in range(2)
        ]
        for g in range(2):
            block += [rows[g * nh : (g + 1) * nh] for rows in pair]
    block = jnp.concatenate(block, axis=0)
    in_small[0].wait()
    squares = jnp.sum(block * block, axis=1, keepdims=True)
    scaled = (block * again[...].astype(F32)).astype(BF16)

    def put(target, b, values):
        half = target.shape[3] // LANES
        at = (b % half) * LANES
        for xp in range(NX):
            for g in range(2):
                row = (2 * xp + g) * nz
                target[g, 2 * xp + b // half, :, at : at + LANES] = values[row : row + nz].astype(
                    BF16
                )

    def project(copy, weight, target, start):
        copy.wait()
        part = dot(scaled, weight[...])
        for b in range(weight.shape[1] // LANES):
            put(target, start + b, part[:, b * LANES : (b + 1) * LANES])

    left, right = z * NX + xl, z * NX + xr

    def x_first(src, first, back, stage):
        out_sem, in_left, in_right, in_back = [xsem.at[stage, k] for k in range(4)]
        send(src.at[2 * xo], first.at[0], out_sem, in_left, right, c)
        send(src.at[2 * xo + 1], first.at[1], out_sem, in_right, left, c)

    def x_direct(src, first, back, stage):
        out_sem, in_left, in_right, in_back = [xsem.at[stage, k] for k in range(4)]
        send(src.at[2 * xr + 1], back.at[1], out_sem, in_back, right, c)
        send(src.at[2 * xl], back.at[2], out_sem, in_back, left, c)

    def x_second(src, first, relay, back, stage):
        out_sem, in_left, in_right, in_back = [xsem.at[stage, k] for k in range(4)]
        remote(first.at[0], first.at[0], out_sem, in_left, left, c).wait_recv()
        relay[0] = (src[2 * xr].astype(F32) + first[0].astype(F32)).astype(BF16)
        send(relay.at[0], back.at[0], out_sem, in_back, right, c)
        remote(first.at[1], first.at[1], out_sem, in_right, right, c).wait_recv()
        relay[1] = (src[2 * xl + 1].astype(F32) + first[1].astype(F32)).astype(BF16)
        send(relay.at[1], back.at[3], out_sem, in_back, left, c)

    def x_wait(back, stage):
        remote(back, back, xsem.at[stage, 0], xsem.at[stage, 3], left, c).wait_recv()

    def x_drain(src, stage):
        part = src.at[pl.ds(0, 6)]
        remote(part, part, xsem.at[stage, 0], xsem.at[stage, 3], left, c).wait_send()

    def x_sum(src, back, half):
        return (
            src[2 * x + half].astype(F32) + back[half].astype(F32) + back[2 + half].astype(F32)
        )

    def x_stage(g, col):
        src, first, relay, back = ((xa, xfa, xsa, xba), (xb, xfb, xsb, xbb))[col]
        return src.at[g], first.at[g], relay.at[g], back.at[g], 2 * g + col

    def x_one(g, col):
        src, first, relay, back, stage = x_stage(g, col)
        x_first(src, first, back, stage)

    def x_ind(g, col):
        src, first, relay, back, stage = x_stage(g, col)
        x_direct(src, first, back, stage)

    project(in_w[0], wq, xa, 0)
    project(in_w[1], wk, xa, qb)
    project(in_w[2], wd, xa, 2 * qb)
    put(xa, 3 * qb, jnp.broadcast_to(squares, (squares.shape[0], LANES)))
    for b in range(3 * qb + 1, 2 * (xa.shape[3] // LANES)):
        put(xa, b, jnp.zeros((squares.shape[0], LANES), F32))
    x_one(0, 0)
    mark("project_b")
    project(in_w[3], wv, xb, 0)
    project(in_w[4], wg, xb, vb)
    x_one(0, 1)
    x_ind(0, 0)
    x_ind(0, 1)
    x_one(1, 0)
    x_one(1, 1)

    span = ck.shape[2]
    hb = vb // 2
    later = (
        lax.broadcasted_iota(jnp.int32, (span, span), 1)
        > lax.broadcasted_iota(jnp.int32, (span, span), 0)
    ).astype(BF16)
    ones = jnp.ones((span, LANES), BF16)
    slots = lax.broadcasted_iota(jnp.int32, (span, 1), 0)

    def fold(i, h):
        live = (slots < lens[i]).astype(F32)
        rates = cr[i, h] * live
        high, low = high_low(rates)
        rest = dot(later, high) + dot(later, low)
        keys = jnp.exp(-rest) * ck[i, h].astype(F32) * live
        shrink = jnp.exp(-(dot(high, ones, ((0,), (0,))) + dot(low, ones, ((0,), (0,)))))
        high, low = high_low(keys)
        value = cv[i, h]
        inner = dot(high, value, ((0,), (0,))) + dot(low, value, ((0,), (0,)))
        for b in range(hb):
            cols = slice(b * LANES, (b + 1) * LANES)
            memory[i, h, :, cols] = (st[i, h, :, cols] * shrink + inner[:, cols]).astype(BF16)

    mark("fold_a")
    chain_wait(0)
    chain_send(1)
    in_out.wait()
    send(wo.at[c], wo.at[c], psem.at[2], psem.at[3], kv, other)
    zf[...] = jnp.zeros_like(zf)
    for copy in in_small[1:]:
        copy.wait()
    mgainf[...] = mgain[...].astype(F32)
    for h in range(2):
        for b in range(hb):
            hg[h * hb + b : h * hb + b + 1, :] = hgain[
                h : h + 1, b * LANES : (b + 1) * LANES
            ].astype(F32)
    for copy in in_cache:
        copy.wait()
    in_state.wait()
    for h in range(2):
        fold(0, h)
    chain_wait(1)
    chain_send(2)
    mark("x_second_a")
    x_second(*x_stage(0, 0))
    x_second(*x_stage(0, 1))
    mark("x_second_b")
    x_ind(1, 0)
    x_ind(1, 1)
    x_second(*x_stage(1, 0))
    x_second(*x_stage(1, 1))

    slots_row = zf.shape[0] // (2 * nh)

    def z_send(g, col):
        src, first, relay, back, stage = x_stage(g, col)
        half = src.shape[2] // LANES
        x_wait(back, stage)
        for hh in (0, 1):
            total = x_sum(src, back, hh)
            for b in range(half):
                for i in range(2):
                    zf[pl.ds(i * slots_row + hh * half + b, nh, stride=2 * slots_row), :] = total[
                        i * nh : (i + 1) * nh, b * LANES : (b + 1) * LANES
                    ]
        for j in by_distance(g):
            zs[stage, j] = zf[j * 2 * slots_row : (j + 1) * 2 * slots_row, :].astype(BF16)
            if (g, j) != (self_g, self_j):
                send(
                    zs.at[stage, j],
                    zr.at[stage, j],
                    zsem.at[stage, 0],
                    zsem.at[stage, 1],
                    zrel(g, j) * NX + x,
                    c,
                )

    def z_part(g, col):
        return zr.at[2 * g + col, pl.ds(0, nh - (g == self_g))]

    def z_sum(col):
        for g in range(2):
            part = z_part(g, col)
            stage = 2 * g + col
            remote(part, part, zsem.at[stage, 0], zsem.at[stage, 1], left, c).wait_recv()
        total = zs[2 * self_g + col, self_j].astype(F32)
        for g in range(2):
            for j in range(nh):
                if (g, j) != (self_g, self_j):
                    total = total + zr[2 * g + col, j].astype(F32)
        return total

    chain_wait(2)
    mark("z_send_a")
    z_send(0, 0)
    z_send(0, 1)
    mark("fold_b")
    for h in range(2):
        fold(1, h)
    mark("z_send_b")
    z_send(1, 0)
    z_send(1, 1)

    mark("share")
    pltpu.make_async_copy(wm.at[c], wm.at[c], lsem.at[11]).wait()
    for k in range(3):
        send(wm.at[c, k], wm.at[c, k], psem.at[6], psem.at[7], kv, other)
    mark("z_wait_a")
    pack0[...] = z_sum(0)
    mark("heads_a")
    own = []
    inverse = []
    qh = qb // 2
    for i in range(2):
        at = i * slots_row
        inv = lax.rsqrt(pack0[at + 3 * qb : at + 3 * qb + 1, :] * (1.0 / width) + EPS)
        inverse.append(inv)
        query = pack0[at : at + qb, :] * inv * dk ** (-0.5)
        key = pack0[at + qb : at + 2 * qb, :] * inv
        raw = pack0[at + 2 * qb : at + 3 * qb, :] * inv
        decay = (jnp.minimum(raw, 0.0) - jnp.log1p(jnp.exp(-jnp.abs(raw)))) / GATE_NORM
        qe[i * qb : (i + 1) * qb, :] = query * jnp.exp(decay)
        both = query * key
        for h in range(2):
            part = jnp.sum(both[h * qh : (h + 1) * qh, :], axis=0, keepdims=True)
            own.append(jnp.sum(part, axis=1, keepdims=True))
    for i in range(2):
        for h in range(2):
            row = jnp.concatenate(
                [qe[i * qb + h * qh + b : i * qb + h * qh + b + 1, :] for b in range(qh)], axis=1
            )
            high, low = high_low(row)
            got = dot(jnp.concatenate([high, low], axis=0), memory[i, h])
            got = got[0:1] + got[1:2]
            for b in range(hb):
                att[i * vb + h * hb + b : i * vb + h * hb + b + 1, :] = got[
                    :, b * LANES : (b + 1) * LANES
                ]
    mark("z_wait_b")
    pack1[...] = z_sum(1)
    for i in range(2):
        at = i * slots_row
        if i == 0:
            mark("heads_b")
        value = pack1[at : at + vb, :] * inverse[i]
        gate = pack1[at + vb : at + 2 * vb, :] * inverse[i]
        attended = att[i * vb : (i + 1) * vb, :]
        for h in range(2):
            part = slice(h * hb, (h + 1) * hb)
            full = attended[part] + own[2 * i + h] * value[part]
            mean = jnp.sum(jnp.sum(full * full, axis=0, keepdims=True), axis=1, keepdims=True)
            norm = full * lax.rsqrt(mean * (1.0 / (hb * LANES)) + EPS) * hg[part, :]
            g = gate[part]
            headf[i * (headf.shape[0] // 2) + h * hb : i * (headf.shape[0] // 2) + (h + 1) * hb, :] = (
                g / (1.0 + jnp.exp(-g)) * norm
            )
    headb[kv] = headf[...].astype(BF16)

    def gather(buf, sems, consume):
        out_sem = sems.at[0]
        mine = buf.at[kv]

        def in_z(zp):
            return sems.at[1 + zp]

        def in_x(zp):
            return sems.at[1 + nz + zp]

        for zp in far:
            send(mine, mine, out_sem, in_z(z), zp * NX + x, c)
        for xp in sides:
            send(mine, mine, out_sem, in_x(z), z * NX + xp, c)
        for zp in near:
            slot = buf.at[zp * NX + x]
            remote(slot, slot, out_sem, in_z(zp), zp * NX + x, c).wait_recv()
            for xp in sides:
                send(slot, slot, out_sem, in_x(zp), z * NX + xp, c)
        mark("take_x")
        for zp in [z] + near:
            part = buf.at[pl.ds(0, NX - 1)]
            remote(part, part, out_sem, in_x(zp), left, c).wait_recv()
            consume(zp)

    def gather_drain(buf, sems):
        part = buf.at[pl.ds(0, nz * NX - 1)]
        remote(part, part, sems.at[0], sems.at[1], left, c).wait_send()

    n_kv = nz * NX
    hrows = headf.shape[0]

    def widen(zp):
        for k in range(NX):
            slot = NX * zp + k
            headsf[pl.ds(pl.multiple_of(slot * hrows, 8), hrows), :] = headb[slot].astype(F32)

    mark("gather_heads")
    gather(headb, hsem, widen)

    mark("project_out")
    for b in range(vb):
        for i in range(2):
            lhs[i * n_kv : (i + 1) * n_kv, b * LANES : (b + 1) * LANES] = headsf[
                pl.ds(i * (hrows // 2) + b, n_kv, stride=hrows), :
            ].astype(BF16)
    remote(wo.at[other], wo.at[other], psem.at[2], psem.at[3], kv, other).wait_recv()
    own_rows = pl.ds(pl.multiple_of(c * vb * LANES, LANES), vb * LANES)
    partial[0] = dot(lhs[...], wo[:, :, own_rows].reshape(LANES, vb * LANES), ((1,), (1,)))
    send(partial.at[0], partial.at[1], psem.at[4], psem.at[5], kv, other)
    remote(partial.at[1], partial.at[1], psem.at[4], psem.at[5], kv, other).wait_recv()
    projected = partial[0] + partial[1]
    after = [
        (tokf[pl.ds(i, n_kv, stride=2), :] + projected[i * n_kv : (i + 1) * n_kv]).astype(BF16)
        for i in range(2)
    ]
    for i in range(2):
        kept[i] = after[i].astype(F32)
    whole[kv] = jnp.where(c == 0, after[0].astype(F32), after[1].astype(F32)).astype(BF16)

    mark("gather_after")
    remote(wm.at[other], wm.at[other], psem.at[6], psem.at[7], kv, other).wait_recv()
    units = hidden.shape[2]
    energy = [jnp.zeros((n_kv, LANES), F32)]
    sums = [jnp.zeros((n_kv, units), F32) for _ in range(4)]

    def multiply(zp):
        parts = []
        for xp in range(NX):
            k = zp * NX + xp
            rows = whole[k].astype(F32)
            energy[0] = energy[0] + rows * rows
            parts.append((rows * mgainf[pl.ds(k, 1), :]).astype(BF16))
        rows = jnp.concatenate(parts, axis=1)
        cols = pl.ds(pl.multiple_of(zp * NX * LANES, LANES), NX * LANES)
        for k in range(4):
            sums[k] = sums[k] + dot(rows, wm[k // 2, k % 2, :, cols], ((1,), (1,)))

    gather(whole, asem, multiply)

    mark("mlp_in")
    inv = lax.rsqrt(jnp.sum(energy[0], axis=1, keepdims=True) * (1.0 / width) + EPS)
    for cc in range(2):
        gate = sums[2 * cc] * inv
        up = sums[2 * cc + 1] * inv
        hidden[cc] = (gate / (1.0 + jnp.exp(-gate)) * up).astype(BF16)
    mark("mlp_down")
    for g in range(2):
        for j in range(nh):
            cols = pl.ds(pl.multiple_of(zrel(g, j) * NX * LANES, LANES), NX * LANES)
            part = (dot(hidden[0], wm[0, 2, :, cols]) + dot(hidden[1], wm[1, 2, :, cols])).astype(
                BF16
            )
            for xp in range(NX):
                for k in range(2):
                    dx[g, 2 * xp + k, :, j * LANES : (j + 1) * LANES] = part[
                        k * n_kv // 2 : (k + 1) * n_kv // 2, xp * LANES : (xp + 1) * LANES
                    ]
        for n, xp in enumerate(sides):
            send(
                dx.at[g, pl.ds(2 * xp, 2)],
                drb.at[g, pl.ds(2 * n, 2)],
                dxsem.at[g, 0],
                dxsem.at[g, 1],
                z * NX + xp,
                c,
            )
    low_lanes = lax.broadcasted_iota(jnp.int32, (n_kv // 2, LANES), 1) < LANES // 2

    def squeeze(top, bottom, right):
        if right:
            top = pltpu.roll(top, LANES // 2, 1)
        else:
            bottom = pltpu.roll(bottom, LANES // 2, 1)
        return jnp.where(low_lanes, top, bottom)

    mark("down_x2")
    for g in range(2):
        part = drb.at[g]
        remote(part, part, dxsem.at[g, 0], dxsem.at[g, 1], left, c).wait_recv()
        top, bottom = [
            dx[g, 2 * x + k].astype(F32)
            + sum(drb[g, 2 * n + k].astype(F32) for n in range(NX - 1))
            for k in range(2)
        ]
        for j in by_distance(g):
            cols = slice(j * LANES, (j + 1) * LANES)
            slot = 2 * (g * nh + j)
            for cc in range(2):
                dzs[slot + cc] = squeeze(top[:, cols], bottom[:, cols], cc == 1).astype(BF16)
            if (g, j) == (self_g, self_j):
                dzr[slot + c] = dzs[slot + c]
                send(dzs.at[slot + other], dzr.at[slot + c], dzsem.at[0], dzsem.at[1], kv, other)
            else:
                for cc in (other, c):
                    send(
                        dzs.at[slot + cc],
                        dzr.at[slot + c],
                        dzsem.at[0],
                        dzsem.at[1],
                        zrel(g, j) * NX + x,
                        cc,
                    )
    mark("down_z")
    part = dzr.at[pl.ds(0, 2 * nz - 1)]
    remote(part, part, dzsem.at[0], dzsem.at[1], kv, other).wait_recv()
    mark("finish")
    for i in range(2):
        rows = kept[i]
        halves = rows[: n_kv // 2], rows[n_kv // 2 :]
        total = jnp.where(c == 1, squeeze(*halves, True), squeeze(*halves, False))
        for zp in range(nz):
            total = total + dzr[2 * zp + i].astype(F32)
        outf[pl.ds(i, n_kv // 2, stride=2), :] = total
        outf[pl.ds(i + n_kv, n_kv // 2, stride=2), :] = pltpu.roll(total, LANES // 2, 1)
    out[...] = outf[:, : LANES // 2].astype(BF16)
    mark("drain")
    remote(tok.at[c], tok.at[c], psem.at[0], psem.at[1], kv, other).wait_send()
    remote(wo.at[c], wo.at[c], psem.at[2], psem.at[3], kv, other).wait_send()
    for g in range(2):
        for col in range(2):
            stage = 2 * g + col
            x_drain((xa, xb)[col].at[g], stage)
            part = z_part(g, col)
            remote(part, part, zsem.at[stage, 0], zsem.at[stage, 1], left, c).wait_send()
        part = drb.at[g]
        remote(part, part, dxsem.at[g, 0], dxsem.at[g, 1], left, c).wait_send()
    gather_drain(headb, hsem)
    gather_drain(whole, asem)
    remote(partial.at[0], partial.at[1], psem.at[4], psem.at[5], kv, other).wait_send()
    remote(wm.at[c], wm.at[c], psem.at[6], psem.at[7], kv, other).wait_send()
    part = dzr.at[pl.ds(0, 2 * nz - 1)]
    remote(part, part, dzsem.at[0], dzsem.at[1], kv, other).wait_send()
    mark()


def shards(
    tokens,
    lengths,
    state,
    cache_keys,
    cache_values,
    cache_rates,
    attn_gain,
    w_query,
    w_key,
    w_value,
    w_gate,
    w_decay,
    head_gain,
    w_out,
    mlp_gain,
    w_mlp_gate,
    w_mlp_up,
    w_mlp_down,
):
    n_kv = lax.axis_size("kv")
    nz = n_kv // NX
    heads, dk, dv = state.shape[1], state.shape[2], state.shape[3]
    width = mlp_gain.shape[0]
    qb, vb = heads * dk // LANES, heads * dv // LANES
    half0, half1 = (3 * qb + 2) // 2, vb
    slots = -(-2 * max(half0, half1) // 8) * 8
    nh = nz // 2
    seqs = 2 * n_kv
    hrows = 2 * vb
    units = w_mlp_down.shape[0]
    cols5 = nh * LANES
    vmem, dma = pltpu.VMEM, pltpu.SemaphoreType.DMA
    bf, fl = BF16, F32
    scratch = [
        vmem((2, seqs, LANES // 2), bf),
        vmem((seqs, LANES), fl),
        vmem(w_query.shape, bf),
        vmem(w_key.shape, bf),
        vmem(w_decay.shape, bf),
        vmem(w_value.shape, bf),
        vmem(w_gate.shape, bf),
        vmem(state.shape, fl),
        vmem(cache_keys.shape, bf),
        vmem(cache_values.shape, bf),
        vmem(cache_rates.shape, fl),
        vmem((2,) + w_out.shape[::-1], bf),
        vmem((2, 3) + w_mlp_down.shape, bf),
        vmem((2, NX * 2, nz, half0 * LANES), bf),
        vmem((2, NX * 2, nz, half1 * LANES), bf),
        vmem((2, 2, nz, half0 * LANES), bf),
        vmem((2, 2, nz, half1 * LANES), bf),
        vmem((2, 2, nz, half0 * LANES), bf),
        vmem((2, 2, nz, half1 * LANES), bf),
        vmem((2, 4, nz, half0 * LANES), bf),
        vmem((2, 4, nz, half1 * LANES), bf),
        vmem((nz * slots, LANES), fl),
        vmem((4, nh, 2 * slots, LANES), bf),
        vmem((4, nh, 2 * slots, LANES), bf),
        vmem(state.shape, bf),
        vmem((2 * slots, LANES), fl),
        vmem((2 * slots, LANES), fl),
        vmem((2 * qb, LANES), fl),
        vmem((2 * vb, LANES), fl),
        vmem((vb, LANES), fl),
        vmem((hrows, LANES), fl),
        vmem((n_kv, hrows, LANES), bf),
        vmem((n_kv * hrows, LANES), fl),
        vmem((seqs, vb * LANES), bf),
        vmem((n_kv, n_kv, LANES), bf),
        vmem((2, n_kv, units), bf),
        vmem((2, seqs, LANES), fl),
        vmem((2, n_kv, LANES), fl),
        vmem((2, NX * 2, n_kv // 2, cols5), bf),
        vmem((2, 2 * (NX - 1), n_kv // 2, cols5), bf),
        vmem((2 * nz, n_kv // 2, LANES), bf),
        vmem((2 * nz, n_kv // 2, LANES), bf),
        vmem((seqs, LANES), fl),
        vmem((1, LANES), bf),
        vmem((heads, dv), bf),
        vmem((n_kv, LANES), bf),
        vmem((n_kv, LANES), fl),
        pltpu.SMEM((2,), jnp.int32),
        dma((16,)),
        dma((8,)),
        dma((4, 4)),
        dma((4, 2)),
        dma((1 + 2 * nz,)),
        dma((1 + 2 * nz,)),
        dma((2, 2)),
        dma((2,)),
        pltpu.SemaphoreType.REGULAR((max(1, 2 * (nz // 2) - 3),)),
    ]
    anywhere = pl.BlockSpec(memory_space=pl.ANY)
    in_vmem = pl.BlockSpec(memory_space=pltpu.VMEM)
    specs = [anywhere] * 18
    return pl.pallas_call(
        functools.partial(kernel, (nz, qb, vb, dk, width)),
        out_shape=pltpu.VMEM(tokens.shape, BF16),
        in_specs=specs,
        out_specs=in_vmem,
        scratch_shapes=scratch,
        compiler_params=pltpu.CompilerParams(collective_id=0, has_side_effects=True),
        name="layer",
    )(
        tokens,
        lengths,
        state,
        cache_keys,
        cache_values,
        cache_rates,
        attn_gain.reshape(1, -1),
        w_query,
        w_key,
        w_value,
        w_gate,
        w_decay,
        head_gain,
        w_out.T,
        mlp_gain.reshape(-1, LANES),
        w_mlp_gate.T,
        w_mlp_up.T,
        w_mlp_down,
    )


def solution(mesh):
    placed = (
        P("dp", ("kv", "tp")),
        P(("dp", "kv")),
        P(("dp", "kv"), "tp", None, None),
        P(("dp", "kv"), "tp", None, None),
        P(("dp", "kv"), "tp", None, None),
        P(("dp", "kv"), "tp", None, None),
        P("kv"),
        P("kv", "tp"),
        P("kv", "tp"),
        P("kv", "tp"),
        P("kv", "tp"),
        P("kv", "tp"),
        P("tp", None),
        P(None, ("kv", "tp")),
        P(),
        P(None, ("kv", "tp")),
        P(None, ("kv", "tp")),
        P(("kv", "tp"), None),
    )
    return jax.shard_map(
        shards, mesh=mesh, in_specs=placed, out_specs=P("dp", ("kv", "tp")), check_vma=False
    )
```

```python
import functools

import jax
import jax.numpy as jnp
from jax import lax
from jax.experimental import pallas as pl
from jax.experimental.pallas import tpu as pltpu
from jax.sharding import PartitionSpec as P

EPS = 1e-06
GATE_NORM = 16.0
NX = 4
LANES = 128
MESH = pl.DeviceIdType.MESH
F32 = jnp.float32
BF16 = jnp.bfloat16


def dot(a, b, dims=((1,), (0,))):
    return lax.dot_general(a, b, (dims, ((), ())), preferred_element_type=F32)


def high_low(a):
    high = a.astype(BF16)
    return high, (a - high.astype(F32)).astype(BF16)


def kernel(
    sizes,
    tokens,
    lengths,
    state,
    cache_keys,
    cache_values,
    cache_rates,
    attn_gain,
    w_query,
    w_key,
    w_value,
    w_gate,
    w_decay,
    head_gain,
    w_out,
    mlp_gain,
    w_mlp_gate,
    w_mlp_up,
    w_mlp_down,
    out,
    tok,
    tokf,
    wq,
    wk,
    wd,
    wv,
    wg,
    st,
    ck,
    cv,
    cr,
    wo,
    wm,
    xa,
    xb,
    xfa,
    xfb,
    xsa,
    xsb,
    xba,
    xbb,
    zf,
    zs,
    zr,
    memory,
    pack0,
    pack1,
    qe,
    att,
    hg,
    headf,
    hmine,
    headb,
    headsf,
    lhs,
    whole,
    hidden,
    kept,
    dx,
    drb,
    dzs,
    dzr,
    outf,
    again,
    hgain,
    mgain,
    mgainf,
    lens,
    lsem,
    psem,
    xsem,
    zsem,
    hsem,
    asem,
    dxsem,
    dzsem,
    csem,
):
    nz, qb, vb, dk, width = sizes
    nh = nz // 2
    kv = lax.axis_index("kv")
    c = lax.axis_index("tp")
    other = 1 - c
    z = kv // NX
    x = kv % NX
    xr = (x + 1) % NX
    xl = (x + NX - 1) % NX
    xo = (x + 2) % NX
    steps = [((d + 1) // 2) * (1 if d % 2 else -1) for d in range(1, nz)]
    far = [(z + (s % nz)) % nz for s in steps][::-1]
    near = [(z + (s % nz)) % nz for s in steps]
    sides = [(x + d) % NX for d in (2, 1, 3)]

    def turn(g, j):
        return (nz // 4 + g * nh + j) % nz

    def zrel(g, j):
        return (z + turn(g, j)) % nz

    def by_distance(g):
        return sorted(range(nh), key=lambda j: -min(turn(g, j), nz - turn(g, j)))

    self_g, self_j = divmod((nz - nz // 4) % nz, nh)

    def local(i, src, dst):
        copy = pltpu.make_async_copy(src, dst, lsem.at[i])
        copy.start()
        return copy

    def remote(src, dst, send, recv, to_kv, to_tp):
        return pltpu.make_async_remote_copy(
            src_ref=src,
            dst_ref=dst,
            send_sem=send,
            recv_sem=recv,
            device_id={"kv": to_kv, "tp": to_tp},
            device_id_type=MESH,
        )

    scopes = []

    def mark(name=None):
        if scopes:
            scopes.pop().__exit__(None, None, None)
        if name:
            scopes.append(jax.named_scope(name))
            scopes[-1].__enter__()

    def send(*args):
        remote(*args).start()

    mark("barrier")
    barrier = pltpu.get_barrier_semaphore()

    def greet(to_kv, to_tp):
        pl.semaphore_signal(
            barrier, inc=1, device_id={"kv": to_kv, "tp": to_tp}, device_id_type=MESH
        )

    up, down = (z + 1) % nz, (z + nz - 1) % nz
    beside = [up, down][: nz - 1]
    for zp in beside:
        greet(zp * NX + x, c)
    for xp in (xr, xl):
        greet(z * NX + xp, c)
    greet(kv, other)
    mark("load")
    in_tok = local(0, tokens, tok.at[c])
    in_small = [
        local(12 + i, src, dst)
        for i, (src, dst) in enumerate(
            ((attn_gain, again), (head_gain, hgain), (mlp_gain, mgain), (lengths, lens))
        )
    ]
    in_w = [
        local(1 + i, src, dst)
        for i, (src, dst) in enumerate(
            ((w_query, wq), (w_key, wk), (w_decay, wd), (w_value, wv), (w_gate, wg))
        )
    ]
    in_cache = [
        local(6 + i, src, dst)
        for i, (src, dst) in enumerate(((cache_rates, cr), (cache_keys, ck), (cache_values, cv)))
    ]
    in_state = local(9, state, st)
    in_out = local(10, w_out, wo.at[c])
    in_mlp = [
        pltpu.make_async_copy(src, wm.at[c, i], lsem.at[11])
        for i, src in enumerate((w_mlp_gate, w_mlp_up, w_mlp_down))
    ]
    for copy in in_mlp:
        copy.start()

    mark("meet")
    pl.semaphore_wait(barrier, len(beside) + 3)

    rounds = nz // 2 - 1

    def chain_send(r):
        if r < rounds:
            device = {"kv": up * NX + x, "tp": c}
            pl.semaphore_signal(csem.at[2 * r], inc=1, device_id=device, device_id_type=MESH)
            if r + 2 <= (nz - 1) // 2:
                device = {"kv": down * NX + x, "tp": c}
                pl.semaphore_signal(
                    csem.at[2 * r + 1], inc=1, device_id=device, device_id_type=MESH
                )

    def chain_wait(r):
        if r < rounds:
            pl.semaphore_wait(csem.at[2 * r], 1)
            if r + 2 <= (nz - 1) // 2:
                pl.semaphore_wait(csem.at[2 * r + 1], 1)

    chain_send(0)

    mark("tokens")
    in_tok.wait()
    send(tok.at[c], tok.at[c], psem.at[0], psem.at[1], kv, other)
    remote(tok.at[other], tok.at[other], psem.at[0], psem.at[1], kv, other).wait_recv()
    tokf[...] = jnp.concatenate([tok[0].astype(F32), tok[1].astype(F32)], axis=1)
    block = []
    for xp in range(NX):
        pair = [
            pltpu.roll(
                tokf[pl.ds(2 * xp + i, nz, stride=2 * NX), :], (2 * nz - z - nz // 4) % nz, 0
            )
            for i in range(2)
        ]
        for g in range(2):
            block += [rows[g * nh : (g + 1) * nh] for rows in pair]
    block = jnp.concatenate(block, axis=0)
    in_small[0].wait()
    squares = jnp.sum(block * block, axis=1, keepdims=True)
    scaled = (block * again[...].astype(F32)).astype(BF16)

    def put(target, b, values):
        half = target.shape[3] // LANES
        at = (b % half) * LANES
        for xp in range(NX):
            for g in range(2):
                row = (2 * xp + g) * nz
                target[g, 2 * xp + b // half, :, at : at + LANES] = values[row : row + nz].astype(
                    BF16
                )

    def project(copy, weight, target, start):
        copy.wait()
        part = dot(scaled, weight[...])
        for b in range(weight.shape[1] // LANES):
            put(target, start + b, part[:, b * LANES : (b + 1) * LANES])

    left, right = z * NX + xl, z * NX + xr

    def x_first(src, first, back, stage):
        out_sem, in_left, in_right, in_back = [xsem.at[stage, k] for k in range(4)]
        send(src.at[2 * xo], first.at[0], out_sem, in_left, right, c)
        send(src.at[2 * xo + 1], first.at[1], out_sem, in_right, left, c)

    def x_direct(src, first, back, stage):
        out_sem, in_left, in_right, in_back = [xsem.at[stage, k] for k in range(4)]
        send(src.at[2 * xr + 1], back.at[1], out_sem, in_back, right, c)
        send(src.at[2 * xl], back.at[2], out_sem, in_back, left, c)

    def x_second(src, first, relay, back, stage):
        out_sem, in_left, in_right, in_back = [xsem.at[stage, k] for k in range(4)]
        remote(first.at[0], first.at[0], out_sem, in_left, left, c).wait_recv()
        relay[0] = (src[2 * xr].astype(F32) + first[0].astype(F32)).astype(BF16)
        send(relay.at[0], back.at[0], out_sem, in_back, right, c)
        remote(first.at[1], first.at[1], out_sem, in_right, right, c).wait_recv()
        relay[1] = (src[2 * xl + 1].astype(F32) + first[1].astype(F32)).astype(BF16)
        send(relay.at[1], back.at[3], out_sem, in_back, left, c)

    def x_wait(back, stage):
        remote(back, back, xsem.at[stage, 0], xsem.at[stage, 3], left, c).wait_recv()

    def x_drain(src, stage):
        part = src.at[pl.ds(0, 6)]
        remote(part, part, xsem.at[stage, 0], xsem.at[stage, 3], left, c).wait_send()

    def x_sum(src, back, half):
        return (
            src[2 * x + half].astype(F32) + back[half].astype(F32) + back[2 + half].astype(F32)
        )

    def x_stage(g, col):
        src, first, relay, back = ((xa, xfa, xsa, xba), (xb, xfb, xsb, xbb))[col]
        return src.at[g], first.at[g], relay.at[g], back.at[g], 2 * g + col

    def x_one(g, col):
        src, first, relay, back, stage = x_stage(g, col)
        x_first(src, first, back, stage)

    def x_ind(g, col):
        src, first, relay, back, stage = x_stage(g, col)
        x_direct(src, first, back, stage)

    project(in_w[0], wq, xa, 0)
    project(in_w[1], wk, xa, qb)
    project(in_w[2], wd, xa, 2 * qb)
    put(xa, 3 * qb, jnp.broadcast_to(squares, (squares.shape[0], LANES)))
    for b in range(3 * qb + 1, 2 * (xa.shape[3] // LANES)):
        put(xa, b, jnp.zeros((squares.shape[0], LANES), F32))
    x_one(0, 0)
    mark("project_b")
    project(in_w[3], wv, xb, 0)
    project(in_w[4], wg, xb, vb)
    x_one(0, 1)
    x_ind(0, 0)
    x_ind(0, 1)
    x_one(1, 0)
    x_one(1, 1)

    span = ck.shape[2]
    hb = vb // 2
    later = (
        lax.broadcasted_iota(jnp.int32, (span, span), 1)
        > lax.broadcasted_iota(jnp.int32, (span, span), 0)
    ).astype(BF16)
    ones = jnp.ones((span, LANES), BF16)
    slots = lax.broadcasted_iota(jnp.int32, (span, 1), 0)

    def fold(i, h):
        live = (slots < lens[i]).astype(F32)
        rates = cr[i, h] * live
        high, low = high_low(rates)
        rest = dot(later, high) + dot(later, low)
        keys = jnp.exp(-rest) * ck[i, h].astype(F32) * live
        shrink = jnp.exp(-(dot(high, ones, ((0,), (0,))) + dot(low, ones, ((0,), (0,)))))
        high, low = high_low(keys)
        value = cv[i, h]
        inner = dot(high, value, ((0,), (0,))) + dot(low, value, ((0,), (0,)))
        for b in range(hb):
            cols = slice(b * LANES, (b + 1) * LANES)
            memory[i, h, :, cols] = (st[i, h, :, cols] * shrink + inner[:, cols]).astype(BF16)

    mark("fold_a")
    chain_wait(0)
    chain_send(1)
    in_out.wait()
    send(wo.at[c], wo.at[c], psem.at[2], psem.at[3], kv, other)
    zf[...] = jnp.zeros_like(zf)
    for copy in in_small[1:]:
        copy.wait()
    mgainf[...] = mgain[...].astype(F32)
    for h in range(2):
        for b in range(hb):
            hg[h * hb + b : h * hb + b + 1, :] = hgain[
                h : h + 1, b * LANES : (b + 1) * LANES
            ].astype(F32)
    for copy in in_cache:
        copy.wait()
    in_state.wait()
    for h in range(2):
        fold(0, h)
    chain_wait(1)
    chain_send(2)
    mark("x_second_a")
    x_second(*x_stage(0, 0))
    x_second(*x_stage(0, 1))
    mark("x_second_b")
    x_ind(1, 0)
    x_ind(1, 1)
    x_second(*x_stage(1, 0))
    x_second(*x_stage(1, 1))

    slots_of = (pack0.shape[0] // 2, pack1.shape[0] // 2)

    def z_send(g, col):
        src, first, relay, back, stage = x_stage(g, col)
        half = src.shape[2] // LANES
        slots_row = slots_of[col]
        x_wait(back, stage)
        for hh in (0, 1):
            total = x_sum(src, back, hh)
            for b in range(half):
                for i in range(2):
                    zf[pl.ds(i * slots_row + hh * half + b, nh, stride=2 * slots_row), :] = total[
                        i * nh : (i + 1) * nh, b * LANES : (b + 1) * LANES
                    ]
        for j in by_distance(g):
            zs[stage, j, : 2 * slots_row] = zf[j * 2 * slots_row : (j + 1) * 2 * slots_row, :].astype(BF16)
            if (g, j) != (self_g, self_j):
                send(
                    zs.at[stage, j, pl.ds(0, 2 * slots_row)],
                    zr.at[stage, j, pl.ds(0, 2 * slots_row)],
                    zsem.at[stage, 0],
                    zsem.at[stage, 1],
                    zrel(g, j) * NX + x,
                    c,
                )

    def z_part(g, col):
        return zr.at[2 * g + col, pl.ds(0, nh - (g == self_g)), pl.ds(0, 2 * slots_of[col])]

    def z_sum(col):
        for g in range(2):
            part = z_part(g, col)
            stage = 2 * g + col
            remote(part, part, zsem.at[stage, 0], zsem.at[stage, 1], left, c).wait_recv()
        rows = slice(0, 2 * slots_of[col])
        total = zs[2 * self_g + col, self_j, rows].astype(F32)
        for g in range(2):
            for j in range(nh):
                if (g, j) != (self_g, self_j):
                    total = total + zr[2 * g + col, j, rows].astype(F32)
        return total

    chain_wait(2)
    mark("z_send_a")
    z_send(0, 0)
    z_send(0, 1)
    mark("fold_b")
    for h in range(2):
        fold(1, h)
    mark("z_send_b")
    z_send(1, 0)
    z_send(1, 1)

    mark("share")
    pltpu.make_async_copy(wm.at[c], wm.at[c], lsem.at[11]).wait()
    for k in range(3):
        send(wm.at[c, k], wm.at[c, k], psem.at[6], psem.at[7], kv, other)
    mark("z_wait_a")
    pack0[...] = z_sum(0)
    mark("heads_a")
    own = []
    inverse = []
    qh = qb // 2
    for i in range(2):
        at = i * slots_of[0]
        inv = lax.rsqrt(pack0[at + 3 * qb : at + 3 * qb + 1, :] * (1.0 / width) + EPS)
        inverse.append(inv)
        query = pack0[at : at + qb, :] * inv * dk ** (-0.5)
        key = pack0[at + qb : at + 2 * qb, :] * inv
        raw = pack0[at + 2 * qb : at + 3 * qb, :] * inv
        decay = (jnp.minimum(raw, 0.0) - jnp.log1p(jnp.exp(-jnp.abs(raw)))) / GATE_NORM
        qe[i * qb : (i + 1) * qb, :] = query * jnp.exp(decay)
        both = query * key
        for h in range(2):
            part = jnp.sum(both[h * qh : (h + 1) * qh, :], axis=0, keepdims=True)
            own.append(jnp.sum(part, axis=1, keepdims=True))
    for i in range(2):
        for h in range(2):
            row = jnp.concatenate(
                [qe[i * qb + h * qh + b : i * qb + h * qh + b + 1, :] for b in range(qh)], axis=1
            )
            high, low = high_low(row)
            got = dot(jnp.concatenate([high, low], axis=0), memory[i, h])
            got = got[0:1] + got[1:2]
            for b in range(hb):
                att[i * vb + h * hb + b : i * vb + h * hb + b + 1, :] = got[
                    :, b * LANES : (b + 1) * LANES
                ]
    mark("z_wait_b")
    pack1[...] = z_sum(1)
    for i in range(2):
        at = i * slots_of[1]
        if i == 0:
            mark("heads_b")
        value = pack1[at : at + vb, :] * inverse[i]
        gate = pack1[at + vb : at + 2 * vb, :] * inverse[i]
        attended = att[i * vb : (i + 1) * vb, :]
        for h in range(2):
            part = slice(h * hb, (h + 1) * hb)
            full = attended[part] + own[2 * i + h] * value[part]
            mean = jnp.sum(jnp.sum(full * full, axis=0, keepdims=True), axis=1, keepdims=True)
            norm = full * lax.rsqrt(mean * (1.0 / (hb * LANES)) + EPS) * hg[part, :]
            g = gate[part]
            headf[i * (headf.shape[0] // 2) + h * hb : i * (headf.shape[0] // 2) + (h + 1) * hb, :] = (
                g / (1.0 + jnp.exp(-g)) * norm
            )
    mrows = headf.shape[0] // 2
    for i in range(2):
        hmine[i] = headf[i * mrows : (i + 1) * mrows, :].astype(BF16)
    headb[2 * kv + c] = jnp.where(c == 0, headf[:mrows, :], headf[mrows:, :]).astype(BF16)

    def gather(buf, sems, consume):
        out_sem = sems.at[0]
        mine = buf.at[kv]

        def in_z(zp):
            return sems.at[1 + zp]

        def in_x(zp):
            return sems.at[1 + nz + zp]

        for zp in far:
            send(mine, mine, out_sem, in_z(z), zp * NX + x, c)
        for xp in sides:
            send(mine, mine, out_sem, in_x(z), z * NX + xp, c)
        for zp in near:
            slot = buf.at[zp * NX + x]
            remote(slot, slot, out_sem, in_z(zp), zp * NX + x, c).wait_recv()
            for xp in sides:
                send(slot, slot, out_sem, in_x(zp), z * NX + xp, c)
        mark("take_x")
        for zp in [z] + near:
            part = buf.at[pl.ds(0, NX - 1)]
            remote(part, part, out_sem, in_x(zp), left, c).wait_recv()
            consume(zp)

    def gather_drain(buf, sems):
        part = buf.at[pl.ds(0, nz * NX - 1)]
        remote(part, part, sems.at[0], sems.at[1], left, c).wait_send()

    n_kv = nz * NX

    mark("gather_heads")
    out_sem = hsem.at[0]
    slot = headb.at[2 * kv + c]
    for zp in far:
        send(hmine.at[c], slot, out_sem, hsem.at[1 + z], zp * NX + x, c)
        send(hmine.at[other], slot, out_sem, hsem.at[1 + z], zp * NX + x, other)
    send(hmine.at[other], slot, out_sem, hsem.at[1 + z], kv, other)
    for zp in [z] + near:
        part = headb.at[pl.ds(0, 2 - (zp is z))]
        remote(part, part, out_sem, hsem.at[1 + zp], zp * NX + x, other).wait_recv()
        pair = headb.at[pl.ds(2 * (zp * NX + x), 2)]
        for xp in sides:
            send(pair, pair, out_sem, hsem.at[1 + nz + zp], z * NX + xp, c)
    mark("heads_x")
    for zp in [z] + near:
        part = headb.at[pl.ds(0, 2 * (NX - 1))]
        remote(part, part, out_sem, hsem.at[1 + nz + zp], left, c).wait_recv()
        for k in range(2 * NX):
            at = 2 * NX * zp + k
            headsf[pl.ds(pl.multiple_of(at * mrows, 8), mrows), :] = headb[at].astype(F32)

    mark("project_out")
    for cc in range(2):
        for b in range(vb):
            at = (cc * vb + b) * LANES
            lhs[:, at : at + LANES] = headsf[
                pl.ds(cc * mrows + b, n_kv, stride=2 * mrows), :
            ].astype(BF16)
    remote(wo.at[other], wo.at[other], psem.at[2], psem.at[3], kv, other).wait_recv()
    projected = dot(lhs[...], wo[...].reshape(LANES, 2 * vb * LANES), ((1,), (1,)))
    tokens_half = jnp.where(
        c == 0, tokf[pl.ds(0, n_kv, stride=2), :], tokf[pl.ds(1, n_kv, stride=2), :]
    )
    after = (tokens_half + projected).astype(BF16)
    whole[kv] = after
    kept[c] = after

    mark("gather_after")
    remote(wm.at[other], wm.at[other], psem.at[6], psem.at[7], kv, other).wait_recv()
    units = hidden.shape[2]
    energy = [jnp.zeros((n_kv, LANES), F32)]
    sums = [jnp.zeros((n_kv, units), F32) for _ in range(4)]

    def multiply(zp):
        parts = []
        for xp in range(NX):
            k = zp * NX + xp
            rows = whole[k].astype(F32)
            energy[0] = energy[0] + rows * rows
            parts.append((rows * mgainf[pl.ds(k, 1), :]).astype(BF16))
        rows = jnp.concatenate(parts, axis=1)
        cols = pl.ds(pl.multiple_of(zp * NX * LANES, LANES), NX * LANES)
        for k in range(4):
            sums[k] = sums[k] + dot(rows, wm[k // 2, k % 2, :, cols], ((1,), (1,)))

    gather(whole, asem, multiply)
    send(kept.at[c], kept.at[c], psem.at[4], psem.at[5], kv, other)

    mark("mlp_in")
    inv = lax.rsqrt(jnp.sum(energy[0], axis=1, keepdims=True) * (1.0 / width) + EPS)
    for cc in range(2):
        gate = sums[2 * cc] * inv
        up = sums[2 * cc + 1] * inv
        hidden[cc] = (gate / (1.0 + jnp.exp(-gate)) * up).astype(BF16)
    mark("mlp_down")
    for g in range(2):
        for j in range(nh):
            cols = pl.ds(pl.multiple_of(zrel(g, j) * NX * LANES, LANES), NX * LANES)
            part = (dot(hidden[0], wm[0, 2, :, cols]) + dot(hidden[1], wm[1, 2, :, cols])).astype(
                BF16
            )
            for xp in range(NX):
                for k in range(2):
                    dx[g, 2 * xp + k, :, j * LANES : (j + 1) * LANES] = part[
                        k * n_kv // 2 : (k + 1) * n_kv // 2, xp * LANES : (xp + 1) * LANES
                    ]
        for n, xp in enumerate(sides):
            send(
                dx.at[g, pl.ds(2 * xp, 2)],
                drb.at[g, pl.ds(2 * n, 2)],
                dxsem.at[g, 0],
                dxsem.at[g, 1],
                z * NX + xp,
                c,
            )
    low_lanes = lax.broadcasted_iota(jnp.int32, (n_kv // 2, LANES), 1) < LANES // 2

    def squeeze(top, bottom, right):
        if right:
            top = pltpu.roll(top, LANES // 2, 1)
        else:
            bottom = pltpu.roll(bottom, LANES // 2, 1)
        return jnp.where(low_lanes, top, bottom)

    mark("down_x2")
    for g in range(2):
        part = drb.at[g]
        remote(part, part, dxsem.at[g, 0], dxsem.at[g, 1], left, c).wait_recv()
        top, bottom = [
            dx[g, 2 * x + k].astype(F32)
            + sum(drb[g, 2 * n + k].astype(F32) for n in range(NX - 1))
            for k in range(2)
        ]
        for j in by_distance(g):
            cols = slice(j * LANES, (j + 1) * LANES)
            slot = 2 * (g * nh + j)
            for cc in range(2):
                dzs[slot + cc] = squeeze(top[:, cols], bottom[:, cols], cc == 1).astype(BF16)
            if (g, j) == (self_g, self_j):
                dzr[slot + c] = dzs[slot + c]
                send(dzs.at[slot + other], dzr.at[slot + c], dzsem.at[0], dzsem.at[1], kv, other)
            else:
                for cc in (other, c):
                    send(
                        dzs.at[slot + cc],
                        dzr.at[slot + c],
                        dzsem.at[0],
                        dzsem.at[1],
                        zrel(g, j) * NX + x,
                        cc,
                    )
    mark("down_z")
    part = dzr.at[pl.ds(0, 2 * nz - 1)]
    remote(part, part, dzsem.at[0], dzsem.at[1], kv, other).wait_recv()
    mark("finish")
    remote(kept.at[other], kept.at[other], psem.at[4], psem.at[5], kv, other).wait_recv()
    for i in range(2):
        rows = kept[i].astype(F32)
        halves = rows[: n_kv // 2], rows[n_kv // 2 :]
        total = jnp.where(c == 1, squeeze(*halves, True), squeeze(*halves, False))
        for zp in range(nz):
            total = total + dzr[2 * zp + i].astype(F32)
        outf[pl.ds(i, n_kv // 2, stride=2), :] = total
        outf[pl.ds(i + n_kv, n_kv // 2, stride=2), :] = pltpu.roll(total, LANES // 2, 1)
    out[...] = outf[:, : LANES // 2]
    mark("drain")
    remote(tok.at[c], tok.at[c], psem.at[0], psem.at[1], kv, other).wait_send()
    remote(wo.at[c], wo.at[c], psem.at[2], psem.at[3], kv, other).wait_send()
    for g in range(2):
        for col in range(2):
            stage = 2 * g + col
            x_drain((xa, xb)[col].at[g], stage)
            part = z_part(g, col)
            remote(part, part, zsem.at[stage, 0], zsem.at[stage, 1], left, c).wait_send()
        part = drb.at[g]
        remote(part, part, dxsem.at[g, 0], dxsem.at[g, 1], left, c).wait_send()
    part = headb.at[pl.ds(0, 2 * nz * NX - 1)]
    remote(part, part, hsem.at[0], hsem.at[1], left, c).wait_send()
    gather_drain(whole, asem)
    remote(kept.at[c], kept.at[c], psem.at[4], psem.at[5], kv, other).wait_send()
    remote(wm.at[c], wm.at[c], psem.at[6], psem.at[7], kv, other).wait_send()
    part = dzr.at[pl.ds(0, 2 * nz - 1)]
    remote(part, part, dzsem.at[0], dzsem.at[1], kv, other).wait_send()
    mark()


def shards(
    tokens,
    lengths,
    state,
    cache_keys,
    cache_values,
    cache_rates,
    attn_gain,
    w_query,
    w_key,
    w_value,
    w_gate,
    w_decay,
    head_gain,
    w_out,
    mlp_gain,
    w_mlp_gate,
    w_mlp_up,
    w_mlp_down,
):
    n_kv = lax.axis_size("kv")
    nz = n_kv // NX
    heads, dk, dv = state.shape[1], state.shape[2], state.shape[3]
    width = mlp_gain.shape[0]
    qb, vb = heads * dk // LANES, heads * dv // LANES
    half0, half1 = (3 * qb + 2) // 2, vb
    slots_a, slots_b = [-(-2 * half // 4) * 4 for half in (half0, half1)]
    slots = max(slots_a, slots_b)
    nh = nz // 2
    seqs = 2 * n_kv
    mrows = -(-vb // 8) * 8
    units = w_mlp_down.shape[0]
    cols5 = nh * LANES
    vmem, dma = pltpu.VMEM, pltpu.SemaphoreType.DMA
    bf, fl = BF16, F32
    scratch = [
        vmem((2, seqs, LANES // 2), bf),
        vmem((seqs, LANES), fl),
        vmem(w_query.shape, bf),
        vmem(w_key.shape, bf),
        vmem(w_decay.shape, bf),
        vmem(w_value.shape, bf),
        vmem(w_gate.shape, bf),
        vmem(state.shape, fl),
        vmem(cache_keys.shape, bf),
        vmem(cache_values.shape, bf),
        vmem(cache_rates.shape, fl),
        vmem((2,) + w_out.shape[::-1], bf),
        vmem((2, 3) + w_mlp_down.shape, bf),
        vmem((2, NX * 2, nz, half0 * LANES), bf),
        vmem((2, NX * 2, nz, half1 * LANES), bf),
        vmem((2, 2, nz, half0 * LANES), bf),
        vmem((2, 2, nz, half1 * LANES), bf),
        vmem((2, 2, nz, half0 * LANES), bf),
        vmem((2, 2, nz, half1 * LANES), bf),
        vmem((2, 4, nz, half0 * LANES), bf),
        vmem((2, 4, nz, half1 * LANES), bf),
        vmem((nz * slots, LANES), fl),
        vmem((4, nh, 2 * slots, LANES), bf),
        vmem((4, nh, 2 * slots, LANES), bf),
        vmem(state.shape, bf),
        vmem((2 * slots_a, LANES), fl),
        vmem((2 * slots_b, LANES), fl),
        vmem((2 * qb, LANES), fl),
        vmem((2 * vb, LANES), fl),
        vmem((vb, LANES), fl),
        vmem((2 * mrows, LANES), fl),
        vmem((2, mrows, LANES), bf),
        vmem((2 * n_kv, mrows, LANES), bf),
        vmem((2 * n_kv * mrows, LANES), fl),
        vmem((n_kv, 2 * vb * LANES), bf),
        vmem((n_kv, n_kv, LANES), bf),
        vmem((2, n_kv, units), bf),
        vmem((2, n_kv, LANES), bf),
        vmem((2, NX * 2, n_kv // 2, cols5), bf),
        vmem((2, 2 * (NX - 1), n_kv // 2, cols5), bf),
        vmem((2 * nz, n_kv // 2, LANES), bf),
        vmem((2 * nz, n_kv // 2, LANES), bf),
        vmem((seqs, LANES), fl),
        vmem((1, LANES), bf),
        vmem((heads, dv), bf),
        vmem((n_kv, LANES), bf),
        vmem((n_kv, LANES), fl),
        pltpu.SMEM((2,), jnp.int32),
        dma((16,)),
        dma((8,)),
        dma((4, 4)),
        dma((4, 2)),
        dma((1 + 2 * nz,)),
        dma((1 + 2 * nz,)),
        dma((2, 2)),
        dma((2,)),
        pltpu.SemaphoreType.REGULAR((max(1, 2 * (nz // 2) - 3),)),
    ]
    anywhere = pl.BlockSpec(memory_space=pl.ANY)
    in_vmem = pl.BlockSpec(memory_space=pltpu.VMEM)
    specs = [anywhere] * 18
    summed = pl.pallas_call(
        functools.partial(kernel, (nz, qb, vb, dk, width)),
        out_shape=pltpu.VMEM(tokens.shape, F32),
        in_specs=specs,
        out_specs=in_vmem,
        scratch_shapes=scratch,
        compiler_params=pltpu.CompilerParams(collective_id=0, has_side_effects=True),
        name="layer",
    )(
        tokens,
        lengths,
        state,
        cache_keys,
        cache_values,
        cache_rates,
        attn_gain.reshape(1, -1),
        w_query,
        w_key,
        w_value,
        w_gate,
        w_decay,
        head_gain,
        w_out.T,
        mlp_gain.reshape(-1, LANES),
        w_mlp_gate.T,
        w_mlp_up.T,
        w_mlp_down,
    )
    return summed.astype(BF16)


def solution(mesh):
    placed = (
        P("dp", ("kv", "tp")),
        P(("dp", "kv")),
        P(("dp", "kv"), "tp", None, None),
        P(("dp", "kv"), "tp", None, None),
        P(("dp", "kv"), "tp", None, None),
        P(("dp", "kv"), "tp", None, None),
        P("kv"),
        P("kv", "tp"),
        P("kv", "tp"),
        P("kv", "tp"),
        P("kv", "tp"),
        P("kv", "tp"),
        P("tp", None),
        P(None, ("kv", "tp")),
        P(),
        P(None, ("kv", "tp")),
        P(None, ("kv", "tp")),
        P(("kv", "tp"), None),
    )
    return jax.shard_map(
        shards, mesh=mesh, in_specs=placed, out_specs=P("dp", ("kv", "tp")), check_vma=False
    )
```

```python
import functools

import jax
import jax.numpy as jnp
from jax import lax
from jax.experimental import pallas as pl
from jax.experimental.pallas import tpu as pltpu
from jax.sharding import PartitionSpec as P

EPS = 1e-06
GATE_NORM = 16.0
NX = 4
LANES = 128
MESH = pl.DeviceIdType.MESH
F32 = jnp.float32
BF16 = jnp.bfloat16


def dot(a, b, dims=((1,), (0,))):
    return lax.dot_general(a, b, (dims, ((), ())), preferred_element_type=F32)


def high_low(a):
    high = a.astype(BF16)
    return high, (a - high.astype(F32)).astype(BF16)


def kernel(
    sizes,
    tokens,
    lengths,
    state,
    cache_keys,
    cache_values,
    cache_rates,
    attn_gain,
    w_query,
    w_key,
    w_value,
    w_gate,
    w_decay,
    head_gain,
    w_out,
    mlp_gain,
    w_mlp_gate,
    w_mlp_up,
    w_mlp_down,
    out,
    tok,
    tokf,
    wq,
    wk,
    wd,
    wv,
    wg,
    st,
    ck,
    cv,
    cr,
    wo,
    wm,
    xa,
    xb,
    xfa,
    xfb,
    xsa,
    xsb,
    xba,
    xbb,
    zf,
    zs,
    zr,
    memory,
    pack0,
    pack1,
    qe,
    att,
    hg,
    headf,
    hmine,
    headb,
    headsf,
    lhs,
    whole,
    hidden,
    kept,
    dx,
    drb,
    dzs,
    dzr,
    outf,
    again,
    hgain,
    mgain,
    mgainf,
    lens,
    lsem,
    psem,
    xsem,
    zsem,
    hsem,
    asem,
    dxsem,
    dzsem,
    csem,
):
    nz, qb, vb, dk, width = sizes
    nh = nz // 2
    kv = lax.axis_index("kv")
    c = lax.axis_index("tp")
    other = 1 - c
    z = kv // NX
    x = kv % NX
    xr = (x + 1) % NX
    xl = (x + NX - 1) % NX
    xo = (x + 2) % NX
    steps = [((d + 1) // 2) * (1 if d % 2 else -1) for d in range(1, nz)]
    far = [(z + (s % nz)) % nz for s in steps][::-1]
    near = [(z + (s % nz)) % nz for s in steps]
    sides = [(x + d) % NX for d in (2, 1, 3)]

    def turn(g, j):
        return (nz // 4 + g * nh + j) % nz

    def zrel(g, j):
        return (z + turn(g, j)) % nz

    def by_distance(g):
        return sorted(range(nh), key=lambda j: -min(turn(g, j), nz - turn(g, j)))

    self_g, self_j = divmod((nz - nz // 4) % nz, nh)

    def local(i, src, dst):
        copy = pltpu.make_async_copy(src, dst, lsem.at[i])
        copy.start()
        return copy

    def remote(src, dst, send, recv, to_kv, to_tp):
        return pltpu.make_async_remote_copy(
            src_ref=src,
            dst_ref=dst,
            send_sem=send,
            recv_sem=recv,
            device_id={"kv": to_kv, "tp": to_tp},
            device_id_type=MESH,
        )

    scopes = []

    def mark(name=None):
        if scopes:
            scopes.pop().__exit__(None, None, None)
        if name:
            scopes.append(jax.named_scope(name))
            scopes[-1].__enter__()

    def send(*args):
        remote(*args).start()

    mark("barrier")
    barrier = pltpu.get_barrier_semaphore()

    def greet(to_kv, to_tp):
        pl.semaphore_signal(
            barrier, inc=1, device_id={"kv": to_kv, "tp": to_tp}, device_id_type=MESH
        )

    up, down = (z + 1) % nz, (z + nz - 1) % nz
    beside = [up, down][: nz - 1]
    for zp in beside:
        greet(zp * NX + x, c)
    for xp in (xr, xl):
        greet(z * NX + xp, c)
    greet(kv, other)
    mark("load")
    in_tok = local(0, tokens, tok.at[c])
    in_small = [
        local(12 + i, src, dst)
        for i, (src, dst) in enumerate(
            ((attn_gain, again), (head_gain, hgain), (mlp_gain, mgain), (lengths, lens))
        )
    ]
    in_w = [
        local(1 + i, src, dst)
        for i, (src, dst) in enumerate(
            ((w_query, wq), (w_key, wk), (w_decay, wd), (w_value, wv), (w_gate, wg))
        )
    ]
    in_cache = [
        local(6 + i, src, dst)
        for i, (src, dst) in enumerate(((cache_rates, cr), (cache_keys, ck), (cache_values, cv)))
    ]
    in_state = local(9, state, st)
    in_out = local(10, w_out, wo.at[c])
    in_mlp = [
        pltpu.make_async_copy(src, wm.at[c, i], lsem.at[11])
        for i, src in enumerate((w_mlp_gate, w_mlp_up, w_mlp_down))
    ]
    for copy in in_mlp:
        copy.start()

    mark("meet")
    pl.semaphore_wait(barrier, len(beside) + 3)

    rounds = nz // 2 - 1

    def chain_send(r):
        if r < rounds:
            device = {"kv": up * NX + x, "tp": c}
            pl.semaphore_signal(csem.at[2 * r], inc=1, device_id=device, device_id_type=MESH)
            if r + 2 <= (nz - 1) // 2:
                device = {"kv": down * NX + x, "tp": c}
                pl.semaphore_signal(
                    csem.at[2 * r + 1], inc=1, device_id=device, device_id_type=MESH
                )

    def chain_wait(r):
        if r < rounds:
            pl.semaphore_wait(csem.at[2 * r], 1)
            if r + 2 <= (nz - 1) // 2:
                pl.semaphore_wait(csem.at[2 * r + 1], 1)

    chain_send(0)

    mark("tokens")
    in_tok.wait()
    send(tok.at[c], tok.at[c], psem.at[0], psem.at[1], kv, other)
    remote(tok.at[other], tok.at[other], psem.at[0], psem.at[1], kv, other).wait_recv()
    tokf[...] = jnp.concatenate([tok[0].astype(F32), tok[1].astype(F32)], axis=1)
    block = []
    for xp in range(NX):
        pair = [
            pltpu.roll(
                tokf[pl.ds(2 * xp + i, nz, stride=2 * NX), :], (2 * nz - z - nz // 4) % nz, 0
            )
            for i in range(2)
        ]
        for g in range(2):
            block += [rows[g * nh : (g + 1) * nh] for rows in pair]
    block = jnp.concatenate(block, axis=0)
    in_small[0].wait()
    squares = jnp.sum(block * block, axis=1, keepdims=True)
    scaled = (block * again[...].astype(F32)).astype(BF16)

    def put(target, b, values):
        half = target.shape[3] // LANES
        at = (b % half) * LANES
        for xp in range(NX):
            for g in range(2):
                row = (2 * xp + g) * nz
                target[g, 2 * xp + b // half, :, at : at + LANES] = values[row : row + nz].astype(
                    BF16
                )

    def project(copy, weight, target, start):
        copy.wait()
        part = dot(scaled, weight[...])
        for b in range(weight.shape[1] // LANES):
            put(target, start + b, part[:, b * LANES : (b + 1) * LANES])

    left, right = z * NX + xl, z * NX + xr

    def x_first(src, first, back, stage):
        out_sem, in_left, in_right, in_back = [xsem.at[stage, k] for k in range(4)]
        send(src.at[2 * xo], first.at[0], out_sem, in_left, right, c)
        send(src.at[2 * xo + 1], first.at[1], out_sem, in_right, left, c)

    def x_direct(src, first, back, stage):
        out_sem, in_left, in_right, in_back = [xsem.at[stage, k] for k in range(4)]
        send(src.at[2 * xr + 1], back.at[1], out_sem, in_back, right, c)
        send(src.at[2 * xl], back.at[2], out_sem, in_back, left, c)

    def x_second(src, first, relay, back, stage):
        out_sem, in_left, in_right, in_back = [xsem.at[stage, k] for k in range(4)]
        remote(first.at[0], first.at[0], out_sem, in_left, left, c).wait_recv()
        relay[0] = (src[2 * xr].astype(F32) + first[0].astype(F32)).astype(BF16)
        send(relay.at[0], back.at[0], out_sem, in_back, right, c)
        remote(first.at[1], first.at[1], out_sem, in_right, right, c).wait_recv()
        relay[1] = (src[2 * xl + 1].astype(F32) + first[1].astype(F32)).astype(BF16)
        send(relay.at[1], back.at[3], out_sem, in_back, left, c)

    def x_wait(back, stage):
        remote(back, back, xsem.at[stage, 0], xsem.at[stage, 3], left, c).wait_recv()

    def x_drain(src, stage):
        part = src.at[pl.ds(0, 6)]
        remote(part, part, xsem.at[stage, 0], xsem.at[stage, 3], left, c).wait_send()

    def x_sum(src, back, half):
        return (
            src[2 * x + half].astype(F32) + back[half].astype(F32) + back[2 + half].astype(F32)
        )

    def x_stage(g, col):
        src, first, relay, back = ((xa, xfa, xsa, xba), (xb, xfb, xsb, xbb))[col]
        return src.at[g], first.at[g], relay.at[g], back.at[g], 2 * g + col

    def x_one(g, col):
        src, first, relay, back, stage = x_stage(g, col)
        x_first(src, first, back, stage)

    def x_ind(g, col):
        src, first, relay, back, stage = x_stage(g, col)
        x_direct(src, first, back, stage)

    project(in_w[0], wq, xa, 0)
    project(in_w[1], wk, xa, qb)
    project(in_w[2], wd, xa, 2 * qb)
    put(xa, 3 * qb, jnp.broadcast_to(squares, (squares.shape[0], LANES)))
    for b in range(3 * qb + 1, 2 * (xa.shape[3] // LANES)):
        put(xa, b, jnp.zeros((squares.shape[0], LANES), F32))
    x_one(0, 0)
    mark("project_b")
    project(in_w[3], wv, xb, 0)
    project(in_w[4], wg, xb, vb)
    x_one(0, 1)
    x_ind(0, 0)
    x_ind(0, 1)
    x_one(1, 0)
    x_one(1, 1)

    span = ck.shape[2]
    hb = vb // 2
    later = (
        lax.broadcasted_iota(jnp.int32, (span, span), 1)
        > lax.broadcasted_iota(jnp.int32, (span, span), 0)
    ).astype(BF16)
    ones = jnp.ones((span, LANES), BF16)
    slots = lax.broadcasted_iota(jnp.int32, (span, 1), 0)

    def fold(i, h):
        live = (slots < lens[i]).astype(F32)
        rates = cr[i, h] * live
        high, low = high_low(rates)
        rest = dot(later, high) + dot(later, low)
        keys = jnp.exp(-rest) * ck[i, h].astype(F32) * live
        shrink = jnp.exp(-(dot(high, ones, ((0,), (0,))) + dot(low, ones, ((0,), (0,)))))
        high, low = high_low(keys)
        value = cv[i, h]
        inner = dot(high, value, ((0,), (0,))) + dot(low, value, ((0,), (0,)))
        for b in range(hb):
            cols = slice(b * LANES, (b + 1) * LANES)
            memory[i, h, :, cols] = (st[i, h, :, cols] * shrink + inner[:, cols]).astype(BF16)

    mark("fold_a")
    chain_wait(0)
    chain_send(1)
    in_out.wait()
    send(wo.at[c], wo.at[c], psem.at[2], psem.at[3], kv, other)
    zf[...] = jnp.zeros_like(zf)
    for copy in in_small[1:]:
        copy.wait()
    mgainf[...] = mgain[...].astype(F32)
    for h in range(2):
        for b in range(hb):
            hg[h * hb + b : h * hb + b + 1, :] = hgain[
                h : h + 1, b * LANES : (b + 1) * LANES
            ].astype(F32)
    for copy in in_cache:
        copy.wait()
    in_state.wait()
    for h in range(2):
        fold(0, h)
    chain_wait(1)
    chain_send(2)
    mark("x_second_a")
    x_second(*x_stage(0, 0))
    x_second(*x_stage(0, 1))
    mark("x_second_b")
    x_ind(1, 0)
    x_ind(1, 1)
    x_second(*x_stage(1, 0))
    x_second(*x_stage(1, 1))

    slots_of = (pack0.shape[0] // 2, pack1.shape[0] // 2)

    def z_send(g, col):
        src, first, relay, back, stage = x_stage(g, col)
        half = src.shape[2] // LANES
        slots_row = slots_of[col]
        x_wait(back, stage)
        for hh in (0, 1):
            total = x_sum(src, back, hh)
            for b in range(half):
                for i in range(2):
                    zf[pl.ds(i * slots_row + hh * half + b, nh, stride=2 * slots_row), :] = total[
                        i * nh : (i + 1) * nh, b * LANES : (b + 1) * LANES
                    ]
        for j in by_distance(g):
            zs[stage, j, : 2 * slots_row] = zf[j * 2 * slots_row : (j + 1) * 2 * slots_row, :].astype(BF16)
            if (g, j) != (self_g, self_j):
                send(
                    zs.at[stage, j, pl.ds(0, 2 * slots_row)],
                    zr.at[stage, j, pl.ds(0, 2 * slots_row)],
                    zsem.at[stage, 0],
                    zsem.at[stage, 1],
                    zrel(g, j) * NX + x,
                    c,
                )

    def z_part(g, col):
        return zr.at[2 * g + col, pl.ds(0, nh - (g == self_g)), pl.ds(0, 2 * slots_of[col])]

    def z_sum(col):
        for g in range(2):
            part = z_part(g, col)
            stage = 2 * g + col
            remote(part, part, zsem.at[stage, 0], zsem.at[stage, 1], left, c).wait_recv()
        rows = slice(0, 2 * slots_of[col])
        total = zs[2 * self_g + col, self_j, rows].astype(F32)
        for g in range(2):
            for j in range(nh):
                if (g, j) != (self_g, self_j):
                    total = total + zr[2 * g + col, j, rows].astype(F32)
        return total

    chain_wait(2)
    mark("z_send_a")
    z_send(0, 0)
    z_send(0, 1)
    mark("fold_b")
    for h in range(2):
        fold(1, h)
    mark("z_send_b")
    z_send(1, 0)
    z_send(1, 1)

    mark("share")
    pltpu.make_async_copy(wm.at[c], wm.at[c], lsem.at[11]).wait()
    for k in range(3):
        send(wm.at[c, k], wm.at[c, k], psem.at[6], psem.at[7], kv, other)
    mark("z_wait_a")
    pack0[...] = z_sum(0)
    mark("heads_a")
    own = []
    inverse = []
    qh = qb // 2
    for i in range(2):
        at = i * slots_of[0]
        inv = lax.rsqrt(pack0[at + 3 * qb : at + 3 * qb + 1, :] * (1.0 / width) + EPS)
        inverse.append(inv)
        query = pack0[at : at + qb, :] * inv * dk ** (-0.5)
        key = pack0[at + qb : at + 2 * qb, :] * inv
        raw = pack0[at + 2 * qb : at + 3 * qb, :] * inv
        decay = (jnp.minimum(raw, 0.0) - jnp.log1p(jnp.exp(-jnp.abs(raw)))) / GATE_NORM
        qe[i * qb : (i + 1) * qb, :] = query * jnp.exp(decay)
        both = query * key
        for h in range(2):
            part = jnp.sum(both[h * qh : (h + 1) * qh, :], axis=0, keepdims=True)
            own.append(jnp.sum(part, axis=1, keepdims=True))
    for i in range(2):
        for h in range(2):
            row = jnp.concatenate(
                [qe[i * qb + h * qh + b : i * qb + h * qh + b + 1, :] for b in range(qh)], axis=1
            )
            high, low = high_low(row)
            got = dot(jnp.concatenate([high, low], axis=0), memory[i, h])
            got = got[0:1] + got[1:2]
            for b in range(hb):
                att[i * vb + h * hb + b : i * vb + h * hb + b + 1, :] = got[
                    :, b * LANES : (b + 1) * LANES
                ]
    mark("z_wait_b")
    pack1[...] = z_sum(1)
    for i in range(2):
        at = i * slots_of[1]
        if i == 0:
            mark("heads_b")
        value = pack1[at : at + vb, :] * inverse[i]
        gate = pack1[at + vb : at + 2 * vb, :] * inverse[i]
        attended = att[i * vb : (i + 1) * vb, :]
        for h in range(2):
            part = slice(h * hb, (h + 1) * hb)
            full = attended[part] + own[2 * i + h] * value[part]
            mean = jnp.sum(jnp.sum(full * full, axis=0, keepdims=True), axis=1, keepdims=True)
            norm = full * lax.rsqrt(mean * (1.0 / (hb * LANES)) + EPS) * hg[part, :]
            g = gate[part]
            headf[i * (headf.shape[0] // 2) + h * hb : i * (headf.shape[0] // 2) + (h + 1) * hb, :] = (
                g / (1.0 + jnp.exp(-g)) * norm
            )
    mrows = headf.shape[0] // 2
    for i in range(2):
        hmine[i] = headf[i * mrows : (i + 1) * mrows, :].astype(BF16)
    headb[2 * kv + c] = jnp.where(c == 0, headf[:mrows, :], headf[mrows:, :]).astype(BF16)

    def gather(buf, sems, consume):
        out_sem = sems.at[0]
        mine = buf.at[kv]

        def in_z(zp):
            return sems.at[1 + zp]

        def in_x(zp):
            return sems.at[1 + nz + zp]

        for zp in far:
            send(mine, mine, out_sem, in_z(z), zp * NX + x, c)
        for xp in sides:
            send(mine, mine, out_sem, in_x(z), z * NX + xp, c)
        for zp in near:
            slot = buf.at[zp * NX + x]
            remote(slot, slot, out_sem, in_z(zp), zp * NX + x, c).wait_recv()
            for xp in sides:
                send(slot, slot, out_sem, in_x(zp), z * NX + xp, c)
        mark("take_x")
        for zp in [z] + near:
            part = buf.at[pl.ds(0, NX - 1)]
            remote(part, part, out_sem, in_x(zp), left, c).wait_recv()
            consume(zp)

    def gather_drain(buf, sems):
        part = buf.at[pl.ds(0, nz * NX - 1)]
        remote(part, part, sems.at[0], sems.at[1], left, c).wait_send()

    n_kv = nz * NX

    mark("gather_heads")
    out_sem = hsem.at[0]
    slot = headb.at[2 * kv + c]
    for zp in far:
        send(hmine.at[c], slot, out_sem, hsem.at[1 + z], zp * NX + x, c)
        send(hmine.at[other], slot, out_sem, hsem.at[1 + z], zp * NX + x, other)
    send(hmine.at[other], slot, out_sem, hsem.at[1 + z], kv, other)
    for zp in [z] + near:
        part = headb.at[pl.ds(0, 2 - (zp is z))]
        remote(part, part, out_sem, hsem.at[1 + zp], zp * NX + x, other).wait_recv()
        pair = headb.at[pl.ds(2 * (zp * NX + x), 2)]
        for xp in sides:
            send(pair, pair, out_sem, hsem.at[1 + nz + zp], z * NX + xp, c)
    mark("heads_x")
    for zp in [z] + near:
        part = headb.at[pl.ds(0, 2 * (NX - 1))]
        remote(part, part, out_sem, hsem.at[1 + nz + zp], left, c).wait_recv()
        for k in range(2 * NX):
            at = 2 * NX * zp + k
            headsf[pl.ds(pl.multiple_of(at * mrows, 8), mrows), :] = headb[at].astype(F32)

    mark("project_out")
    for cc in range(2):
        for b in range(vb):
            at = (cc * vb + b) * LANES
            lhs[:, at : at + LANES] = headsf[
                pl.ds(cc * mrows + b, n_kv, stride=2 * mrows), :
            ].astype(BF16)
    remote(wo.at[other], wo.at[other], psem.at[2], psem.at[3], kv, other).wait_recv()
    projected = dot(lhs[...], wo[...].reshape(LANES, 2 * vb * LANES), ((1,), (1,)))
    tokens_half = jnp.where(
        c == 0, tokf[pl.ds(0, n_kv, stride=2), :], tokf[pl.ds(1, n_kv, stride=2), :]
    )
    after = (tokens_half + projected).astype(BF16)
    whole[kv] = after
    kept[c] = after

    mark("gather_after")
    remote(wm.at[other], wm.at[other], psem.at[6], psem.at[7], kv, other).wait_recv()
    units = hidden.shape[2]
    energy = [jnp.zeros((n_kv, LANES), F32)]
    sums = [jnp.zeros((n_kv, units), F32) for _ in range(4)]

    def multiply(zp):
        parts = []
        for xp in range(NX):
            k = zp * NX + xp
            rows = whole[k].astype(F32)
            energy[0] = energy[0] + rows * rows
            parts.append((rows * mgainf[pl.ds(k, 1), :]).astype(BF16))
        rows = jnp.concatenate(parts, axis=1)
        cols = pl.ds(pl.multiple_of(zp * NX * LANES, LANES), NX * LANES)
        for k in range(4):
            sums[k] = sums[k] + dot(rows, wm[k // 2, k % 2, :, cols], ((1,), (1,)))

    gather(whole, asem, multiply)
    send(kept.at[c], kept.at[c], psem.at[4], psem.at[5], kv, other)

    mark("mlp_in")
    inv = lax.rsqrt(jnp.sum(energy[0], axis=1, keepdims=True) * (1.0 / width) + EPS)
    for cc in range(2):
        gate = sums[2 * cc] * inv
        up = sums[2 * cc + 1] * inv
        hidden[cc] = (gate / (1.0 + jnp.exp(-gate)) * up).astype(BF16)
    mark("mlp_down")
    for g in range(2):
        for j in range(nh):
            cols = pl.ds(pl.multiple_of(zrel(g, j) * NX * LANES, LANES), NX * LANES)
            part = (dot(hidden[0], wm[0, 2, :, cols]) + dot(hidden[1], wm[1, 2, :, cols])).astype(
                BF16
            )
            for xp in range(NX):
                for k in range(2):
                    dx[g, 2 * xp + k, :, j * LANES : (j + 1) * LANES] = part[
                        k * n_kv // 2 : (k + 1) * n_kv // 2, xp * LANES : (xp + 1) * LANES
                    ]
        for n, xp in enumerate(sides):
            send(
                dx.at[g, pl.ds(2 * xp, 2)],
                drb.at[g, pl.ds(2 * n, 2)],
                dxsem.at[g, 0],
                dxsem.at[g, 1],
                z * NX + xp,
                c,
            )
    low_lanes = lax.broadcasted_iota(jnp.int32, (n_kv // 2, LANES), 1) < LANES // 2

    def squeeze(top, bottom, right):
        if right:
            top = pltpu.roll(top, LANES // 2, 1)
        else:
            bottom = pltpu.roll(bottom, LANES // 2, 1)
        return jnp.where(low_lanes, top, bottom)

    mark("down_x2")
    for g in range(2):
        part = drb.at[g]
        remote(part, part, dxsem.at[g, 0], dxsem.at[g, 1], left, c).wait_recv()
        top, bottom = [
            dx[g, 2 * x + k].astype(F32)
            + sum(drb[g, 2 * n + k].astype(F32) for n in range(NX - 1))
            for k in range(2)
        ]
        for j in by_distance(g):
            cols = slice(j * LANES, (j + 1) * LANES)
            slot = 2 * (g * nh + j)
            for cc in range(2):
                dzs[slot + cc] = squeeze(top[:, cols], bottom[:, cols], cc == 1).astype(BF16)
            if (g, j) == (self_g, self_j):
                dzr[slot + c] = dzs[slot + c]
                send(dzs.at[slot + other], dzr.at[slot + c], dzsem.at[0], dzsem.at[1], kv, other)
            else:
                for cc in (other, c):
                    send(
                        dzs.at[slot + cc],
                        dzr.at[slot + c],
                        dzsem.at[0],
                        dzsem.at[1],
                        zrel(g, j) * NX + x,
                        cc,
                    )
    mark("down_z")
    part = dzr.at[pl.ds(0, 2 * nz - 1)]
    remote(part, part, dzsem.at[0], dzsem.at[1], kv, other).wait_recv()
    mark("finish")
    remote(kept.at[other], kept.at[other], psem.at[4], psem.at[5], kv, other).wait_recv()
    for i in range(2):
        rows = kept[i].astype(F32)
        halves = rows[: n_kv // 2], rows[n_kv // 2 :]
        total = jnp.where(c == 1, squeeze(*halves, True), squeeze(*halves, False))
        for zp in range(nz):
            total = total + dzr[2 * zp + i].astype(F32)
        outf[pl.ds(i, n_kv // 2, stride=2), :] = total
        outf[pl.ds(i + n_kv, n_kv // 2, stride=2), :] = pltpu.roll(total, LANES // 2, 1)
    out[...] = outf[:, : LANES // 2]
    mark("drain")
    remote(tok.at[c], tok.at[c], psem.at[0], psem.at[1], kv, other).wait_send()
    remote(wo.at[c], wo.at[c], psem.at[2], psem.at[3], kv, other).wait_send()
    for g in range(2):
        for col in range(2):
            stage = 2 * g + col
            x_drain((xa, xb)[col].at[g], stage)
            part = z_part(g, col)
            remote(part, part, zsem.at[stage, 0], zsem.at[stage, 1], left, c).wait_send()
        part = drb.at[g]
        remote(part, part, dxsem.at[g, 0], dxsem.at[g, 1], left, c).wait_send()
    part = headb.at[pl.ds(0, 2 * nz * NX - 1)]
    remote(part, part, hsem.at[0], hsem.at[1], left, c).wait_send()
    gather_drain(whole, asem)
    remote(kept.at[c], kept.at[c], psem.at[4], psem.at[5], kv, other).wait_send()
    remote(wm.at[c], wm.at[c], psem.at[6], psem.at[7], kv, other).wait_send()
    part = dzr.at[pl.ds(0, 2 * nz - 1)]
    remote(part, part, dzsem.at[0], dzsem.at[1], kv, other).wait_send()
    mark()


def shards(
    tokens,
    lengths,
    state,
    cache_keys,
    cache_values,
    cache_rates,
    attn_gain,
    w_query,
    w_key,
    w_value,
    w_gate,
    w_decay,
    head_gain,
    w_out,
    mlp_gain,
    w_mlp_gate,
    w_mlp_up,
    w_mlp_down,
):
    n_kv = lax.axis_size("kv")
    nz = n_kv // NX
    heads, dk, dv = state.shape[1], state.shape[2], state.shape[3]
    width = mlp_gain.shape[0]
    qb, vb = heads * dk // LANES, heads * dv // LANES
    half0, half1 = (3 * qb + 2) // 2, vb
    slots_a, slots_b = [-(-2 * half // 4) * 4 for half in (half0, half1)]
    slots = max(slots_a, slots_b)
    nh = nz // 2
    seqs = 2 * n_kv
    mrows = -(-vb // 8) * 8
    units = w_mlp_down.shape[0]
    cols5 = nh * LANES
    vmem, dma = pltpu.VMEM, pltpu.SemaphoreType.DMA
    bf, fl = BF16, F32
    scratch = [
        vmem((2, seqs, LANES // 2), bf),
        vmem((seqs, LANES), fl),
        vmem(w_query.shape, bf),
        vmem(w_key.shape, bf),
        vmem(w_decay.shape, bf),
        vmem(w_value.shape, bf),
        vmem(w_gate.shape, bf),
        vmem(state.shape, fl),
        vmem(cache_keys.shape, bf),
        vmem(cache_values.shape, bf),
        vmem(cache_rates.shape, fl),
        vmem((2,) + w_out.shape[::-1], bf),
        vmem((2, 3) + w_mlp_down.shape, bf),
        vmem((2, NX * 2, nz, half0 * LANES), bf),
        vmem((2, NX * 2, nz, half1 * LANES), bf),
        vmem((2, 2, nz, half0 * LANES), bf),
        vmem((2, 2, nz, half1 * LANES), bf),
        vmem((2, 2, nz, half0 * LANES), bf),
        vmem((2, 2, nz, half1 * LANES), bf),
        vmem((2, 4, nz, half0 * LANES), bf),
        vmem((2, 4, nz, half1 * LANES), bf),
        vmem((2 * nz * slots, LANES), fl),
        vmem((4, nh, 2 * slots, LANES), bf),
        vmem((4, nh, 2 * slots, LANES), bf),
        vmem(state.shape, bf),
        vmem((2 * slots_a, LANES), fl),
        vmem((2 * slots_b, LANES), fl),
        vmem((2 * qb, LANES), fl),
        vmem((2 * vb, LANES), fl),
        vmem((vb, LANES), fl),
        vmem((2 * mrows, LANES), fl),
        vmem((2, mrows, LANES), bf),
        vmem((2 * n_kv, mrows, LANES), bf),
        vmem((2 * n_kv * mrows, LANES), fl),
        vmem((n_kv, 2 * vb * LANES), bf),
        vmem((n_kv, n_kv, LANES), bf),
        vmem((2, n_kv, units), bf),
        vmem((2, n_kv, LANES), bf),
        vmem((2, NX * 2, n_kv // 2, cols5), bf),
        vmem((2, 2 * (NX - 1), n_kv // 2, cols5), bf),
        vmem((2 * nz, n_kv // 2, LANES), bf),
        vmem((2 * nz, n_kv // 2, LANES), bf),
        vmem((seqs, LANES), fl),
        vmem((1, LANES), bf),
        vmem((heads, dv), bf),
        vmem((n_kv, LANES), bf),
        vmem((n_kv, LANES), fl),
        pltpu.SMEM((2,), jnp.int32),
        dma((16,)),
        dma((8,)),
        dma((4, 4)),
        dma((4, 2)),
        dma((1 + 2 * nz,)),
        dma((1 + 2 * nz,)),
        dma((2, 2)),
        dma((2,)),
        pltpu.SemaphoreType.REGULAR((max(1, 2 * (nz // 2) - 3),)),
    ]
    anywhere = pl.BlockSpec(memory_space=pl.ANY)
    in_vmem = pl.BlockSpec(memory_space=pltpu.VMEM)
    specs = [anywhere] * 18
    summed = pl.pallas_call(
        functools.partial(kernel, (nz, qb, vb, dk, width)),
        out_shape=pltpu.VMEM(tokens.shape, F32),
        in_specs=specs,
        out_specs=in_vmem,
        scratch_shapes=scratch,
        compiler_params=pltpu.CompilerParams(collective_id=0, has_side_effects=True),
        name="layer",
    )(
        tokens,
        lengths,
        state,
        cache_keys,
        cache_values,
        cache_rates,
        attn_gain.reshape(1, -1),
        w_query,
        w_key,
        w_value,
        w_gate,
        w_decay,
        head_gain,
        w_out.T,
        mlp_gain.reshape(-1, LANES),
        w_mlp_gate.T,
        w_mlp_up.T,
        w_mlp_down,
    )
    return summed.astype(BF16)


def solution(mesh):
    placed = (
        P("dp", ("kv", "tp")),
        P(("dp", "kv")),
        P(("dp", "kv"), "tp", None, None),
        P(("dp", "kv"), "tp", None, None),
        P(("dp", "kv"), "tp", None, None),
        P(("dp", "kv"), "tp", None, None),
        P("kv"),
        P("kv", "tp"),
        P("kv", "tp"),
        P("kv", "tp"),
        P("kv", "tp"),
        P("kv", "tp"),
        P("tp", None),
        P(None, ("kv", "tp")),
        P(),
        P(None, ("kv", "tp")),
        P(None, ("kv", "tp")),
        P(("kv", "tp"), None),
    )
    return jax.shard_map(
        shards, mesh=mesh, in_specs=placed, out_specs=P("dp", ("kv", "tp")), check_vma=False
    )
```
